256 devices in a mesh: st: 64 (over z, y, core), tp: 4 (over x).
Axes of the slice: x: 4, y: 4, z: 8, core: 2. Of those that a mesh axis runs over, the one named last changes fastest.
Arguments:
- tokens: bfloat16 [24576, 2048], P('st', 'tp'), may hold values from -6 to 6
- cotangent: bfloat16 [24576, 1024], P('st', 'tp'), may hold values from -48 to 48
- mix_query: bfloat16 [24576, 1024], P('st', 'tp'), may hold values from -6 to 6
- mix_key: bfloat16 [24576, 1024], P('st', 'tp'), may hold values from -6 to 6
- mix_value: bfloat16 [24576, 1024], P('st', 'tp'), may hold values from -24 to 24
- beta_pre: float32 [8, 24576], P('tp', 'st'), may hold values from -9 to 9
- decay_pre: float32 [8, 24576], P('tp', 'st'), may hold values from -8 to 6
- decay_rate: float32 [8], P('tp'), may hold values from 0.001 to 0.06
- passages: bfloat16 [1024, 64, 2048], P('st'), may hold values from -16 to 16
- passage_ids: int32 [384, 4], P('st'), may hold values from 0 to 1023, as said below
- query_weight: bfloat16 [2048, 1024], P(None, 'tp'), may hold values from -0.125 to 0.125
- key_weight: bfloat16 [2048, 1024], P(None, 'tp'), may hold values from -0.125 to 0.125
- value_weight: bfloat16 [2048, 1024], P(None, 'tp'), may hold values from -0.125 to 0.125
- gate_weight: bfloat16 [4, 2048], P('tp'), may hold values from -0.125 to 0.125
Outputs:
- token_grad: bfloat16 [24576, 2048], P('st', 'tp')
- passage_grad: bfloat16 [1024, 64, 2048], P('st', None, 'tp')
- key_weight_grad: float32 [2048, 1024], P('st', 'tp')
The draws below stay inside these ranges and needn't reach their ends.
Inputs may be any that keep to these rules, and one draw needn't show every extreme that they name: Passage p is stored on index p // 16 of st. The rows of passage_ids read by one index of st name at most 1 passages stored on any one index of st, and exactly 1 on some.
All inputs are finite; a program needn't handle non-finite values.
Results may differ from the reference program's by a relative error of at most 0.012.
The reference program's roundings to bfloat16 on the way count: a program that leaves them out, or rounds other values in their place, can miss the bound.
Values may be sent and summed in bfloat16 or wider, within the bound.
A program may use at most 128 MiB of HBM per device.

```python
import math
import jax
import jax.numpy as jnp
from jax import lax

D = 2048
HEADS = 4
HEAD = 256
MIX_HEADS = 8
MIX_DIM = 128
SPAN = 64
BLOCK = 64
PER_BLOCK = 4
PROWS = 64
TOK_DEV = 384
PASS_DEV = 16
TOKENS = 24576
BLOCKS = 384
REQ_DEV = 24
CAP = 1
PASSAGES = 1024
N_ST = 64


def draw_passage_ids(key, part):
    slot_count = N_ST * CAP
    shift_table = jax.random.randint(jax.random.fold_in(key, 9001), (N_ST,), 0, PASS_DEV)

    def per_reader(reader_idx):
        keys_split = jax.random.split(jax.random.fold_in(key, reader_idx), 4)
        rank_score = jax.random.permutation(keys_split[0], slot_count).astype(jnp.int32)
        slot_owner = jnp.arange(slot_count, dtype=jnp.int32) // CAP
        forced = (slot_owner == (reader_idx - 1) % N_ST) | (slot_owner == (reader_idx + N_ST // 2) % N_ST)
        rank_score = rank_score + forced.astype(jnp.int32) * (2 * slot_count)
        _, chosen = lax.top_k(rank_score, REQ_DEV)
        chosen = chosen.astype(jnp.int32)[jax.random.permutation(keys_split[1], REQ_DEV)]
        owner_ids = chosen // CAP
        first_draw = jax.random.randint(keys_split[2], (REQ_DEV,), 0, PASS_DEV)
        second_draw = jax.random.randint(keys_split[3], (REQ_DEV,), 0, PASS_DEV)
        local_ids = (jnp.minimum(first_draw, second_draw) + shift_table[owner_ids]) % PASS_DEV
        return (owner_ids * PASS_DEV + local_ids).astype(jnp.int32)
    every_id = jax.vmap(per_reader)(jnp.arange(N_ST, dtype=jnp.int32))
    return every_id.reshape(BLOCKS, PER_BLOCK)


def draw_decay_pre(key, part):
    keys_split = jax.random.split(key, 3)
    noise_part = 0.7 * jax.random.normal(keys_split[0], (MIX_HEADS, TOKENS), jnp.float32)
    slow_part = jax.random.uniform(keys_split[1], (MIX_HEADS, TOKENS // SPAN), jnp.float32, -1.2, 1.2)
    device_part = jax.random.uniform(keys_split[2], (MIX_HEADS, N_ST), jnp.float32, -1.0, 1.0)
    values_out = noise_part + jnp.repeat(slow_part, SPAN, axis=1) + jnp.repeat(device_part, TOK_DEV, axis=1)
    return jnp.clip(values_out, -8.0, 6.0)


def spiked(array, rng, source, target, parts, factor):
    owner, partner = [(jnp.arange(array.shape[dim]) // (array.shape[dim] // parts)).reshape([-1 if axis == dim else 1 for axis in range(array.ndim)]) for dim in (source, target)]
    chosen = jax.random.permutation(rng, parts)[partner]
    strong = (owner == chosen) | (owner == (partner + parts // 2) % parts)
    return jnp.where(strong, factor * array, array)


def level_of(key, extent, cuts, low, largest):
    def one(axis_at, blocks):
        draws = jax.random.uniform(jax.random.fold_in(jax.random.fold_in(key, 6), axis_at), (blocks,), jnp.float32, low / len(cuts), largest / len(cuts))
        return jnp.repeat(jnp.exp(draws), extent[axis_at] // blocks).reshape((-1,) + (1,) * (len(extent) - axis_at - 1))

    level = one(*cuts[0])
    for cut in cuts[1:]:
        level = level * one(*cut)
    return level


def scatter_about(rng, shape, scale, reach, pieces=(), kind=jnp.bfloat16):
    loudness = level_of(rng, shape, pieces, -0.22, 0.18) if pieces else 1.0
    values = jax.random.normal(rng, shape, jnp.float32) * scale * loudness
    return jnp.minimum(jnp.maximum(values, -reach), reach).astype(kind)


def noise_with(rng, extent, deviation, most, cuts, heavy, kind=jnp.bfloat16):
    entries = deviation * jax.random.normal(rng, extent, jnp.float32)
    if cuts:
        entries = entries * level_of(rng, extent, cuts, -0.22, 0.18)
    return jnp.clip(spiked(entries, jax.random.fold_in(rng, 3), *heavy), -most, most).astype(kind)


def setup_inputs(seed: int = 0) -> dict:
    streams_of = jax.random.split(jax.random.key(seed), 15)
    tokens = scatter_about(streams_of[0], (TOKENS, D), 1.0, 6.0, ((0, 64), (1, 4)))
    cotangent = scatter_about(streams_of[1], (TOKENS, HEADS * HEAD), 8.0, 48.0, ((0, 64), (1, 4)))
    mix_query = scatter_about(streams_of[2], (TOKENS, MIX_HEADS * MIX_DIM), 1.0, 6.0, ((0, 64), (1, 4)))
    mix_key = scatter_about(streams_of[3], (TOKENS, MIX_HEADS * MIX_DIM), 1.0, 6.0, ((0, 64), (1, 4)))
    mix_value = scatter_about(streams_of[4], (TOKENS, MIX_HEADS * MIX_DIM), 4.0, 24.0, ((0, 64), (1, 4)))
    beta_pre = scatter_about(streams_of[5], (MIX_HEADS, TOKENS), 1.5, 9.0, ((0, 4), (1, 64)), jnp.float32)
    decay_pre = draw_decay_pre(jax.random.fold_in(streams_of[14], 71), 0)
    decay_rate = jnp.clip(jnp.exp(math.log(0.06) - 4.0943445 * jax.random.uniform(streams_of[7], (MIX_HEADS,), jnp.float32) ** level_of(streams_of[7], (MIX_HEADS,), ((0, 4),), -0.2, 0.2)), 0.001, 0.06)
    passages = noise_with(streams_of[8], (PASSAGES, PROWS, D), 1.0, 16.0, ((0, 64),), (0, 2, 64, 4.0))
    passage_ids = draw_passage_ids(jax.random.fold_in(streams_of[14], 71), 0)
    query_weight = scatter_about(streams_of[10], (D, HEADS * HEAD), D ** -0.5, 0.125, ((1, 4),))
    key_weight = scatter_about(streams_of[11], (D, HEADS * HEAD), D ** -0.5, 0.125, ((1, 4),))
    value_weight = scatter_about(streams_of[12], (D, HEADS * HEAD), D ** -0.5, 0.125, ((1, 4),))
    gate_weight = scatter_about(streams_of[13], (HEADS, D), D ** -0.5, 0.125, ((0, 4),))
    return dict(tokens=tokens, cotangent=cotangent, mix_query=mix_query, mix_key=mix_key, mix_value=mix_value, beta_pre=beta_pre, decay_pre=decay_pre, decay_rate=decay_rate, passages=passages, passage_ids=passage_ids, query_weight=query_weight, key_weight=key_weight, value_weight=value_weight, gate_weight=gate_weight)


NORM_FLOOR = 1.0
SCORE_GAIN = 4.0
HIGHEST = lax.Precision.HIGHEST

def to_low(value):
    return lax.optimization_barrier(value.astype(jnp.bfloat16))

def neumann_inverse(strict_part):
    span_size = strict_part.shape[-1]
    unit_eye = jnp.eye(span_size, dtype=jnp.float32)
    running = unit_eye - strict_part
    power_term = strict_part
    for _ in range(span_size.bit_length() - 2):
        power_term = jnp.einsum('...ij,...jk->...ik', power_term, power_term, precision=HIGHEST)
        running = jnp.einsum('...ij,...jk->...ik', running, unit_eye + power_term, precision=HIGHEST)
    return running

def delta_mixer(queries, keys_in, values_in, strength, log_decay):
    heads_n, length, key_dim = queries.shape
    blocks_n = length // SPAN

    def to_blocks(tensor):
        return tensor.reshape(heads_n, blocks_n, SPAN, *tensor.shape[2:])
    queries, keys_in, values_in = (to_blocks(queries), to_blocks(keys_in), to_blocks(values_in))
    strength, log_decay = (to_blocks(strength), to_blocks(log_decay))
    cumulative = jnp.cumsum(log_decay, axis=-1)
    position = jnp.arange(SPAN)
    inclusive = position[:, None] >= position[None, :]
    strictly = position[:, None] > position[None, :]
    spread = jnp.where(inclusive, cumulative[..., :, None] - cumulative[..., None, :], -jnp.inf)
    decay_map = jnp.exp(spread)
    key_gram = jnp.einsum('hncd,hnmd->hncm', keys_in, keys_in, precision=HIGHEST)
    strict_part = jnp.where(strictly, strength[..., :, None] * key_gram * decay_map, 0.0)
    inverse = neumann_inverse(strict_part)
    fresh_vals = jnp.einsum('hncm,hnme->hnce', inverse, values_in * strength[..., None], precision=HIGHEST)
    correction = jnp.einsum('hncm,hnmd->hncd', inverse, keys_in * (strength * jnp.exp(cumulative))[..., None], precision=HIGHEST)
    attend_map = jnp.where(inclusive, jnp.einsum('hncd,hnmd->hncm', queries, keys_in, precision=HIGHEST) * decay_map, 0.0)
    query_dec = queries * jnp.exp(cumulative)[..., None]
    key_dec = keys_in * jnp.exp(cumulative[..., -1:] - cumulative)[..., None]
    carry_decay = jnp.exp(cumulative[..., -1])

    def advance(memory_state, inputs):
        fresh_blk, correct_blk, attend_blk, query_blk, key_blk, decay_blk = inputs
        new_values = fresh_blk - jnp.einsum('hcd,hde->hce', correct_blk, memory_state, precision=HIGHEST)
        output = jnp.einsum('hcd,hde->hce', query_blk, memory_state, precision=HIGHEST) + jnp.einsum('hcm,hme->hce', attend_blk, new_values, precision=HIGHEST)
        memory_state = memory_state * decay_blk[:, None, None] + jnp.einsum('hcd,hce->hde', key_blk, new_values, precision=HIGHEST)
        return (memory_state, output)
    stacked = tuple((jnp.moveaxis(tensor, 1, 0) for tensor in (fresh_vals, correction, attend_map, query_dec, key_dec, carry_decay)))
    initial = jnp.zeros((heads_n, key_dim, values_in.shape[-1]), jnp.float32)
    _, outputs = lax.scan(advance, initial, stacked)
    return jnp.transpose(outputs, (1, 0, 2, 3)).reshape(heads_n, length, -1)

def mixer_output(query_raw, key_raw, value_raw, beta_raw, decay_raw, rate_vals):
    length = query_raw.shape[0]
    heads_n = beta_raw.shape[0]

    def heads_first(matrix):
        return jnp.transpose(matrix.astype(jnp.float32).reshape(length, heads_n, -1), (1, 0, 2))
    queries = heads_first(query_raw)
    keys_in = heads_first(key_raw)
    values_in = heads_first(value_raw)
    queries = queries * lax.rsqrt(lax.optimization_barrier(jnp.sum(queries * queries, axis=-1, keepdims=True)) + NORM_FLOOR) * queries.shape[-1] ** (-0.5)
    keys_in = keys_in * lax.rsqrt(lax.optimization_barrier(jnp.sum(keys_in * keys_in, axis=-1, keepdims=True)) + NORM_FLOOR)
    strength = jax.nn.sigmoid(beta_raw)
    log_decay = -rate_vals[:, None] * jax.nn.softplus(decay_raw)
    mixer_out = delta_mixer(queries, keys_in, values_in, strength, log_decay)
    return jnp.transpose(mixer_out, (1, 0, 2)).reshape(length, -1)

def request_slots(id_rows, pass_count):
    owners = id_rows // pass_count
    local_idx = id_rows % pass_count
    req_count = id_rows.shape[-1]
    req_order = jnp.arange(req_count, dtype=jnp.int32)
    earlier = (owners[..., :, None] == owners[..., None, :]) & (req_order[None, :] < req_order[:, None])
    ranks = lax.optimization_barrier(jnp.sum(earlier.astype(jnp.int32), axis=-1, dtype=jnp.int32))
    return (owners, local_idx, ranks)

def reference(tokens, cotangent, mix_query, mix_key, mix_value, beta_pre, decay_pre, decay_rate, passages, passage_ids, query_weight, key_weight, value_weight, gate_weight):
    score_scale = SCORE_GAIN * HEAD ** (-0.5)
    every_id = passage_ids.reshape(N_ST, REQ_DEV)
    query_heads = query_weight.astype(jnp.float32).reshape(D, HEADS, HEAD)
    key_heads = key_weight.astype(jnp.float32).reshape(D, HEADS, HEAD)
    value_heads = value_weight.astype(jnp.float32).reshape(D, HEADS, HEAD)
    gate_float = gate_weight.astype(jnp.float32)
    blocks_n = TOK_DEV // BLOCK

    def reader(reader_idx):
        first_row = reader_idx * TOK_DEV
        tok_block = lax.dynamic_slice_in_dim(tokens, first_row, TOK_DEV, 0)
        query_low = to_low(jnp.dot(tok_block, query_weight, preferred_element_type=jnp.float32))
        query_float = query_low.astype(jnp.float32).reshape(TOK_DEV, HEADS, HEAD)
        query_scale = lax.rsqrt(lax.optimization_barrier(jnp.mean(query_float * query_float, axis=-1, keepdims=True)) + NORM_FLOOR)
        query_hat = to_low(query_float * query_scale)
        gate_open = jax.nn.sigmoid(jnp.dot(tok_block, gate_weight.T, preferred_element_type=jnp.float32))
        row_block = passages[every_id[reader_idx]].reshape(REQ_DEV * PROWS, D)
        key_low = to_low(jnp.dot(row_block, key_weight, preferred_element_type=jnp.float32))
        key_float = key_low.astype(jnp.float32).reshape(REQ_DEV * PROWS, HEADS, HEAD)
        key_scale = lax.rsqrt(lax.optimization_barrier(jnp.mean(key_float * key_float, axis=-1, keepdims=True)) + NORM_FLOOR)
        key_hat = to_low(key_float * key_scale)
        value_low = to_low(jnp.dot(row_block, value_weight, preferred_element_type=jnp.float32))
        key_blocks = key_hat.astype(jnp.float32).reshape(blocks_n, PER_BLOCK * PROWS, HEADS, HEAD)
        value_blocks = value_low.astype(jnp.float32).reshape(blocks_n, PER_BLOCK * PROWS, HEADS, HEAD)
        query_blocks = query_hat.astype(jnp.float32).reshape(blocks_n, BLOCK, HEADS, HEAD)
        scores = jnp.einsum('bihd,bjhd->bhij', query_blocks, key_blocks) * score_scale
        exp_scores = jnp.exp(scores)
        attn_probs = exp_scores / lax.optimization_barrier(jnp.sum(exp_scores, axis=-1, keepdims=True))
        probs_low = to_low(attn_probs).astype(jnp.float32)
        retrieved = jnp.einsum('bhij,bjhd->bihd', probs_low, value_blocks).reshape(TOK_DEV, HEADS, HEAD)
        mixer_out = mixer_output(lax.dynamic_slice_in_dim(mix_query, first_row, TOK_DEV, 0), lax.dynamic_slice_in_dim(mix_key, first_row, TOK_DEV, 0), lax.dynamic_slice_in_dim(mix_value, first_row, TOK_DEV, 0), lax.dynamic_slice_in_dim(beta_pre, first_row, TOK_DEV, 1), lax.dynamic_slice_in_dim(decay_pre, first_row, TOK_DEV, 1), decay_rate).reshape(TOK_DEV, HEADS, HEAD)
        grad_out = lax.dynamic_slice_in_dim(cotangent, first_row, TOK_DEV, 0).astype(jnp.float32).reshape(TOK_DEV, HEADS, HEAD)
        grad_ret = to_low(gate_open[..., None] * grad_out).astype(jnp.float32)
        gate_grad = lax.optimization_barrier(jnp.sum(grad_out * (retrieved - mixer_out), axis=-1)) * gate_open * (1.0 - gate_open)
        grad_blocks = grad_ret.reshape(blocks_n, BLOCK, HEADS, HEAD)
        grad_probs = jnp.einsum('bihd,bjhd->bhij', grad_blocks, value_blocks)
        score_grad = to_low(attn_probs * (grad_probs - lax.optimization_barrier(jnp.sum(grad_probs * attn_probs, axis=-1, keepdims=True)))).astype(jnp.float32)
        qhat_grad = score_scale * jnp.einsum('bhij,bjhd->bihd', score_grad, key_blocks).reshape(TOK_DEV, HEADS, HEAD)
        khat_grad = to_low(score_scale * jnp.einsum('bhij,bihd->bjhd', score_grad, query_blocks)).astype(jnp.float32).reshape(REQ_DEV, PROWS, HEADS, HEAD)
        value_grad = to_low(jnp.einsum('bhij,bihd->bjhd', probs_low, grad_blocks)).astype(jnp.float32).reshape(REQ_DEV, PROWS, HEADS, HEAD)
        query_grad = to_low(query_scale * qhat_grad - query_scale ** 3 * query_float * lax.optimization_barrier(jnp.mean(query_float * qhat_grad, axis=-1, keepdims=True))).astype(jnp.float32)
        partial_value = jnp.einsum('thd,ehd->the', query_grad, query_heads) + gate_grad[..., None] * gate_float[None]
        token_rows = lax.optimization_barrier(jnp.sum(to_low(partial_value).astype(jnp.float32), axis=1)).astype(jnp.bfloat16)
        return (token_rows, khat_grad, value_grad)
    token_rows, khat_all, value_all = lax.map(reader, jnp.arange(N_ST, dtype=jnp.int32))
    owner_all, local_all, rank_all = request_slots(every_id, PASS_DEV)
    cap_iota = jnp.arange(CAP, dtype=jnp.int32)
    req_iota = jnp.arange(REQ_DEV, dtype=jnp.int32)
    readers = jnp.arange(N_ST, dtype=jnp.int32)[:, None]
    pass_iota = jnp.arange(PASS_DEV, dtype=jnp.int32)

    def owner_step(weight_acc, owner_idx):
        wanted = (owner_all == owner_idx)[:, None, :] & (rank_all[:, None, :] == cap_iota[None, :, None])
        slot_used = jnp.any(wanted, axis=-1)
        slot_local = lax.optimization_barrier(jnp.sum(jnp.where(wanted, local_all[:, None, :], 0), axis=-1, dtype=jnp.int32))
        req_pick = lax.optimization_barrier(jnp.sum(jnp.where(wanted, req_iota[None, None, :], 0), axis=-1, dtype=jnp.int32))
        khat_slots = jnp.where(slot_used[:, :, None, None, None], khat_all[readers, req_pick], 0.0)
        value_slots = jnp.where(slot_used[:, :, None, None, None], value_all[readers, req_pick], 0.0)
        onehot = ((slot_local.reshape(-1)[None, :] == pass_iota[:, None]) & slot_used.reshape(-1)[None, :]).astype(jnp.float32)
        khat_pass = jnp.dot(onehot, khat_slots.reshape(N_ST * CAP, -1), precision=HIGHEST).reshape(PASS_DEV * PROWS, HEADS, HEAD)
        value_pass = jnp.dot(onehot, value_slots.reshape(N_ST * CAP, -1), precision=HIGHEST).reshape(PASS_DEV * PROWS, HEADS, HEAD)
        row_block = lax.dynamic_slice_in_dim(passages, owner_idx * PASS_DEV, PASS_DEV, 0).reshape(PASS_DEV * PROWS, D)
        key_low = to_low(jnp.dot(row_block, key_weight, preferred_element_type=jnp.float32))
        key_float = key_low.astype(jnp.float32).reshape(PASS_DEV * PROWS, HEADS, HEAD)
        key_scale = lax.rsqrt(lax.optimization_barrier(jnp.mean(key_float * key_float, axis=-1, keepdims=True)) + NORM_FLOOR)
        key_grad = to_low(key_scale * khat_pass - key_scale ** 3 * key_float * lax.optimization_barrier(jnp.mean(key_float * khat_pass, axis=-1, keepdims=True)))
        value_grad_low = to_low(value_pass)
        partial_value = jnp.einsum('rhd,ehd->rhe', key_grad.astype(jnp.float32), key_heads) + jnp.einsum('rhd,ehd->rhe', value_grad_low.astype(jnp.float32), value_heads)
        rows_grad = lax.optimization_barrier(jnp.sum(to_low(partial_value).astype(jnp.float32), axis=1)).astype(jnp.bfloat16).reshape(PASS_DEV, PROWS, D)
        weight_acc = weight_acc + jnp.dot(row_block.T, key_grad.reshape(PASS_DEV * PROWS, HEADS * HEAD), preferred_element_type=jnp.float32)
        return (weight_acc, rows_grad)
    weight_grad, store_grad = lax.scan(owner_step, jnp.zeros((D, HEADS * HEAD), jnp.float32), jnp.arange(N_ST, dtype=jnp.int32))
    return (token_rows.reshape(TOKENS, D), store_grad.reshape(PASSAGES, PROWS, D), weight_grad)
```

```python
import functools

import jax
import jax.numpy as jnp
from jax import lax
from jax.experimental import pallas as pl
from jax.experimental.pallas import tpu as pltpu
from jax.sharding import Mesh
from jax.sharding import PartitionSpec as P

SPAN = 64
ST = ("st_0", "st_1", "st_2")


NORM_FLOOR = 1.0
SCORE_GAIN = 4.0
CONTRACT_LAST = (((1,), (1,)), ((), ()))
CONTRACT_FIRST = (((0,), (0,)), ((), ()))


AXES = {"st_0": 8, "st_1": 4, "st_2": 2, "tp": 4}
MESH_ID = pl.DeviceIdType.MESH


def ring_starts(job, x_ref, o_ref, sems):
    axis, n, chunks = job["axis"], AXES[job["axis"]], job.get("chunks", 1)
    rows = x_ref.shape[0]
    me = lax.axis_index(axis)
    step_rows = rows // chunks

    def part(k, d, ch):
        lo, size = ch * step_rows, step_rows
        if k == n // 2 - 1:
            size = step_rows // 2
            lo = lo + (size if d else 0)
        return pl.ds(lo, size)

    def copy(k, d, ch):
        sgn = -1 if d else 1
        origin = lax.rem(me - sgn * k + 2 * n, n)
        rng = part(k, d, ch)
        src = x_ref.at[rng] if k == 0 else o_ref.at[origin, rng]
        return pltpu.make_async_remote_copy(
            src_ref=src, dst_ref=o_ref.at[origin, rng],
            send_sem=sems.at[0, d, k * chunks + ch], recv_sem=sems.at[1, d, k * chunks + ch],
            device_id={axis: lax.rem(me + sgn + n, n)}, device_id_type=MESH_ID)

    def arrival(k, d, ch):
        sgn = -1 if d else 1
        origin = lax.rem(me - sgn * (k + 1) + 2 * n, n)
        rng = part(k, d, ch)
        return pltpu.make_async_remote_copy(
            src_ref=o_ref.at[origin, rng], dst_ref=o_ref.at[origin, rng],
            send_sem=sems.at[0, d, k * chunks + ch], recv_sem=sems.at[1, d, k * chunks + ch],
            device_id={axis: lax.rem(me + sgn + n, n)}, device_id_type=MESH_ID)

    return copy, arrival, n // 2, chunks


def ring_peers(job):
    axis, n = job["axis"], AXES[job["axis"]]
    me = lax.axis_index(axis)
    return [{axis: lax.rem(me + 1, n)}, {axis: lax.rem(me + n - 1, n)}]


def shifts_of(axes):
    out = [()]
    for a in axes:
        out = [s + (d,) for s in out for d in range(AXES[a])]
    return [s for s in out if any(s)]


def index_of(axes, shift, sign):
    idx, dev = 0, {}
    for a, d in zip(axes, shift):
        n = AXES[a]
        c = lax.rem(lax.axis_index(a) + sign * d + n, n)
        dev[a] = c
        idx = idx * n + c
    return idx, dev


def a2a_copies(job, x_ref, o_ref, sems):
    axes = job["axes"]
    my_idx, _ = index_of(axes, (0,) * len(axes), 1)
    out = []
    for i, s in enumerate(shifts_of(axes)):
        dst_i, dst_d = index_of(axes, s, 1)
        src_i, _ = index_of(axes, s, -1)
        send = pltpu.make_async_remote_copy(
            src_ref=x_ref.at[dst_i], dst_ref=o_ref.at[my_idx], send_sem=sems.at[0, i],
            recv_sem=sems.at[1, i], device_id=dst_d, device_id_type=MESH_ID)
        recv = pltpu.make_async_remote_copy(
            src_ref=o_ref.at[src_i], dst_ref=o_ref.at[src_i], send_sem=sems.at[0, i],
            recv_sem=sems.at[1, i], device_id=dst_d, device_id_type=MESH_ID)
        out.append((send, recv))
    return my_idx, out


def a2a_peers(job):
    return [index_of(job["axes"], s, 1)[1] for s in shifts_of(job["axes"])]


def comm_kernel(jobs, *refs):
    nj = len(jobs)
    xs, os_, sems = refs[:nj], refs[nj:2 * nj], refs[2 * nj:]
    barrier = pltpu.get_barrier_semaphore()
    peers = []
    for job in jobs:
        peers += ring_peers(job) if job["kind"] == "ring" else a2a_peers(job)
    for p in peers:
        pl.semaphore_signal(barrier, inc=1, device_id=p, device_id_type=MESH_ID)
    pl.semaphore_wait(barrier, len(peers))
    rings, alls, sent = [], [], []
    for job, x, o, s in zip(jobs, xs, os_, sems):
        if job["kind"] == "ring":
            rings.append(ring_starts(job, x, o, s))
            c, a, steps, chunks = rings[-1]
            for ch in range(chunks):
                for d in range(2):
                    cp = c(0, d, ch); cp.start(); sent.append(cp)
    for job, x, o, s in zip(jobs, xs, os_, sems):
        if job["kind"] == "a2a":
            mine, cps = a2a_copies(job, x, o, s)
            for cp, _ in cps:
                cp.start(); sent.append(cp)
            alls.append((cps, mine, x, o))
            o[mine] = x[mine]
    for job, x, o in zip(jobs, xs, os_):
        if job["kind"] == "ring":
            o[lax.axis_index(job["axis"])] = x[...]
    for k in range(max([r[2] for r in rings], default=0)):
        for c, a, steps, chunks in rings:
            if k < steps:
                for ch in range(chunks):
                    for d in range(2):
                        a(k, d, ch).wait_recv()
                        if k + 1 < steps:
                            cp = c(k + 1, d, ch); cp.start(); sent.append(cp)
    for cps, *_ in alls:
        for _, r in cps:
            r.wait_recv()
    for cp in sent:
        cp.wait_send()


def comm(jobs, xs, cid):
    outs, sems = [], []
    for job, x in zip(jobs, xs):
        if job["kind"] == "ring":
            n = AXES[job["axis"]]
            outs.append(jax.ShapeDtypeStruct((n, *x.shape), x.dtype))
            sems.append(pltpu.SemaphoreType.DMA((2, 2, n // 2 * job.get("chunks", 1))))
        else:
            outs.append(jax.ShapeDtypeStruct(x.shape, x.dtype))
            sems.append(pltpu.SemaphoreType.DMA((2, len(shifts_of(job["axes"])))))
    return pl.pallas_call(
        functools.partial(comm_kernel, jobs),
        out_shape=outs,
        in_specs=[pl.BlockSpec(memory_space=pltpu.VMEM)] * len(xs),
        out_specs=[pl.BlockSpec(memory_space=pltpu.VMEM)] * len(xs),
        scratch_shapes=sems,
        compiler_params=pltpu.CompilerParams(collective_id=cid, has_side_effects=True),
    )(*xs)


def neumann_inverse(strict_part):
    span_size = strict_part.shape[-1]
    unit_eye = jnp.eye(span_size, dtype=jnp.float32)
    running = unit_eye - strict_part
    power_term = strict_part
    for _ in range(span_size.bit_length() - 2):
        power_term = jnp.einsum("...ij,...jk->...ik", power_term, power_term)
        running = jnp.einsum("...ij,...jk->...ik", running, unit_eye + power_term)
    return running


def delta_mixer(queries, keys_in, values_in, strength, log_decay):
    heads_n, length, key_dim = queries.shape
    blocks_n = length // SPAN

    def to_blocks(tensor):
        return tensor.reshape(heads_n, blocks_n, SPAN, *tensor.shape[2:])

    queries, keys_in, values_in = (to_blocks(queries), to_blocks(keys_in), to_blocks(values_in))
    strength, log_decay = (to_blocks(strength), to_blocks(log_decay))
    cumulative = jnp.cumsum(log_decay, axis=-1)
    position = jnp.arange(SPAN)
    inclusive = position[:, None] >= position[None, :]
    strictly = position[:, None] > position[None, :]
    spread = jnp.where(inclusive, cumulative[..., :, None] - cumulative[..., None, :], -jnp.inf)
    decay_map = jnp.exp(spread)
    key_gram = jnp.einsum("hncd,hnmd->hncm", keys_in, keys_in)
    strict_part = jnp.where(strictly, strength[..., :, None] * key_gram * decay_map, 0.0)
    inverse = neumann_inverse(strict_part)
    fresh_vals = jnp.einsum("hncm,hnme->hnce", inverse, values_in * strength[..., None])
    correction = jnp.einsum(
        "hncm,hnmd->hncd", inverse, keys_in * (strength * jnp.exp(cumulative))[..., None]
    )
    attend_map = jnp.where(
        inclusive, jnp.einsum("hncd,hnmd->hncm", queries, keys_in) * decay_map, 0.0
    )
    query_dec = queries * jnp.exp(cumulative)[..., None]
    key_dec = keys_in * jnp.exp(cumulative[..., -1:] - cumulative)[..., None]
    carry_decay = jnp.exp(cumulative[..., -1])

    def advance(memory_state, inputs):
        fresh_blk, correct_blk, attend_blk, query_blk, key_blk, decay_blk = inputs
        new_values = fresh_blk - jnp.einsum("hcd,hde->hce", correct_blk, memory_state)
        output = jnp.einsum("hcd,hde->hce", query_blk, memory_state) + jnp.einsum(
            "hcm,hme->hce", attend_blk, new_values
        )
        memory_state = memory_state * decay_blk[:, None, None] + jnp.einsum(
            "hcd,hce->hde", key_blk, new_values
        )
        return (memory_state, output)

    stacked = tuple(
        (
            jnp.moveaxis(tensor, 1, 0)
            for tensor in (fresh_vals, correction, attend_map, query_dec, key_dec, carry_decay)
        )
    )
    initial = jnp.zeros((heads_n, key_dim, values_in.shape[-1]), jnp.float32)
    _, outputs = lax.scan(advance, initial, stacked)
    return jnp.transpose(outputs, (1, 0, 2, 3)).reshape(heads_n, length, -1)


def mixer_output(query_raw, key_raw, value_raw, beta_raw, decay_raw, rate_vals):
    length = query_raw.shape[0]
    heads_n = beta_raw.shape[0]

    def heads_first(matrix):
        return jnp.transpose(matrix.astype(jnp.float32).reshape(length, heads_n, -1), (1, 0, 2))

    queries = heads_first(query_raw)
    keys_in = heads_first(key_raw)
    values_in = heads_first(value_raw)
    queries = (
        queries
        * lax.rsqrt(jnp.sum(queries * queries, axis=-1, keepdims=True) + NORM_FLOOR)
        * queries.shape[-1] ** (-0.5)
    )
    keys_in = keys_in * lax.rsqrt(jnp.sum(keys_in * keys_in, axis=-1, keepdims=True) + NORM_FLOOR)
    strength = jax.nn.sigmoid(beta_raw)
    log_decay = -rate_vals[:, None] * jax.nn.softplus(decay_raw)
    mixer_out = delta_mixer(queries, keys_in, values_in, strength, log_decay)
    return jnp.transpose(mixer_out, (1, 0, 2)).reshape(length, -1)


YC = ("st_1", "st_2")


def ring(axis, chunks=1):
    return dict(kind="ring", axis=axis, chunks=chunks)


def a2a(*axes):
    return dict(kind="a2a", axes=axes)


def rows_of(vec):
    flat = vec.reshape(-1, 128)
    return jnp.pad(flat, ((0, 16 - flat.shape[0]), (0, 0)))


def stats_kernel(x_ref, m_ref, w_ref, o_ref, wo_ref, got, tot, every, back, s1, s2, s3, sw):
    jobs = [a2a(*YC), a2a("st_0"), a2a("tp")]
    barrier = pltpu.get_barrier_semaphore()
    peers = []
    for job in jobs:
        peers += a2a_peers(job)
    for p in peers:
        pl.semaphore_signal(barrier, inc=1, device_id=p, device_id_type=MESH_ID)
    pl.semaphore_wait(barrier, len(peers))
    sent = []
    mine, cps = a2a_copies(jobs[0], x_ref, got, s1)
    for cp, _ in cps:
        cp.start()
        sent.append(cp)
    minew, cpw = a2a_copies(jobs[2], w_ref, wo_ref, sw)
    for cp, _ in cpw:
        cp.start()
        sent.append(cp)
    got[mine] = x_ref[mine]
    wo_ref[minew] = w_ref[minew]
    for _, r in cps:
        r.wait_recv()
    for b in range(6):
        acc = got[0] * m_ref[0, b]
        for j in range(1, 8):
            acc = acc + got[j] * m_ref[j, b]
        tot[b] = acc
    z = lax.axis_index("st_0")
    cps2 = []
    for s in range(1, 8):
        dst = lax.rem(z + s, 8)
        src = lax.rem(z - s + 8, 8)
        cp = pltpu.make_async_remote_copy(
            src_ref=tot, dst_ref=every.at[z], send_sem=s2.at[0, s], recv_sem=s2.at[1, s],
            device_id={"st_0": dst}, device_id_type=MESH_ID)
        rv = pltpu.make_async_remote_copy(
            src_ref=tot, dst_ref=every.at[src], send_sem=s2.at[0, s], recv_sem=s2.at[1, s],
            device_id={"st_0": dst}, device_id_type=MESH_ID)
        cp.start()
        sent.append(cp)
        cps2.append(rv)
    every[z] = tot[...]
    for rv in cps2:
        rv.wait_recv()
    whole = []
    for b in range(6):
        acc = every[0, b]
        for k in range(1, 8):
            acc = acc + every[k, b]
        whole.append(acc)
    for j in range(8):
        acc = whole[0] * m_ref[j, 0]
        for b in range(1, 6):
            acc = acc + whole[b] * m_ref[j, b]
        back[j] = acc
    mine, cps3 = a2a_copies(jobs[0], back, o_ref, s3)
    for cp, _ in cps3:
        cp.start()
        sent.append(cp)
    o_ref[mine] = back[mine]
    for _, r in cps3 + cpw:
        r.wait_recv()
    for cp in sent:
        cp.wait_send()


def stats_exchange(x, mask, w, cid):
    v = pl.BlockSpec(memory_space=pltpu.VMEM)
    f = jnp.float32
    return pl.pallas_call(
        stats_kernel,
        out_shape=[jax.ShapeDtypeStruct(x.shape, f), jax.ShapeDtypeStruct(w.shape, w.dtype)],
        in_specs=[v] * 3,
        out_specs=[v] * 2,
        scratch_shapes=[
            pltpu.VMEM((8, 8, 128), f), pltpu.VMEM((6, 8, 128), f), pltpu.VMEM((8, 6, 8, 128), f),
            pltpu.VMEM((8, 8, 128), f), pltpu.SemaphoreType.DMA((2, 7)), pltpu.SemaphoreType.DMA((2, 8)),
            pltpu.SemaphoreType.DMA((2, 7)), pltpu.SemaphoreType.DMA((2, 3))],
        compiler_params=pltpu.CompilerParams(collective_id=cid, has_side_effects=True),
    )(x, mask, w)


def dots_kernel(x_ref, m_ref, o_ref, got, tot, s1, s2):
    jobs = [a2a(*YC), a2a("st_0")]
    barrier = pltpu.get_barrier_semaphore()
    peers = a2a_peers(jobs[0]) + a2a_peers(jobs[1])
    for p in peers:
        pl.semaphore_signal(barrier, inc=1, device_id=p, device_id_type=MESH_ID)
    pl.semaphore_wait(barrier, len(peers))
    sent = []
    mine, cps = a2a_copies(jobs[0], x_ref, got, s1)
    for cp, _ in cps:
        cp.start()
        sent.append(cp)
    got[mine] = x_ref[mine]
    for _, r in cps:
        r.wait_recv()
    for b in range(6):
        acc = got[0] * m_ref[0, b]
        for j in range(1, 8):
            acc = acc + got[j] * m_ref[j, b]
        for zr in range(8):
            tot[zr, b:b + 1, :] = acc[zr:zr + 1, :]
    mine, cps2 = a2a_copies(jobs[1], tot, o_ref, s2)
    for cp, _ in cps2:
        cp.start()
        sent.append(cp)
    o_ref[mine] = tot[mine]
    for _, r in cps2:
        r.wait_recv()
    for cp in sent:
        cp.wait_send()


def dots_exchange(x, mask, cid):
    v = pl.BlockSpec(memory_space=pltpu.VMEM)
    f = jnp.float32
    return pl.pallas_call(
        dots_kernel,
        out_shape=jax.ShapeDtypeStruct((8, 8, 128), f),
        in_specs=[v] * 2,
        out_specs=v,
        scratch_shapes=[
            pltpu.VMEM((8, 8, 128), f), pltpu.VMEM((8, 8, 128), f),
            pltpu.SemaphoreType.DMA((2, 7)), pltpu.SemaphoreType.DMA((2, 7))],
        compiler_params=pltpu.CompilerParams(collective_id=cid, has_side_effects=True),
    )(x, mask)


def body(
    tokens, cotangent, mix_query, mix_key, mix_value, beta_pre, decay_pre, decay_rate,
    passages, passage_ids, query_weight, key_weight, value_weight, gate_weight,
):
    f32, bf16 = jnp.float32, jnp.bfloat16
    scale = SCORE_GAIN * 256 ** (-0.5)
    z = lax.axis_index("st_0")
    ids = passage_ids.reshape(24)
    owner, local = ids // 16, ids % 16
    match = owner[None, :] == jnp.arange(64, dtype=jnp.int32)[:, None]
    code_of = local * 8 + jnp.arange(24, dtype=jnp.int32) // 4
    code = jnp.sum(jnp.where(match, code_of[None, :], 0), axis=-1, dtype=jnp.int32)
    code = jnp.where(jnp.any(match, axis=-1), code, 128)
    table = jnp.pad(code.reshape(8, 8), ((0, 8), (0, 120)))

    tok4, cot_z, table_z = comm([ring("tp"), ring("st_0", 2), ring("st_0")], [tokens, cotangent, table], 1)
    codes = lax.dynamic_slice(table_z, (0, z, 0), (8, 1, 8)).reshape(8, 8)
    slot_block = (jnp.arange(8, dtype=jnp.int32)[:, None] * 6 + codes % 8).T
    cot_slots = cot_z.reshape(48, 64, 256)[slot_block]
    cot_here = lax.all_to_all(cot_slots, YC, split_axis=0, concat_axis=0, tiled=True).reshape(64, 64, 256)

    query_acc = lax.dot_general(
        tok4, query_weight.reshape(4, 512, 256), (((0, 2), (0, 1)), ((), ())), preferred_element_type=f32)
    gate_acc = jnp.einsum("ptk,pk->t", tok4, gate_weight.reshape(4, 512), preferred_element_type=f32)
    query_low = lax.optimization_barrier(query_acc.astype(bf16))
    query_float = query_low.astype(f32)
    query_scale = lax.rsqrt(jnp.mean(query_float * query_float, axis=-1, keepdims=True) + NORM_FLOOR)
    query_hat = (query_float * query_scale).astype(bf16)
    gate_open = jax.nn.sigmoid(gate_acc)

    gw4 = jnp.broadcast_to(gate_weight.reshape(4, 1, 512), (4, 16, 512))
    q_z, gate_z, wk_cols, wv_cols, gw_cols = comm(
        [ring("st_0", 2), ring("st_0"), a2a("tp"), a2a("tp"), a2a("tp")],
        [query_hat, rows_of(gate_open), key_weight.reshape(4, 512, 256), value_weight.reshape(4, 512, 256), gw4], 2)
    q_slots = q_z.reshape(48, 64, 256)[slot_block]
    q_here = lax.all_to_all(q_slots, YC, split_axis=0, concat_axis=0, tiled=True).reshape(64, 64, 256)
    gates = gate_z[:, :3].reshape(48, 64)[slot_block]
    side = jnp.concatenate([gates, jnp.broadcast_to(codes.T[:, :, None], (8, 8, 64)).astype(f32)], axis=-1)
    side_here = comm([a2a(*YC)], [side], 3)[0].reshape(64, 128)
    gate_here = side_here[:, :64]
    code_here = side_here[:, 64].astype(jnp.int32)
    used = code_here < 128
    loc = jnp.where(used, code_here // 8, 0)

    flat_rows = passages.reshape(1024, 2048)
    key_low = lax.optimization_barrier(
        jnp.dot(flat_rows, key_weight, preferred_element_type=f32).astype(bf16))
    value_all = jnp.dot(flat_rows, value_weight, preferred_element_type=f32).astype(bf16)
    key_float = key_low.astype(f32)
    key_scale = lax.rsqrt(jnp.mean(key_float * key_float, axis=-1, keepdims=True) + NORM_FLOOR)
    key_hat = (key_float * key_scale).astype(bf16)
    k_sel = key_hat.reshape(16, 64, 256)[loc]
    v_sel = value_all.reshape(16, 64, 256)[loc]

    scores = jnp.einsum("sid,sjd->sij", q_here, k_sel, preferred_element_type=f32) * scale
    exps = jnp.exp(scores)
    g_here = (gate_here[:, :, None] * cot_here.astype(f32)).astype(bf16)
    grad_probs = jnp.einsum("sid,sjd->sij", g_here, v_sel, preferred_element_type=f32)
    cot_dots = jnp.einsum("sid,sjd->sij", cot_here, v_sel, preferred_element_type=f32)
    sums = jnp.concatenate([jnp.sum(exps, axis=-1), jnp.sum(exps * grad_probs, axis=-1)], axis=-1)

    blk = jnp.where(codes < 128, codes % 8, 7)
    mask = (blk.T[:, None, :] == jnp.arange(6, dtype=jnp.int32)[None, :, None]).astype(f32)
    mask = jnp.broadcast_to(mask[..., None], (8, 6, 8, 128))
    whole, wq_cols = stats_exchange(sums.reshape(8, 8, 128), mask, query_weight.reshape(4, 512, 256), 4)
    whole = whole.reshape(64, 128)
    total = jnp.where(used[:, None], whole[:, :64], 1.0)
    inner = jnp.where(used[:, None], whole[:, 64:], 0.0) / total
    probs = jnp.where(used[:, None, None], exps, 0.0) / total[:, :, None]
    probs_low = probs.astype(bf16)
    score_grad = (probs * (grad_probs - inner[:, :, None])).astype(bf16)
    q_part = (scale * jnp.einsum("sij,sjd->sid", score_grad, k_sel, preferred_element_type=f32)).astype(bf16)
    q_part = jnp.moveaxis(q_part.reshape(8, 8, 64, 256), 0, 1).reshape(64, 64, 256)
    q_back = lax.all_to_all(q_part, ST, split_axis=0, concat_axis=0, tiled=True)
    dots = jnp.sum(probs_low.astype(f32) * cot_dots, axis=-1)
    dots = jnp.pad(dots, ((0, 0), (0, 64))).reshape(8, 8, 128)
    dots_back = dots_exchange(dots, mask, 5)

    key_term = (scale * jnp.einsum("sij,sid->sjd", score_grad, q_here, preferred_element_type=f32)).astype(bf16)
    value_term = jnp.einsum("sij,sid->sjd", probs_low, g_here, preferred_element_type=f32).astype(bf16)
    onehot = ((loc[None, :] == jnp.arange(16, dtype=jnp.int32)[:, None]) & used[None, :]).astype(bf16)
    key_grad_hat = jnp.dot(onehot, key_term.reshape(64, -1), preferred_element_type=f32).reshape(1024, 256)
    value_grad = jnp.dot(onehot, value_term.reshape(64, -1), preferred_element_type=f32).reshape(1024, 256)
    key_grad = (
        key_scale * key_grad_hat
        - key_scale**3 * key_float * jnp.mean(key_float * key_grad_hat, axis=-1, keepdims=True)
    ).astype(bf16)
    value_grad_low = value_grad.astype(bf16)
    weight_term = lax.dot_general(flat_rows, key_grad, CONTRACT_FIRST, preferred_element_type=f32)
    weight_term = jnp.transpose(weight_term.reshape(8, 4, 2, 32, 256), (2, 1, 0, 3, 4)).reshape(2, 1024, 256)
    vg4, w_c = comm([ring("tp", 2), a2a("st_2")], [value_grad_low, weight_term], 6)
    kg4, w_y = comm([ring("tp", 2), a2a("st_1")], [key_grad, (w_c[0] + w_c[1]).reshape(4, 256, 256)], 7)
    w_y = (w_y[0] + w_y[1]) + (w_y[2] + w_y[3])
    row_part = (
        jnp.einsum("hrd,hed->hre", kg4, wk_cols, preferred_element_type=f32)
        + jnp.einsum("hrd,hed->hre", vg4, wv_cols, preferred_element_type=f32)
    ).astype(bf16)
    passage_grad = jnp.sum(row_part.astype(f32), axis=0).astype(bf16).reshape(16, 64, 512)

    mixer_out = mixer_output(mix_query, mix_key, mix_value, beta_pre, decay_pre, decay_rate)
    qhat_grad = jnp.sum(q_back[owner].astype(f32).reshape(6, 4, 64, 256), axis=1).reshape(384, 256)
    read_dot = jnp.sum(dots_back, axis=0)[:6, :64].reshape(384)
    grad_out = cotangent.astype(f32)
    gate_grad = (read_dot - jnp.sum(grad_out * mixer_out, axis=-1)) * gate_open * (1.0 - gate_open)
    query_grad = (
        query_scale * qhat_grad
        - query_scale**3 * query_float * jnp.mean(query_float * qhat_grad, axis=-1, keepdims=True)
    ).astype(bf16)
    qg4, gg4, w_z = comm(
        [ring("tp"), ring("tp"), a2a("st_0")], [query_grad, rows_of(gate_grad), w_y.reshape(8, 32, 256)], 8)
    gg4 = gg4[:, :3].reshape(4, 384)
    token_part = (
        jnp.einsum("htd,hed->hte", qg4, wq_cols, preferred_element_type=f32)
        + gg4[:, :, None] * gw_cols[:, 0].astype(f32)[:, None, :]
    ).astype(bf16)
    token_grad = jnp.sum(token_part.astype(f32), axis=0).astype(bf16)
    key_weight_grad = jnp.sum(w_z, axis=0)
    return token_grad, passage_grad, key_weight_grad


def solution(mesh):
    torus = Mesh(mesh.devices.reshape(8, 4, 2, mesh.shape["tp"]), ("st_0", "st_1", "st_2", "tp"))
    return jax.shard_map(
        body,
        mesh=torus,
        in_specs=(
            P(ST, "tp"),
            P(ST, "tp"),
            P(ST, "tp"),
            P(ST, "tp"),
            P(ST, "tp"),
            P("tp", ST),
            P("tp", ST),
            P("tp"),
            P(ST, None, None),
            P(ST, None),
            P(None, "tp"),
            P(None, "tp"),
            P(None, "tp"),
            P("tp", None),
        ),
        out_specs=(P(ST, "tp"), P(ST, None, "tp"), P(ST, "tp")),
        check_vma=False,
    )
```

```python
import functools

import jax
import jax.numpy as jnp
from jax import lax
from jax.experimental import pallas as pl
from jax.experimental.pallas import tpu as pltpu
from jax.sharding import Mesh
from jax.sharding import PartitionSpec as P

SPAN = 64
ST = ("st_0", "st_1", "st_2")


NORM_FLOOR = 1.0
SCORE_GAIN = 4.0
CONTRACT_LAST = (((1,), (1,)), ((), ()))
CONTRACT_FIRST = (((0,), (0,)), ((), ()))


AXES = {"st_0": 8, "st_1": 4, "st_2": 2, "tp": 4}
MESH_ID = pl.DeviceIdType.MESH


def ring_starts(job, x_ref, o_ref, sems):
    axis, n, chunks = job["axis"], AXES[job["axis"]], job.get("chunks", 1)
    rows = x_ref.shape[0]
    me = lax.axis_index(axis)
    step_rows = rows // chunks

    def part(k, d, ch):
        lo, size = ch * step_rows, step_rows
        if k == n // 2 - 1:
            size = step_rows // 2
            lo = lo + (size if d else 0)
        return pl.ds(lo, size)

    def copy(k, d, ch):
        sgn = -1 if d else 1
        origin = lax.rem(me - sgn * k + 2 * n, n)
        rng = part(k, d, ch)
        src = x_ref.at[rng] if k == 0 else o_ref.at[origin, rng]
        return pltpu.make_async_remote_copy(
            src_ref=src, dst_ref=o_ref.at[origin, rng],
            send_sem=sems.at[0, d, k * chunks + ch], recv_sem=sems.at[1, d, k * chunks + ch],
            device_id={axis: lax.rem(me + sgn + n, n)}, device_id_type=MESH_ID)

    def arrival(k, d, ch):
        sgn = -1 if d else 1
        origin = lax.rem(me - sgn * (k + 1) + 2 * n, n)
        rng = part(k, d, ch)
        return pltpu.make_async_remote_copy(
            src_ref=o_ref.at[origin, rng], dst_ref=o_ref.at[origin, rng],
            send_sem=sems.at[0, d, k * chunks + ch], recv_sem=sems.at[1, d, k * chunks + ch],
            device_id={axis: lax.rem(me + sgn + n, n)}, device_id_type=MESH_ID)

    return copy, arrival, n // 2, chunks


def ring_peers(job):
    axis, n = job["axis"], AXES[job["axis"]]
    me = lax.axis_index(axis)
    return [{axis: lax.rem(me + 1, n)}, {axis: lax.rem(me + n - 1, n)}]


def shifts_of(axes):
    out = [()]
    for a in axes:
        out = [s + (d,) for s in out for d in range(AXES[a])]
    return [s for s in out if any(s)]


def index_of(axes, shift, sign):
    idx, dev = 0, {}
    for a, d in zip(axes, shift):
        n = AXES[a]
        c = lax.rem(lax.axis_index(a) + sign * d + n, n)
        dev[a] = c
        idx = idx * n + c
    return idx, dev


def a2a_copies(job, x_ref, o_ref, sems):
    axes = job["axes"]
    my_idx, _ = index_of(axes, (0,) * len(axes), 1)
    out = []
    for i, s in enumerate(shifts_of(axes)):
        dst_i, dst_d = index_of(axes, s, 1)
        src_i, _ = index_of(axes, s, -1)
        send = pltpu.make_async_remote_copy(
            src_ref=x_ref.at[dst_i], dst_ref=o_ref.at[my_idx], send_sem=sems.at[0, i],
            recv_sem=sems.at[1, i], device_id=dst_d, device_id_type=MESH_ID)
        recv = pltpu.make_async_remote_copy(
            src_ref=o_ref.at[src_i], dst_ref=o_ref.at[src_i], send_sem=sems.at[0, i],
            recv_sem=sems.at[1, i], device_id=dst_d, device_id_type=MESH_ID)
        out.append((send, recv))
    return my_idx, out


def a2a_peers(job):
    return [index_of(job["axes"], s, 1)[1] for s in shifts_of(job["axes"])]


def comm_kernel(jobs, *refs):
    nj = len(jobs)
    xs, os_, sems = refs[:nj], refs[nj:2 * nj], refs[2 * nj:]
    barrier = pltpu.get_barrier_semaphore()
    peers = []
    for job in jobs:
        peers += ring_peers(job) if job["kind"] == "ring" else a2a_peers(job)
    for p in peers:
        pl.semaphore_signal(barrier, inc=1, device_id=p, device_id_type=MESH_ID)
    pl.semaphore_wait(barrier, len(peers))
    rings, alls, sent = [], [], []
    for job, x, o, s in zip(jobs, xs, os_, sems):
        if job["kind"] == "ring":
            rings.append(ring_starts(job, x, o, s))
            c, a, steps, chunks = rings[-1]
            for ch in range(chunks):
                for d in range(2):
                    cp = c(0, d, ch); cp.start(); sent.append(cp)
    for job, x, o, s in zip(jobs, xs, os_, sems):
        if job["kind"] == "a2a":
            mine, cps = a2a_copies(job, x, o, s)
            for cp, _ in cps:
                cp.start(); sent.append(cp)
            alls.append((cps, mine, x, o))
            o[mine] = x[mine]
    for job, x, o in zip(jobs, xs, os_):
        if job["kind"] == "ring":
            o[lax.axis_index(job["axis"])] = x[...]
    for k in range(max([r[2] for r in rings], default=0)):
        for c, a, steps, chunks in rings:
            if k < steps:
                for ch in range(chunks):
                    for d in range(2):
                        a(k, d, ch).wait_recv()
                        if k + 1 < steps:
                            cp = c(k + 1, d, ch); cp.start(); sent.append(cp)
    for cps, *_ in alls:
        for _, r in cps:
            r.wait_recv()
    for cp in sent:
        cp.wait_send()


def comm(jobs, xs, cid):
    outs, sems = [], []
    for job, x in zip(jobs, xs):
        if job["kind"] == "ring":
            n = AXES[job["axis"]]
            outs.append(jax.ShapeDtypeStruct((n, *x.shape), x.dtype))
            sems.append(pltpu.SemaphoreType.DMA((2, 2, n // 2 * job.get("chunks", 1))))
        else:
            outs.append(jax.ShapeDtypeStruct(x.shape, x.dtype))
            sems.append(pltpu.SemaphoreType.DMA((2, len(shifts_of(job["axes"])))))
    return pl.pallas_call(
        functools.partial(comm_kernel, jobs),
        out_shape=outs,
        in_specs=[pl.BlockSpec(memory_space=pltpu.VMEM)] * len(xs),
        out_specs=[pl.BlockSpec(memory_space=pltpu.VMEM)] * len(xs),
        scratch_shapes=sems,
        compiler_params=pltpu.CompilerParams(collective_id=cid, has_side_effects=True),
    )(*xs)


SHIFTS = [(0, 1), (1, 0), (1, 1), (2, 0), (2, 1), (3, 0), (3, 1)]
YC = ("st_1", "st_2")


def near_ring(axis, own, right, left, far, sems, chunks):
    n = AXES[axis]
    me = lax.axis_index(axis)
    size = own.shape[0] // chunks

    def copy(k, d, ch):
        sgn = -1 if d else 1
        line = left if d else right
        last = k == n // 2 - 1
        lo, width = ch * size, size
        if last:
            width = size // 2
            lo = lo + (width if d else 0)
        rng = pl.ds(lo, width)
        src = own if k == 0 else line[k - 1]
        dst = far if last else line[k]
        return pltpu.make_async_remote_copy(
            src_ref=src.at[rng], dst_ref=dst.at[rng],
            send_sem=sems.at[0, d, k * chunks + ch], recv_sem=sems.at[1, d, k * chunks + ch],
            device_id={axis: lax.rem(me + sgn + n, n)}, device_id_type=MESH_ID)

    def start(k, sent):
        for ch in range(chunks):
            for d in range(2):
                cp = copy(k, d, ch)
                cp.start()
                sent.append(cp)

    def take(k, sent):
        for ch in range(chunks):
            for d in range(2):
                copy(k, d, ch).wait_recv()
                if k + 1 < n // 2:
                    cp = copy(k + 1, d, ch)
                    cp.start()
                    sent.append(cp)

    return start, take


def low_dot(a, b, dims=(((1,), (0,)), ((), ()))):
    return lax.dot_general(
        a.astype(jnp.bfloat16), b.astype(jnp.bfloat16), dims, preferred_element_type=jnp.float32)


def mixer_pieces(mq, mk, mv, st, ld, fresh, corr, attend, qdec, kdec, cdec, state, mixed):
    f32 = jnp.float32
    row_i = lax.broadcasted_iota(jnp.int32, (64, 64), 0)
    col_i = lax.broadcasted_iota(jnp.int32, (64, 64), 1)

    def prepare(m, n):
        def run():
            i = m * 6 + n
            rows, cols = pl.ds(n * 64, 64), pl.ds(m * 128, 128)
            q = mq[rows, cols].astype(f32)
            k = mk[rows, cols].astype(f32)
            v = mv[rows, cols].astype(f32)
            q = q * lax.rsqrt(jnp.sum(q * q, axis=-1, keepdims=True) + NORM_FLOOR) * 128 ** (-0.5)
            k = k * lax.rsqrt(jnp.sum(k * k, axis=-1, keepdims=True) + NORM_FLOOR)
            ld_row = jnp.broadcast_to(ld[i:i + 1, :], (64, 64))
            st_row = jnp.broadcast_to(st[i:i + 1, :], (64, 64))
            ld_col = jnp.sum(jnp.where(row_i == col_i, ld_row, 0.0), axis=1, keepdims=True)
            st_col = jnp.sum(jnp.where(row_i == col_i, st_row, 0.0), axis=1, keepdims=True)
            cum_col = jnp.sum(jnp.where(col_i <= row_i, ld_row, 0.0), axis=1, keepdims=True)
            cum_row = jnp.sum(jnp.where(row_i <= col_i, jnp.broadcast_to(ld_col, (64, 64)), 0.0), axis=0, keepdims=True)
            whole = jnp.sum(ld_col, axis=0, keepdims=True)
            decay = jnp.where(row_i >= col_i, jnp.exp(jnp.minimum(cum_col - cum_row, 0.0)), 0.0)
            gram = low_dot(k, k, CONTRACT_LAST)
            strict = jnp.where(row_i > col_i, st_col * gram * decay, 0.0)
            eye = jnp.where(row_i == col_i, 1.0, 0.0)
            running = eye - strict
            power = strict
            for _ in range(5):
                power = low_dot(power, power)
                running = low_dot(running, eye + power)
            grow = jnp.exp(cum_col)
            fresh[i] = low_dot(running, v * st_col)
            corr[i] = low_dot(running, k * (st_col * grow)).astype(jnp.bfloat16)
            attend[i] = (low_dot(q, k, CONTRACT_LAST) * decay).astype(jnp.bfloat16)
            qdec[i] = (q * grow).astype(jnp.bfloat16)
            kdec[i] = (k * jnp.exp(whole - cum_col)).astype(jnp.bfloat16)
            cdec[i] = jnp.broadcast_to(jnp.exp(whole), (8, 128))
        return run

    def advance(n):
        def run():
            for m in range(2):
                i = m * 6 + n
                rows, cols = pl.ds(n * 64, 64), pl.ds(m * 128, 128)
                if n == 0:
                    new = fresh[i]
                    mixed[rows, cols] = low_dot(attend[i], new)
                    state[m] = low_dot(kdec[i], new, CONTRACT_FIRST)
                else:
                    held = state[m]
                    new = fresh[i] - low_dot(corr[i], held)
                    mixed[rows, cols] = low_dot(qdec[i], held) + low_dot(attend[i], new)
                    if n < 5:
                        state[m] = held * cdec[i][0:1, :] + low_dot(kdec[i], new, CONTRACT_FIRST)
        return run

    return [prepare(m, n) for n in range(6) for m in range(2)], [advance(n) for n in range(6)]


def quarters(rows_ref, rows, w):
    acc = None
    for p in range(4):
        term = jnp.dot(rows_ref[rows, p * 512:(p + 1) * 512], w[p], preferred_element_type=jnp.float32)
        acc = term if acc is None else acc + term
    return acc


def forward_kernel(
    tok, cot, tab, tab_s, wq, gw, pas, wk, wv, mq, mk, mv, st, ld,
    cot_o, q_o, gate_o, code_o, tabs_o, qlow, gate, klow, vlow, mixed, wkc, wvc, wqc, gwc,
    t_r, t_l, t_f, c_r, c_l, c_f, q_own, q_r, q_l, q_f, g_r, g_l, g_f, b_r, b_l, b_f, tsm,
    cst, qst, gst, codest, fresh, corr, attend, qdec, kdec, cdec, state,
    s_t, s_c, s_q, s_g, s_b, s_m, s_cy, s_qy, s_gy, s_by, s_w0, s_w1, s_w2, s_w3,
):
    f32, bf16 = jnp.float32, jnp.bfloat16
    z = lax.axis_index("st_0")
    x = lax.axis_index("tp")
    jobs = [ring_peers(dict(axis="tp")), ring_peers(dict(axis="st_0")), a2a_peers(dict(axes=YC)),
            a2a_peers(dict(axes=("tp",)))]
    barrier = pltpu.get_barrier_semaphore()
    peers = [p for job in jobs for p in job]
    for p in peers:
        pl.semaphore_signal(barrier, inc=1, device_id=p, device_id_type=MESH_ID)
    pl.semaphore_wait(barrier, len(peers))
    sent = []
    b_start, b_take = near_ring("st_0", tab, b_r, b_l, b_f, s_b, 1)
    c_start, c_take = near_ring("st_0", cot, c_r, c_l, c_f, s_c, 3)
    t_start, t_take = near_ring("tp", tok, [t_r], [t_l], t_f, s_t, 3)
    q_start, q_take = near_ring("st_0", q_own, q_r, q_l, q_f, s_q, 3)
    g_start, g_take = near_ring("st_0", gate, g_r, g_l, g_f, s_g, 1)
    b_start(0, sent)
    t_start(0, sent)
    c_start(0, sent)

    my_yc, _ = index_of(YC, (0, 0), 1)
    dsts = [index_of(YC, s, 1) for s in SHIFTS]
    srcs = [index_of(YC, s, -1)[0] for s in SHIFTS]
    tabs = [None] + list(b_r) + list(b_l) + [b_f]
    origins = [lax.rem(z - d + 8, 8) for d in (0, 1, 2, 3, -1, -2, -3, 4)]

    def table_copy(i):
        return pltpu.make_async_copy(tabs[i].at[0], tsm.at[i - 1], s_m.at[i - 1])

    def block_for(i, j):
        code = tab_s[z, j] if i == 0 else tsm[i - 1, z, j]
        return lax.rem(code, 8)

    def push(i, buf, stage, out, sems):
        zr = origins[i]
        for s in range(7):
            stage[s, zr] = buf[block_for(i, dsts[s][0])]
        out[my_yc, zr] = buf[block_for(i, my_yc)]
        for s in range(7):
            cp = pltpu.make_async_remote_copy(
                src_ref=stage.at[s, zr], dst_ref=out.at[my_yc, zr], send_sem=sems.at[0, i, s],
                recv_sem=sems.at[1, i, s], device_id=dsts[s][1], device_id_type=MESH_ID)
            cp.start()
            sent.append(cp)

    def pulled(out, sems):
        for i in range(8):
            for s in range(7):
                pltpu.make_async_remote_copy(
                    src_ref=out.at[srcs[s], origins[i]], dst_ref=out.at[srcs[s], origins[i]],
                    send_sem=sems.at[0, i, s], recv_sem=sems.at[1, i, s], device_id=dsts[s][1],
                    device_id_type=MESH_ID).wait_recv()

    cots = [cot] + list(c_r) + list(c_l) + [c_f]
    qs = [q_own] + list(q_r) + list(q_l) + [q_f]
    gs = [gate] + list(g_r) + list(g_l) + [g_f]

    def project(t):
        def run():
            rows = pl.ds(t * 256, 256)
            klow[rows, :] = quarters(pas, rows, wk).astype(bf16)
            vlow[rows, :] = quarters(pas, rows, wv).astype(bf16)
        return run

    prep, scan = mixer_pieces(mq, mk, mv, st, ld, fresh, corr, attend, qdec, kdec, cdec, state, mixed)
    work = [project(t) for t in range(4)] + prep + scan
    work.reverse()

    def fill(count):
        for _ in range(count):
            if work:
                work.pop()()

    push(0, cot, cst, cot_o, s_cy)
    fill(2)
    b_take(0, sent)
    table_copy(1).start()
    table_copy(4).start()
    t_take(0, sent)
    c_take(0, sent)
    fill(1)
    for i in (1, 4):
        table_copy(i).wait()
        push(i, cots[i], cst, cot_o, s_cy)
    b_take(1, sent)
    table_copy(2).start()
    table_copy(5).start()
    c_take(1, sent)
    fill(1)
    for i in (2, 5):
        table_copy(i).wait()
        push(i, cots[i], cst, cot_o, s_cy)
    t_take(1, sent)

    parts = [(tok, x), (t_r, lax.rem(x + 3, 4)), (t_l, lax.rem(x + 1, 4)), (t_f, lax.rem(x + 2, 4))]
    for half in range(2):
        acc = None
        for buf, p in parts:
            rows = buf[half * 3:half * 3 + 3].reshape(192, 512)
            term = jnp.dot(rows, wq[p], preferred_element_type=f32)
            acc = term if acc is None else acc + term
        low = acc.astype(bf16)
        qlow[half * 192:half * 192 + 192, :] = low
        wide = low.astype(f32)
        norm = lax.rsqrt(jnp.mean(wide * wide, axis=-1, keepdims=True) + NORM_FLOOR)
        q_own[half * 3:half * 3 + 3] = (wide * norm).astype(bf16).reshape(3, 64, 256)
    for b in range(6):
        acc = None
        for buf, p in parts:
            term = lax.dot_general(gw[p], buf[b], CONTRACT_LAST, preferred_element_type=f32)
            acc = term if acc is None else acc + term
        gate[b, :, 0:64] = jax.nn.sigmoid(acc[0:8])
        gate[b, :, 64:128] = jnp.zeros((8, 64), f32)
    g_start(0, sent)
    q_start(0, sent)
    wcp = []
    for src, dst, sem in ((gw, gwc, s_w3), (wk, wkc, s_w0), (wv, wvc, s_w1), (wq, wqc, s_w2)):
        mine, cps = a2a_copies(dict(axes=("tp",)), src, dst, sem)
        for cp, _ in cps:
            cp.start()
            sent.append(cp)
        dst[mine] = src[mine]
        wcp += cps

    b_take(2, sent)
    table_copy(3).start()
    table_copy(6).start()
    c_take(2, sent)
    fill(1)
    for i in (3, 6):
        table_copy(i).wait()
        push(i, cots[i], cst, cot_o, s_cy)
    b_take(3, sent)
    table_copy(7).start()
    c_take(3, sent)
    push(0, q_own, qst, q_o, s_qy)
    fill(1)
    table_copy(7).wait()
    push(7, c_f, cst, cot_o, s_cy)
    g_take(0, sent)
    q_take(0, sent)
    for i in (1, 4):
        push(i, qs[i], qst, q_o, s_qy)
    fill(5)
    g_take(1, sent)
    q_take(1, sent)
    for i in (2, 5):
        push(i, qs[i], qst, q_o, s_qy)
    fill(5)
    g_take(2, sent)
    q_take(2, sent)
    for i in (3, 6):
        push(i, qs[i], qst, q_o, s_qy)
    fill(3)
    g_take(3, sent)
    q_take(3, sent)
    push(7, q_f, qst, q_o, s_qy)
    for i in range(8):
        zr = origins[i]
        table = tab if i == 0 else tabs[i]
        row = table[0, pl.ds(z, 1), :]
        codest[zr] = jnp.broadcast_to(row, (8, 128))
        tabs_o[zr] = jnp.broadcast_to(row, (8, 128))
        code_o[my_yc, zr] = jnp.broadcast_to(row, (8, 128))
        for s in range(7):
            gst[s, zr] = gs[i][block_for(i, dsts[s][0])]
        gate_o[my_yc, zr] = gs[i][block_for(i, my_yc)]
    side = []
    for s in range(7):
        for src, dst, sems in ((codest, code_o, s_by), (gst.at[s], gate_o, s_gy)):
            cp = pltpu.make_async_remote_copy(
                src_ref=src, dst_ref=dst.at[my_yc], send_sem=sems.at[0, s], recv_sem=sems.at[1, s],
                device_id=dsts[s][1], device_id_type=MESH_ID)
            cp.start()
            sent.append(cp)
            side.append(pltpu.make_async_remote_copy(
                src_ref=src, dst_ref=dst.at[srcs[s]], send_sem=sems.at[0, s], recv_sem=sems.at[1, s],
                device_id=dsts[s][1], device_id_type=MESH_ID))
    fill(99)
    for r in side:
        r.wait_recv()
    for _, r in wcp:
        r.wait_recv()
    pulled(cot_o, s_cy)
    pulled(q_o, s_qy)
    for cp in sent:
        cp.wait_send()


def forward(ins, cid):
    v = pl.BlockSpec(memory_space=pltpu.VMEM)
    f32, bf16, i32 = jnp.float32, jnp.bfloat16, jnp.int32
    sds = jax.ShapeDtypeStruct
    dma = pltpu.SemaphoreType.DMA
    slots = sds((8, 8, 64, 256), bf16)
    wide = sds((4, 512, 256), bf16)
    return pl.pallas_call(
        forward_kernel,
        out_shape=[
            slots, slots, sds((8, 8, 8, 128), f32), sds((8, 8, 8, 128), i32), sds((8, 8, 128), i32),
            sds((384, 256), bf16), sds((6, 8, 128), f32), sds((1024, 256), bf16), sds((1024, 256), bf16),
            sds((384, 256), f32), wide, wide, wide, sds((4, 16, 512), bf16)],
        in_specs=[v, v, v, pl.BlockSpec(memory_space=pltpu.SMEM)] + [v] * 10,
        out_specs=[v] * 14,
        scratch_shapes=[
            pltpu.VMEM((6, 64, 512), bf16), pltpu.VMEM((6, 64, 512), bf16), pltpu.VMEM((6, 64, 512), bf16),
            [pltpu.VMEM((6, 64, 256), bf16)] * 3, [pltpu.VMEM((6, 64, 256), bf16)] * 3, pltpu.VMEM((6, 64, 256), bf16),
            pltpu.VMEM((6, 64, 256), bf16),
            [pltpu.VMEM((6, 64, 256), bf16)] * 3, [pltpu.VMEM((6, 64, 256), bf16)] * 3, pltpu.VMEM((6, 64, 256), bf16),
            [pltpu.VMEM((6, 8, 128), f32)] * 3, [pltpu.VMEM((6, 8, 128), f32)] * 3, pltpu.VMEM((6, 8, 128), f32),
            [pltpu.VMEM((2, 8, 128), i32)] * 3, [pltpu.VMEM((2, 8, 128), i32)] * 3, pltpu.VMEM((2, 8, 128), i32),
            pltpu.SMEM((7, 8, 128), i32),
            pltpu.VMEM((7, 8, 64, 256), bf16), pltpu.VMEM((7, 8, 64, 256), bf16), pltpu.VMEM((7, 8, 8, 128), f32),
            pltpu.VMEM((8, 8, 128), i32),
            pltpu.VMEM((12, 64, 128), f32), pltpu.VMEM((12, 64, 128), bf16), pltpu.VMEM((12, 64, 64), bf16),
            pltpu.VMEM((12, 64, 128), bf16), pltpu.VMEM((12, 64, 128), bf16), pltpu.VMEM((12, 8, 128), f32),
            pltpu.VMEM((2, 128, 128), f32),
            dma((2, 2, 6)), dma((2, 2, 12)), dma((2, 2, 12)), dma((2, 2, 4)), dma((2, 2, 4)), dma((7,)),
            dma((2, 8, 7)), dma((2, 8, 7)), dma((2, 7)), dma((2, 7)),
            dma((2, 3)), dma((2, 3)), dma((2, 3)), dma((2, 3))],
        compiler_params=pltpu.CompilerParams(
            collective_id=cid, has_side_effects=True, vmem_limit_bytes=60 * 1024 * 1024),
    )(*ins)


def ring(axis, chunks=1):
    return dict(kind="ring", axis=axis, chunks=chunks)


def a2a(*axes):
    return dict(kind="a2a", axes=axes)


def rows_of(vec):
    flat = vec.reshape(-1, 128)
    return jnp.pad(flat, ((0, 16 - flat.shape[0]), (0, 0)))


def stats_kernel(x_ref, m_ref, o_ref, whole, got, tot, every, back, s1, s2, s3):
    job = a2a(*YC)
    barrier = pltpu.get_barrier_semaphore()
    peers = a2a_peers(job) + a2a_peers(a2a("st_0"))
    for p in peers:
        pl.semaphore_signal(barrier, inc=1, device_id=p, device_id_type=MESH_ID)
    pl.semaphore_wait(barrier, len(peers))
    sent = []
    mine, cps = a2a_copies(job, x_ref, got, s1)
    for cp, _ in cps:
        cp.start()
        sent.append(cp)
    got[mine] = x_ref[mine]
    for _, r in cps:
        r.wait_recv()
    for b in range(6):
        acc = got[0] * m_ref[0, b]
        for j in range(1, 8):
            acc = acc + got[j] * m_ref[j, b]
        tot[b] = acc
    z = lax.axis_index("st_0")
    arrivals = []
    for s in range(1, 8):
        dst = lax.rem(z + s, 8)
        src = lax.rem(z - s + 8, 8)
        cp = pltpu.make_async_remote_copy(
            src_ref=tot, dst_ref=every.at[z], send_sem=s2.at[0, s], recv_sem=s2.at[1, s],
            device_id={"st_0": dst}, device_id_type=MESH_ID)
        rv = pltpu.make_async_remote_copy(
            src_ref=tot, dst_ref=every.at[src], send_sem=s2.at[0, s], recv_sem=s2.at[1, s],
            device_id={"st_0": dst}, device_id_type=MESH_ID)
        cp.start()
        sent.append(cp)
        arrivals.append(rv)
    every[z] = tot[...]
    for rv in arrivals:
        rv.wait_recv()
    for b in range(6):
        acc = every[0, b]
        for k in range(1, 8):
            acc = acc + every[k, b]
        whole[b] = acc
    for j in range(8):
        acc = whole[0] * m_ref[j, 0]
        for b in range(1, 6):
            acc = acc + whole[b] * m_ref[j, b]
        back[j] = acc
    mine, cps3 = a2a_copies(job, back, o_ref, s3)
    for cp, _ in cps3:
        cp.start()
        sent.append(cp)
    o_ref[mine] = back[mine]
    for _, r in cps3:
        r.wait_recv()
    for cp in sent:
        cp.wait_send()


def stats_exchange(x, mask, cid):
    v = pl.BlockSpec(memory_space=pltpu.VMEM)
    f = jnp.float32
    return pl.pallas_call(
        stats_kernel,
        out_shape=[jax.ShapeDtypeStruct(x.shape, f), jax.ShapeDtypeStruct((6, 8, 256), f)],
        in_specs=[v] * 2,
        out_specs=[v] * 2,
        scratch_shapes=[
            pltpu.VMEM((8, 8, 256), f), pltpu.VMEM((6, 8, 256), f), pltpu.VMEM((8, 6, 8, 256), f),
            pltpu.VMEM((8, 8, 256), f), pltpu.SemaphoreType.DMA((2, 7)), pltpu.SemaphoreType.DMA((2, 8)),
            pltpu.SemaphoreType.DMA((2, 7))],
        compiler_params=pltpu.CompilerParams(collective_id=cid, has_side_effects=True),
    )(x, mask)


def tail_kernel(kg, vg, w, kg_o, vg_o, w_o, wc, wcs, wy, wys, wz, s_k, s_v, s_c, s_y, s_z):
    barrier = pltpu.get_barrier_semaphore()
    peers = ring_peers(ring("tp")) + a2a_peers(a2a("st_2")) + a2a_peers(a2a("st_1")) + a2a_peers(a2a("st_0"))
    for p in peers:
        pl.semaphore_signal(barrier, inc=1, device_id=p, device_id_type=MESH_ID)
    pl.semaphore_wait(barrier, len(peers))
    sent = []
    rings = []
    for src, dst, sems in ((kg, kg_o, s_k), (vg, vg_o, s_v)):
        c, a, steps, chunks = ring_starts(ring("tp", 2), src, dst, sems)
        rings.append((c, a))
        for ch in range(2):
            for d in range(2):
                cp = c(0, d, ch)
                cp.start()
                sent.append(cp)
    core = lax.axis_index("st_2")
    pair = pltpu.make_async_remote_copy(
        src_ref=w.at[1 - core], dst_ref=wc, send_sem=s_c.at[0], recv_sem=s_c.at[1],
        device_id={"st_2": 1 - core}, device_id_type=MESH_ID)
    pair.start()
    sent.append(pair)
    x = lax.axis_index("tp")
    kg_o[x] = kg[...]
    vg_o[x] = vg[...]
    pair.wait_recv()
    for y in range(4):
        wcs[y] = w[core, y] + wc[y]
    ym, ycp = a2a_copies(a2a("st_1"), wcs, wy, s_y)
    for cp, _ in ycp:
        cp.start()
        sent.append(cp)
    wy[ym] = wcs[ym]
    for c, a in rings:
        for ch in range(2):
            for d in range(2):
                a(0, d, ch).wait_recv()
                cp = c(1, d, ch)
                cp.start()
                sent.append(cp)
    for _, r in ycp:
        r.wait_recv()
    for k in range(8):
        wys[k] = (wy[0, k] + wy[1, k]) + (wy[2, k] + wy[3, k])
    zm, zcp = a2a_copies(a2a("st_0"), wys, wz, s_z)
    for cp, _ in zcp:
        cp.start()
        sent.append(cp)
    wz[zm] = wys[zm]
    for c, a in rings:
        for ch in range(2):
            for d in range(2):
                a(1, d, ch).wait_recv()
    for _, r in zcp:
        r.wait_recv()
    acc = wz[0]
    for k in range(1, 8):
        acc = acc + wz[k]
    w_o[...] = acc
    for cp in sent:
        cp.wait_send()


def tail(kg, vg, w, cid):
    v = pl.BlockSpec(memory_space=pltpu.VMEM)
    f32, bf16 = jnp.float32, jnp.bfloat16
    dma = pltpu.SemaphoreType.DMA
    return pl.pallas_call(
        tail_kernel,
        out_shape=[
            jax.ShapeDtypeStruct((4, 1024, 256), bf16), jax.ShapeDtypeStruct((4, 1024, 256), bf16),
            jax.ShapeDtypeStruct((32, 256), f32)],
        in_specs=[v] * 3,
        out_specs=[v] * 3,
        scratch_shapes=[
            pltpu.VMEM((4, 8, 32, 256), f32), pltpu.VMEM((4, 8, 32, 256), f32), pltpu.VMEM((4, 8, 32, 256), f32),
            pltpu.VMEM((8, 32, 256), f32), pltpu.VMEM((8, 32, 256), f32),
            dma((2, 2, 4)), dma((2, 2, 4)), dma((2,)), dma((2, 3)), dma((2, 7))],
        compiler_params=pltpu.CompilerParams(
            collective_id=cid, has_side_effects=True, vmem_limit_bytes=40 * 1024 * 1024),
    )(kg, vg, w)


def body(
    tokens, cotangent, mix_query, mix_key, mix_value, beta_pre, decay_pre, decay_rate,
    passages, passage_ids, query_weight, key_weight, value_weight, gate_weight,
):
    f32, bf16 = jnp.float32, jnp.bfloat16
    scale = SCORE_GAIN * 256 ** (-0.5)
    z = lax.axis_index("st_0")
    my_yc = lax.axis_index(YC)
    ids = passage_ids.reshape(24)
    owner, local = ids // 16, ids % 16
    match = owner[None, :] == jnp.arange(64, dtype=jnp.int32)[:, None]
    code_of = local * 8 + jnp.arange(24, dtype=jnp.int32) // 4
    code = jnp.sum(jnp.where(match, code_of[None, :], 0), axis=-1, dtype=jnp.int32)
    code = jnp.where(jnp.any(match, axis=-1), code, 128).reshape(8, 8)
    table = jnp.pad(code[None], ((0, 1), (0, 0), (0, 120)))
    gw4 = jnp.broadcast_to(gate_weight.reshape(4, 1, 512), (4, 16, 512))
    strength = jax.nn.sigmoid(beta_pre).reshape(12, 64)
    log_decay = (-decay_rate[:, None] * jax.nn.softplus(decay_pre)).reshape(12, 64)
    flat_rows = passages.reshape(1024, 2048)
    (cot_here, q_here, gate_o, code_o, tabs, query_low, gate6, key_low, value_all, mixer_out,
     wk_cols, wv_cols, wq_cols, gw_cols) = forward(
        [tokens.reshape(6, 64, 512), cotangent.reshape(6, 64, 256), table, code,
         query_weight.reshape(4, 512, 256), gw4, flat_rows, key_weight.reshape(4, 512, 256), value_weight.reshape(4, 512, 256),
         mix_query, mix_key, mix_value, strength, log_decay], 1)
    cot_here, q_here = cot_here.reshape(64, 64, 256), q_here.reshape(64, 64, 256)
    codes = tabs[:, 0, :8]
    gate_here = gate_o[:, :, 0, :64].reshape(64, 64)
    code_here = lax.dynamic_slice(code_o, (0, 0, 0, my_yc), (8, 8, 1, 1)).reshape(64)
    used = code_here < 128
    loc = jnp.where(used, code_here // 8, 0)
    gate_open = gate6[:, 0, :64].reshape(384)
    query_float = query_low.astype(f32)
    query_scale = lax.rsqrt(jnp.mean(query_float * query_float, axis=-1, keepdims=True) + NORM_FLOOR)

    key_float = key_low.astype(f32)
    key_scale = lax.rsqrt(jnp.mean(key_float * key_float, axis=-1, keepdims=True) + NORM_FLOOR)
    key_hat = (key_float * key_scale).astype(bf16)
    k_sel = key_hat.reshape(16, 64, 256)[loc]
    v_sel = value_all.reshape(16, 64, 256)[loc]

    scores = jnp.einsum("sid,sjd->sij", q_here, k_sel, preferred_element_type=f32) * scale
    exps = jnp.exp(scores)
    g_here = (gate_here[:, :, None] * cot_here.astype(f32)).astype(bf16)
    grad_probs = jnp.einsum("sid,sjd->sij", g_here, v_sel, preferred_element_type=f32)
    cot_dots = jnp.einsum("sid,sjd->sij", cot_here, v_sel, preferred_element_type=f32)
    sums = jnp.concatenate(
        [jnp.sum(exps, axis=-1), jnp.sum(exps * grad_probs, axis=-1), jnp.sum(exps * cot_dots, axis=-1),
         jnp.zeros((64, 64), f32)], axis=-1)

    blk = jnp.where(codes < 128, codes % 8, 7)
    mask = (blk.T[:, None, :] == jnp.arange(6, dtype=jnp.int32)[None, :, None]).astype(f32)
    mask = jnp.broadcast_to(mask[..., None], (8, 6, 8, 256))
    whole, mine = stats_exchange(sums.reshape(8, 8, 256), mask, 2)
    whole = whole.reshape(64, 256)
    mine = lax.dynamic_slice(mine, (0, z, 0), (6, 1, 256)).reshape(6, 256)
    read_dot = (mine[:, 128:192] / mine[:, :64]).reshape(384)
    total = jnp.where(used[:, None], whole[:, :64], 1.0)
    inner = jnp.where(used[:, None], whole[:, 64:128], 0.0) / total
    probs = jnp.where(used[:, None, None], exps, 0.0) / total[:, :, None]
    probs_low = probs.astype(bf16)
    score_grad = (probs * (grad_probs - inner[:, :, None])).astype(bf16)
    q_part = (scale * jnp.einsum("sij,sjd->sid", score_grad, k_sel, preferred_element_type=f32)).astype(bf16)
    q_part = jnp.moveaxis(q_part.reshape(8, 8, 64, 256), 0, 1).reshape(64, 64, 256)
    q_back = lax.all_to_all(q_part, ST, split_axis=0, concat_axis=0, tiled=True)

    key_term = (scale * jnp.einsum("sij,sid->sjd", score_grad, q_here, preferred_element_type=f32)).astype(bf16)
    value_term = jnp.einsum("sij,sid->sjd", probs_low, g_here, preferred_element_type=f32).astype(bf16)
    onehot = ((loc[None, :] == jnp.arange(16, dtype=jnp.int32)[:, None]) & used[None, :]).astype(bf16)
    key_grad_hat = jnp.dot(onehot, key_term.reshape(64, -1), preferred_element_type=f32).reshape(1024, 256)
    value_grad = jnp.dot(onehot, value_term.reshape(64, -1), preferred_element_type=f32).reshape(1024, 256)
    key_grad = (
        key_scale * key_grad_hat
        - key_scale**3 * key_float * jnp.mean(key_float * key_grad_hat, axis=-1, keepdims=True)
    ).astype(bf16)
    value_grad_low = value_grad.astype(bf16)
    weight_term = lax.dot_general(flat_rows, key_grad, CONTRACT_FIRST, preferred_element_type=f32)
    weight_term = jnp.transpose(weight_term.reshape(8, 4, 2, 32, 256), (2, 1, 0, 3, 4))
    kg4, vg4, key_weight_grad = tail(key_grad, value_grad_low, weight_term, 3)
    row_part = (
        jnp.einsum("hrd,hed->hre", kg4, wk_cols, preferred_element_type=f32)
        + jnp.einsum("hrd,hed->hre", vg4, wv_cols, preferred_element_type=f32)
    ).astype(bf16)
    passage_grad = jnp.sum(row_part.astype(f32), axis=0).astype(bf16).reshape(16, 64, 512)

    qhat_grad = jnp.sum(q_back[owner].astype(f32).reshape(6, 4, 64, 256), axis=1).reshape(384, 256)
    grad_out = cotangent.astype(f32)
    gate_grad = (read_dot - jnp.sum(grad_out * mixer_out, axis=-1)) * gate_open * (1.0 - gate_open)
    query_grad = (
        query_scale * qhat_grad
        - query_scale**3 * query_float * jnp.mean(query_float * qhat_grad, axis=-1, keepdims=True)
    ).astype(bf16)
    qg4, gg4 = comm([ring("tp"), ring("tp")], [query_grad, rows_of(gate_grad)], 4)
    gg4 = gg4[:, :3].reshape(4, 384)
    token_part = (
        jnp.einsum("htd,hed->hte", qg4, wq_cols, preferred_element_type=f32)
        + gg4[:, :, None] * gw_cols[:, 0].astype(f32)[:, None, :]
    ).astype(bf16)
    token_grad = jnp.sum(token_part.astype(f32), axis=0).astype(bf16)
    return token_grad, passage_grad, key_weight_grad


def solution(mesh):
    torus = Mesh(mesh.devices.reshape(8, 4, 2, mesh.shape["tp"]), ("st_0", "st_1", "st_2", "tp"))
    return jax.shard_map(
        body,
        mesh=torus,
        in_specs=(
            P(ST, "tp"),
            P(ST, "tp"),
            P(ST, "tp"),
            P(ST, "tp"),
            P(ST, "tp"),
            P("tp", ST),
            P("tp", ST),
            P("tp"),
            P(ST, None, None),
            P(ST, None),
            P(None, "tp"),
            P(None, "tp"),
            P(None, "tp"),
            P("tp", None),
        ),
        out_specs=(P(ST, "tp"), P(ST, None, "tp"), P(ST, "tp")),
        check_vma=False,
    )
```

```python
import functools

import jax
import jax.numpy as jnp
from jax import lax
from jax.experimental import pallas as pl
from jax.experimental.pallas import tpu as pltpu
from jax.sharding import Mesh
from jax.sharding import PartitionSpec as P

SPAN = 64
ST = ("st_0", "st_1", "st_2")


NORM_FLOOR = 1.0
SCORE_GAIN = 4.0
CONTRACT_LAST = (((1,), (1,)), ((), ()))
CONTRACT_FIRST = (((0,), (0,)), ((), ()))


AXES = {"st_0": 8, "st_1": 4, "st_2": 2, "tp": 4}
MESH_ID = pl.DeviceIdType.MESH


def ring_starts(job, x_ref, o_ref, sems):
    axis, n, chunks = job["axis"], AXES[job["axis"]], job.get("chunks", 1)
    rows = x_ref.shape[0]
    me = lax.axis_index(axis)
    step_rows = rows // chunks

    def part(k, d, ch):
        lo, size = ch * step_rows, step_rows
        if k == n // 2 - 1:
            size = step_rows // 2
            lo = lo + (size if d else 0)
        return pl.ds(lo, size)

    def copy(k, d, ch):
        sgn = -1 if d else 1
        origin = lax.rem(me - sgn * k + 2 * n, n)
        rng = part(k, d, ch)
        src = x_ref.at[rng] if k == 0 else o_ref.at[origin, rng]
        return pltpu.make_async_remote_copy(
            src_ref=src, dst_ref=o_ref.at[origin, rng],
            send_sem=sems.at[0, d, k * chunks + ch], recv_sem=sems.at[1, d, k * chunks + ch],
            device_id={axis: lax.rem(me + sgn + n, n)}, device_id_type=MESH_ID)

    def arrival(k, d, ch):
        sgn = -1 if d else 1
        origin = lax.rem(me - sgn * (k + 1) + 2 * n, n)
        rng = part(k, d, ch)
        return pltpu.make_async_remote_copy(
            src_ref=o_ref.at[origin, rng], dst_ref=o_ref.at[origin, rng],
            send_sem=sems.at[0, d, k * chunks + ch], recv_sem=sems.at[1, d, k * chunks + ch],
            device_id={axis: lax.rem(me + sgn + n, n)}, device_id_type=MESH_ID)

    return copy, arrival, n // 2, chunks


def ring_peers(job):
    axis, n = job["axis"], AXES[job["axis"]]
    me = lax.axis_index(axis)
    return [{axis: lax.rem(me + 1, n)}, {axis: lax.rem(me + n - 1, n)}]


def shifts_of(axes):
    out = [()]
    for a in axes:
        out = [s + (d,) for s in out for d in range(AXES[a])]
    return [s for s in out if any(s)]


def index_of(axes, shift, sign):
    idx, dev = 0, {}
    for a, d in zip(axes, shift):
        n = AXES[a]
        c = lax.rem(lax.axis_index(a) + sign * d + n, n)
        dev[a] = c
        idx = idx * n + c
    return idx, dev


def a2a_copies(job, x_ref, o_ref, sems):
    axes = job["axes"]
    my_idx, _ = index_of(axes, (0,) * len(axes), 1)
    out = []
    for i, s in enumerate(shifts_of(axes)):
        dst_i, dst_d = index_of(axes, s, 1)
        src_i, _ = index_of(axes, s, -1)
        send = pltpu.make_async_remote_copy(
            src_ref=x_ref.at[dst_i], dst_ref=o_ref.at[my_idx], send_sem=sems.at[0, i],
            recv_sem=sems.at[1, i], device_id=dst_d, device_id_type=MESH_ID)
        recv = pltpu.make_async_remote_copy(
            src_ref=o_ref.at[src_i], dst_ref=o_ref.at[src_i], send_sem=sems.at[0, i],
            recv_sem=sems.at[1, i], device_id=dst_d, device_id_type=MESH_ID)
        out.append((send, recv))
    return my_idx, out


def a2a_peers(job):
    return [index_of(job["axes"], s, 1)[1] for s in shifts_of(job["axes"])]


def comm_kernel(jobs, *refs):
    nj = len(jobs)
    xs, os_, sems = refs[:nj], refs[nj:2 * nj], refs[2 * nj:]
    barrier = pltpu.get_barrier_semaphore()
    peers = []
    for job in jobs:
        peers += ring_peers(job) if job["kind"] == "ring" else a2a_peers(job)
    for p in peers:
        pl.semaphore_signal(barrier, inc=1, device_id=p, device_id_type=MESH_ID)
    pl.semaphore_wait(barrier, len(peers))
    rings, alls, sent = [], [], []
    for job, x, o, s in zip(jobs, xs, os_, sems):
        if job["kind"] == "ring":
            rings.append(ring_starts(job, x, o, s))
            c, a, steps, chunks = rings[-1]
            for ch in range(chunks):
                for d in range(2):
                    cp = c(0, d, ch); cp.start(); sent.append(cp)
    for job, x, o, s in zip(jobs, xs, os_, sems):
        if job["kind"] == "a2a":
            mine, cps = a2a_copies(job, x, o, s)
            for cp, _ in cps:
                cp.start(); sent.append(cp)
            alls.append((cps, mine, x, o))
            o[mine] = x[mine]
    for job, x, o in zip(jobs, xs, os_):
        if job["kind"] == "ring":
            o[lax.axis_index(job["axis"])] = x[...]
    for k in range(max([r[2] for r in rings], default=0)):
        for c, a, steps, chunks in rings:
            if k < steps:
                for ch in range(chunks):
                    for d in range(2):
                        a(k, d, ch).wait_recv()
                        if k + 1 < steps:
                            cp = c(k + 1, d, ch); cp.start(); sent.append(cp)
    for cps, *_ in alls:
        for _, r in cps:
            r.wait_recv()
    for cp in sent:
        cp.wait_send()


def comm(jobs, xs, cid):
    outs, sems = [], []
    for job, x in zip(jobs, xs):
        if job["kind"] == "ring":
            n = AXES[job["axis"]]
            outs.append(jax.ShapeDtypeStruct((n, *x.shape), x.dtype))
            sems.append(pltpu.SemaphoreType.DMA((2, 2, n // 2 * job.get("chunks", 1))))
        else:
            outs.append(jax.ShapeDtypeStruct(x.shape, x.dtype))
            sems.append(pltpu.SemaphoreType.DMA((2, len(shifts_of(job["axes"])))))
    return pl.pallas_call(
        functools.partial(comm_kernel, jobs),
        out_shape=outs,
        in_specs=[pl.BlockSpec(memory_space=pltpu.VMEM)] * len(xs),
        out_specs=[pl.BlockSpec(memory_space=pltpu.VMEM)] * len(xs),
        scratch_shapes=sems,
        compiler_params=pltpu.CompilerParams(collective_id=cid, has_side_effects=True),
    )(*xs)


SHIFTS = [(0, 1), (1, 0), (1, 1), (2, 0), (2, 1), (3, 0), (3, 1)]
YC = ("st_1", "st_2")


def near_ring(axis, own, right, left, far, sems, chunks):
    n = AXES[axis]
    me = lax.axis_index(axis)
    size = own.shape[0] // chunks

    def copy(k, d, ch):
        sgn = -1 if d else 1
        line = left if d else right
        last = k == n // 2 - 1
        lo, width = ch * size, size
        if last:
            width = size // 2
            lo = lo + (width if d else 0)
        rng = pl.ds(lo, width)
        src = own if k == 0 else line[k - 1]
        dst = far if last else line[k]
        return pltpu.make_async_remote_copy(
            src_ref=src.at[rng], dst_ref=dst.at[rng],
            send_sem=sems.at[0, d, k * chunks + ch], recv_sem=sems.at[1, d, k * chunks + ch],
            device_id={axis: lax.rem(me + sgn + n, n)}, device_id_type=MESH_ID)

    def start(k, sent):
        for ch in range(chunks):
            for d in range(2):
                cp = copy(k, d, ch)
                cp.start()
                sent.append(cp)

    def take(k, sent, which=None):
        for ch in range(chunks) if which is None else (which,):
            for d in range(2):
                copy(k, d, ch).wait_recv()
                if k + 1 < n // 2:
                    cp = copy(k + 1, d, ch)
                    cp.start()
                    sent.append(cp)

    return start, take


def low_dot(a, b, dims=(((1,), (0,)), ((), ()))):
    return lax.dot_general(
        a.astype(jnp.bfloat16), b.astype(jnp.bfloat16), dims, preferred_element_type=jnp.float32)


def mixer_pieces(mq, mk, mv, st, ld, rate, fresh, corr, attend, qdec, kdec, cdec, state, mixed):
    f32 = jnp.float32
    row_i = lax.broadcasted_iota(jnp.int32, (64, 64), 0)
    col_i = lax.broadcasted_iota(jnp.int32, (64, 64), 1)

    def prepare(m, n):
        def run():
            i = m * 6 + n
            rows, cols = pl.ds(n * 64, 64), pl.ds(m * 128, 128)
            q = mq[rows, cols].astype(f32)
            k = mk[rows, cols].astype(f32)
            v = mv[rows, cols].astype(f32)
            q = q * lax.rsqrt(jnp.sum(q * q, axis=-1, keepdims=True) + NORM_FLOOR) * 128 ** (-0.5)
            k = k * lax.rsqrt(jnp.sum(k * k, axis=-1, keepdims=True) + NORM_FLOOR)
            pre = ld[m:m + 1, n * 64:n * 64 + 64]
            soft = jnp.maximum(pre, 0.0) + jnp.log1p(jnp.exp(-jnp.abs(pre)))
            ld_row = jnp.broadcast_to(-rate[m] * soft, (64, 64))
            st_row = jnp.broadcast_to(jax.nn.sigmoid(st[m:m + 1, n * 64:n * 64 + 64]), (64, 64))
            ld_col = jnp.sum(jnp.where(row_i == col_i, ld_row, 0.0), axis=1, keepdims=True)
            st_col = jnp.sum(jnp.where(row_i == col_i, st_row, 0.0), axis=1, keepdims=True)
            cum_col = jnp.sum(jnp.where(col_i <= row_i, ld_row, 0.0), axis=1, keepdims=True)
            cum_row = jnp.sum(jnp.where(row_i <= col_i, jnp.broadcast_to(ld_col, (64, 64)), 0.0), axis=0, keepdims=True)
            whole = jnp.sum(ld_col, axis=0, keepdims=True)
            decay = jnp.where(row_i >= col_i, jnp.exp(jnp.minimum(cum_col - cum_row, 0.0)), 0.0)
            gram = low_dot(k, k, CONTRACT_LAST)
            strict = jnp.where(row_i > col_i, st_col * gram * decay, 0.0)
            eye = jnp.where(row_i == col_i, 1.0, 0.0)
            running = eye - strict
            power = strict
            for _ in range(5):
                power = low_dot(power, power)
                running = low_dot(running, eye + power)
            grow = jnp.exp(cum_col)
            fresh[i] = low_dot(running, v * st_col)
            corr[i] = low_dot(running, k * (st_col * grow)).astype(jnp.bfloat16)
            attend[i] = (low_dot(q, k, CONTRACT_LAST) * decay).astype(jnp.bfloat16)
            qdec[i] = (q * grow).astype(jnp.bfloat16)
            kdec[i] = (k * jnp.exp(whole - cum_col)).astype(jnp.bfloat16)
            cdec[i] = jnp.broadcast_to(jnp.exp(whole), (8, 128))
        return run

    def advance(n):
        def run():
            for m in range(2):
                i = m * 6 + n
                rows, cols = pl.ds(n * 64, 64), pl.ds(m * 128, 128)
                if n == 0:
                    new = fresh[i]
                    mixed[rows, cols] = low_dot(attend[i], new)
                    state[m] = low_dot(kdec[i], new, CONTRACT_FIRST)
                else:
                    held = state[m]
                    new = fresh[i] - low_dot(corr[i], held)
                    mixed[rows, cols] = low_dot(qdec[i], held) + low_dot(attend[i], new)
                    if n < 5:
                        state[m] = held * cdec[i][0:1, :] + low_dot(kdec[i], new, CONTRACT_FIRST)
        return run

    return [prepare(m, n) for n in range(6) for m in range(2)], [advance(n) for n in range(6)]


def quarters(rows_ref, rows, w):
    acc = None
    for p in range(4):
        term = jnp.dot(rows_ref[rows, p * 512:(p + 1) * 512], w[p], preferred_element_type=jnp.float32)
        acc = term if acc is None else acc + term
    return acc


def forward_kernel(
    tok, cot, tab, wq, gw, pas, wk, wv, mq, mk, mv, st, ld, rate,
    cot_o, q_o, gate_o, tabs_o, qlow, gate, klow, khat, vlow, mixed, wkc, wvc, wqc, gwc,
    t_r, t_l, t_f, c_r, c_l, c_f, q_own, q_r, q_l, q_f, g_r, g_l, g_f, b_r, b_l, b_f, tsm,
    cst, qst, gst, fresh, corr, attend, qdec, kdec, cdec, state,
    s_t, s_c, s_q, s_g, s_b, s_m, s_cy, s_qy, s_gy, s_w0, s_w1, s_w2, s_w3,
):
    f32, bf16 = jnp.float32, jnp.bfloat16
    z = lax.axis_index("st_0")
    x = lax.axis_index("tp")
    jobs = [ring_peers(dict(axis="tp")), ring_peers(dict(axis="st_0")), a2a_peers(dict(axes=YC)),
            a2a_peers(dict(axes=("tp",)))]
    barrier = pltpu.get_barrier_semaphore()
    peers = [p for job in jobs for p in job]
    for p in peers:
        pl.semaphore_signal(barrier, inc=1, device_id=p, device_id_type=MESH_ID)
    pl.semaphore_wait(barrier, len(peers))
    sent = []
    b_start, b_take = near_ring("st_0", tab, b_r, b_l, b_f, s_b, 1)
    c_start, c_take = near_ring("st_0", cot, c_r, c_l, c_f, s_c, 3)
    t_start, t_take = near_ring("tp", tok, [t_r], [t_l], t_f, s_t, 3)
    q_start, q_take = near_ring("st_0", q_own, q_r, q_l, q_f, s_q, 3)
    g_start, g_take = near_ring("st_0", gate, g_r, g_l, g_f, s_g, 1)
    b_start(0, sent)
    t_start(0, sent)
    c_start(0, sent)

    my_yc, _ = index_of(YC, (0, 0), 1)
    dsts = [index_of(YC, s, 1) for s in SHIFTS]
    srcs = [index_of(YC, s, -1)[0] for s in SHIFTS]
    tabs = [tab] + list(b_r) + list(b_l) + [b_f]
    origins = [lax.rem(z - d + 8, 8) for d in (0, 1, 2, 3, -1, -2, -3, 4)]

    def table_copy(i):
        return pltpu.make_async_copy(tabs[i].at[0], tsm.at[i], s_m.at[i])

    def block_for(i, j):
        return lax.rem(tsm[i, z, j], 8)

    def push(i, buf, stage, out, sems):
        zr = origins[i]
        for s in range(7):
            stage[s, zr] = buf[block_for(i, dsts[s][0])]
        out[zr, my_yc] = buf[block_for(i, my_yc)]
        for s in range(7):
            cp = pltpu.make_async_remote_copy(
                src_ref=stage.at[s, zr], dst_ref=out.at[zr, my_yc], send_sem=sems.at[0, i, s],
                recv_sem=sems.at[1, i, s], device_id=dsts[s][1], device_id_type=MESH_ID)
            cp.start()
            sent.append(cp)

    def pulled(out, sems):
        for i in range(8):
            for s in range(7):
                pltpu.make_async_remote_copy(
                    src_ref=out.at[origins[i], srcs[s]], dst_ref=out.at[origins[i], srcs[s]],
                    send_sem=sems.at[0, i, s], recv_sem=sems.at[1, i, s], device_id=dsts[s][1],
                    device_id_type=MESH_ID).wait_recv()

    cots = [cot] + list(c_r) + list(c_l) + [c_f]
    qs = [q_own] + list(q_r) + list(q_l) + [q_f]
    gs = [gate] + list(g_r) + list(g_l) + [g_f]

    def project(t):
        def run():
            rows = pl.ds(t * 256, 256)
            low = quarters(pas, rows, wk).astype(bf16)
            klow[rows, :] = low
            wide = low.astype(f32)
            norm = lax.rsqrt(jnp.mean(wide * wide, axis=-1, keepdims=True) + NORM_FLOOR)
            khat[rows, :] = (wide * norm).astype(bf16)
            vlow[rows, :] = quarters(pas, rows, wv).astype(bf16)
        return run

    prep, scan = mixer_pieces(mq, mk, mv, st, ld, rate, fresh, corr, attend, qdec, kdec, cdec, state, mixed)
    work = [project(t) for t in range(4)] + prep + scan
    work.reverse()

    def fill(count):
        for _ in range(count):
            if work:
                work.pop()()

    table_copy(0).start()
    fill(1)
    table_copy(0).wait()
    push(0, cot, cst, cot_o, s_cy)
    b_take(0, sent)
    table_copy(1).start()
    table_copy(4).start()
    c_take(0, sent, 0)
    t_take(0, sent, 0)
    c_take(0, sent, 1)
    c_take(0, sent, 2)
    for i in (1, 4):
        table_copy(i).wait()
        push(i, cots[i], cst, cot_o, s_cy)
    t_take(0, sent, 1)
    b_take(1, sent)
    table_copy(2).start()
    table_copy(5).start()
    c_take(1, sent, 0)
    c_take(1, sent, 1)
    t_take(0, sent, 2)
    c_take(1, sent, 2)
    for i in (2, 5):
        table_copy(i).wait()
        push(i, cots[i], cst, cot_o, s_cy)
    t_take(1, sent, 0)
    b_take(2, sent)
    table_copy(3).start()
    table_copy(6).start()
    c_take(2, sent, 0)
    t_take(1, sent, 1)
    c_take(2, sent, 1)
    t_take(1, sent, 2)

    parts = [(tok, x), (t_r, lax.rem(x + 3, 4)), (t_l, lax.rem(x + 1, 4)), (t_f, lax.rem(x + 2, 4))]
    for half in range(2):
        acc = None
        for buf, p in parts:
            rows = buf[half * 3:half * 3 + 3].reshape(192, 512)
            term = jnp.dot(rows, wq[p], preferred_element_type=f32)
            acc = term if acc is None else acc + term
        low = acc.astype(bf16)
        qlow[half * 192:half * 192 + 192, :] = low
        wide = low.astype(f32)
        norm = lax.rsqrt(jnp.mean(wide * wide, axis=-1, keepdims=True) + NORM_FLOOR)
        q_own[half * 3:half * 3 + 3] = (wide * norm).astype(bf16).reshape(3, 64, 256)
        if half == 0:
            c_take(2, sent, 2)
    for b in range(6):
        acc = None
        for buf, p in parts:
            term = lax.dot_general(gw[:, pl.ds(pl.multiple_of(p * 512, 512), 512)], buf[b], CONTRACT_LAST, preferred_element_type=f32)
            acc = term if acc is None else acc + term
        gate[b, :, 0:64] = jnp.broadcast_to(jax.nn.sigmoid(acc[0:1]), (8, 64))
        gate[b, :, 64:128] = jnp.zeros((8, 64), f32)
    g_start(0, sent)
    q_start(0, sent)
    wcp = []
    for i in range(1, 4):
        to, frm = lax.rem(x + i, 4), lax.rem(x + 4 - i, 4)
        cols = pl.ds(pl.multiple_of(to * 512, 512), 512)
        mine = pltpu.make_async_remote_copy(
            src_ref=gw.at[:, cols], dst_ref=gwc.at[x], send_sem=s_w3.at[0, i - 1], recv_sem=s_w3.at[1, i - 1],
            device_id={"tp": to}, device_id_type=MESH_ID)
        mine.start()
        sent.append(mine)
        wcp.append((mine, pltpu.make_async_remote_copy(
            src_ref=gw.at[:, cols], dst_ref=gwc.at[frm], send_sem=s_w3.at[0, i - 1], recv_sem=s_w3.at[1, i - 1],
            device_id={"tp": to}, device_id_type=MESH_ID)))
    gwc[x] = gw[:, pl.ds(pl.multiple_of(x * 512, 512), 512)]
    for src, dst, sem in ((wk, wkc, s_w0), (wv, wvc, s_w1), (wq, wqc, s_w2)):
        mine, cps = a2a_copies(dict(axes=("tp",)), src, dst, sem)
        for cp, _ in cps:
            cp.start()
            sent.append(cp)
        dst[mine] = src[mine]
        wcp += cps

    for i in (3, 6):
        table_copy(i).wait()
        push(i, cots[i], cst, cot_o, s_cy)
    b_take(3, sent)
    table_copy(7).start()
    c_take(3, sent)
    push(0, q_own, qst, q_o, s_qy)
    table_copy(7).wait()
    push(7, c_f, cst, cot_o, s_cy)
    for k, some in ((0, (1, 4)), (1, (2, 5)), (2, (3, 6)), (3, (7,))):
        g_take(k, sent)
        for ch in range(3):
            q_take(k, sent, ch)
            if ch < 2 and k < 3:
                fill(1)
        for i in some:
            push(i, qs[i], qst, q_o, s_qy)
        fill(1)
    left_half = lax.broadcasted_iota(jnp.int32, (8, 128), 1) < 64

    def side_for(i, j):
        return jnp.where(left_half, gs[i][block_for(i, j)], tsm[i, z, j].astype(f32))

    for i in range(8):
        zr = origins[i]
        tabs_o[zr] = jnp.broadcast_to(tabs[i][0, pl.ds(z, 1), :], (8, 128))
        for s in range(7):
            gst[s, zr] = side_for(i, dsts[s][0])
        gate_o[zr, my_yc] = side_for(i, my_yc)
    side = []
    for s in range(7):
        cp = pltpu.make_async_remote_copy(
            src_ref=gst.at[s], dst_ref=gate_o.at[:, my_yc], send_sem=s_gy.at[0, s], recv_sem=s_gy.at[1, s],
            device_id=dsts[s][1], device_id_type=MESH_ID)
        cp.start()
        sent.append(cp)
        side.append(pltpu.make_async_remote_copy(
            src_ref=gst.at[s], dst_ref=gate_o.at[:, srcs[s]], send_sem=s_gy.at[0, s], recv_sem=s_gy.at[1, s],
            device_id=dsts[s][1], device_id_type=MESH_ID))
    fill(99)
    for r in side:
        r.wait_recv()
    for _, r in wcp:
        r.wait_recv()
    pulled(cot_o, s_cy)
    pulled(q_o, s_qy)
    for cp in sent:
        cp.wait_send()


def forward(ins, cid):
    v = pl.BlockSpec(memory_space=pltpu.VMEM)
    f32, bf16, i32 = jnp.float32, jnp.bfloat16, jnp.int32
    sds = jax.ShapeDtypeStruct
    dma = pltpu.SemaphoreType.DMA
    slots = sds((8, 8, 64, 256), bf16)
    wide = sds((4, 512, 256), bf16)
    return pl.pallas_call(
        forward_kernel,
        out_shape=[
            slots, slots, sds((8, 8, 8, 128), f32), sds((8, 8, 128), i32),
            sds((384, 256), bf16), sds((6, 8, 128), f32), sds((1024, 256), bf16), sds((1024, 256), bf16),
            sds((1024, 256), bf16), sds((384, 256), f32), wide, wide, wide, sds((4, 1, 512), bf16)],
        in_specs=[v] * 13 + [pl.BlockSpec(memory_space=pltpu.SMEM)],
        out_specs=[v] * 14,
        scratch_shapes=[
            pltpu.VMEM((6, 64, 512), bf16), pltpu.VMEM((6, 64, 512), bf16), pltpu.VMEM((6, 64, 512), bf16),
            [pltpu.VMEM((6, 64, 256), bf16)] * 3, [pltpu.VMEM((6, 64, 256), bf16)] * 3, pltpu.VMEM((6, 64, 256), bf16),
            pltpu.VMEM((6, 64, 256), bf16),
            [pltpu.VMEM((6, 64, 256), bf16)] * 3, [pltpu.VMEM((6, 64, 256), bf16)] * 3, pltpu.VMEM((6, 64, 256), bf16),
            [pltpu.VMEM((6, 8, 128), f32)] * 3, [pltpu.VMEM((6, 8, 128), f32)] * 3, pltpu.VMEM((6, 8, 128), f32),
            [pltpu.VMEM((2, 8, 128), i32)] * 3, [pltpu.VMEM((2, 8, 128), i32)] * 3, pltpu.VMEM((2, 8, 128), i32),
            pltpu.SMEM((8, 8, 128), i32),
            pltpu.VMEM((7, 8, 64, 256), bf16), pltpu.VMEM((7, 8, 64, 256), bf16), pltpu.VMEM((7, 8, 8, 128), f32),
            pltpu.VMEM((12, 64, 128), f32), pltpu.VMEM((12, 64, 128), bf16), pltpu.VMEM((12, 64, 64), bf16),
            pltpu.VMEM((12, 64, 128), bf16), pltpu.VMEM((12, 64, 128), bf16), pltpu.VMEM((12, 8, 128), f32),
            pltpu.VMEM((2, 128, 128), f32),
            dma((2, 2, 6)), dma((2, 2, 12)), dma((2, 2, 12)), dma((2, 2, 4)), dma((2, 2, 4)), dma((8,)),
            dma((2, 8, 7)), dma((2, 8, 7)), dma((2, 7)),
            dma((2, 3)), dma((2, 3)), dma((2, 3)), dma((2, 3))],
        compiler_params=pltpu.CompilerParams(
            collective_id=cid, has_side_effects=True, vmem_limit_bytes=60 * 1024 * 1024),
    )(*ins)


def ring(axis, chunks=1):
    return dict(kind="ring", axis=axis, chunks=chunks)


def a2a(*axes):
    return dict(kind="a2a", axes=axes)


def rows_of(vec):
    flat = vec.reshape(-1, 128)
    return jnp.pad(flat, ((0, 16 - flat.shape[0]), (0, 0)))


def stats_kernel(x_ref, m_ref, o_ref, whole, got, tot, every, back, s1, s2, s3):
    job = a2a(*YC)
    barrier = pltpu.get_barrier_semaphore()
    peers = a2a_peers(job) + a2a_peers(a2a("st_0"))
    for p in peers:
        pl.semaphore_signal(barrier, inc=1, device_id=p, device_id_type=MESH_ID)
    pl.semaphore_wait(barrier, len(peers))
    sent = []
    my_yc, _ = index_of(YC, (0, 0), 1)
    dsts = [index_of(YC, s, 1) for s in SHIFTS]
    srcs = [index_of(YC, s, -1)[0] for s in SHIFTS]

    def swap(s, sems, out):
        if out:
            src, dst, land = back.at[dsts[s][0]], o_ref.at[:, my_yc], o_ref.at[:, srcs[s]]
        else:
            src, dst, land = x_ref.at[:, dsts[s][0]], got.at[my_yc], got.at[srcs[s]]
        return [pltpu.make_async_remote_copy(
            src_ref=src, dst_ref=d, send_sem=sems.at[0, s], recv_sem=sems.at[1, s],
            device_id=dsts[s][1], device_id_type=MESH_ID) for d in (dst, land)]

    first = [swap(s, s1, False) for s in range(7)]
    for cp, _ in first:
        cp.start()
        sent.append(cp)
    got[my_yc] = x_ref[:, my_yc]
    for _, r in first:
        r.wait_recv()
    for b in range(6):
        acc = got[0] * m_ref[0, b]
        for j in range(1, 8):
            acc = acc + got[j] * m_ref[j, b]
        tot[b] = acc
    z = lax.axis_index("st_0")
    arrivals = []
    for s in range(1, 8):
        dst = lax.rem(z + s, 8)
        src = lax.rem(z - s + 8, 8)
        cp = pltpu.make_async_remote_copy(
            src_ref=tot, dst_ref=every.at[z], send_sem=s2.at[0, s], recv_sem=s2.at[1, s],
            device_id={"st_0": dst}, device_id_type=MESH_ID)
        rv = pltpu.make_async_remote_copy(
            src_ref=tot, dst_ref=every.at[src], send_sem=s2.at[0, s], recv_sem=s2.at[1, s],
            device_id={"st_0": dst}, device_id_type=MESH_ID)
        cp.start()
        sent.append(cp)
        arrivals.append(rv)
    every[z] = tot[...]
    for rv in arrivals:
        rv.wait_recv()
    for b in range(6):
        acc = every[0, b]
        for k in range(1, 8):
            acc = acc + every[k, b]
        whole[b] = acc
    for j in range(8):
        acc = whole[0] * m_ref[j, 0]
        for b in range(1, 6):
            acc = acc + whole[b] * m_ref[j, b]
        back[j] = acc
    last = [swap(s, s3, True) for s in range(7)]
    for cp, _ in last:
        cp.start()
        sent.append(cp)
    o_ref[:, my_yc] = back[my_yc]
    for _, r in last:
        r.wait_recv()
    for cp in sent:
        cp.wait_send()


def stats_exchange(x, mask, cid):
    v = pl.BlockSpec(memory_space=pltpu.VMEM)
    f = jnp.float32
    return pl.pallas_call(
        stats_kernel,
        out_shape=[jax.ShapeDtypeStruct(x.shape, f), jax.ShapeDtypeStruct((6, 8, 256), f)],
        in_specs=[v] * 2,
        out_specs=[v] * 2,
        scratch_shapes=[
            pltpu.VMEM((8, 8, 256), f), pltpu.VMEM((6, 8, 256), f), pltpu.VMEM((8, 6, 8, 256), f),
            pltpu.VMEM((8, 8, 256), f), pltpu.SemaphoreType.DMA((2, 7)), pltpu.SemaphoreType.DMA((2, 8)),
            pltpu.SemaphoreType.DMA((2, 7))],
        compiler_params=pltpu.CompilerParams(collective_id=cid, has_side_effects=True),
    )(x, mask)


def tail_kernel(
    kg, vg, pas, wkc, wvc, rows_o, w_o, kg4, vg4, acc, w, wc, wcs, wy, wys, wz, s_k, s_v, s_c, s_y, s_z):
    f32, bf16 = jnp.float32, jnp.bfloat16
    barrier = pltpu.get_barrier_semaphore()
    peers = ring_peers(ring("tp")) + a2a_peers(a2a("st_2")) + a2a_peers(a2a("st_1")) + a2a_peers(a2a("st_0"))
    for p in peers:
        pl.semaphore_signal(barrier, inc=1, device_id=p, device_id_type=MESH_ID)
    pl.semaphore_wait(barrier, len(peers))
    sent = []
    rings = []
    for src, dst, sems in ((kg, kg4, s_k), (vg, vg4, s_v)):
        c, a, steps, chunks = ring_starts(ring("tp", 2), src, dst, sems)
        rings.append((c, a))
        for ch in range(2):
            for d in range(2):
                cp = c(0, d, ch)
                cp.start()
                sent.append(cp)
    core = lax.axis_index("st_2")
    x = lax.axis_index("tp")

    def add_head(k_of, v_of, h, first, final):
        for t in range(4):
            rows = pl.ds(t * 256, 256)
            part = lax.dot_general(k_of(rows), wkc[h], CONTRACT_LAST, preferred_element_type=f32)
            part = part + lax.dot_general(v_of(rows), wvc[h], CONTRACT_LAST, preferred_element_type=f32)
            part = part.astype(bf16).astype(f32)
            part = part if first else acc[rows, :] + part
            if final:
                rows_o[rows, :] = part.astype(bf16)
            else:
                acc[rows, :] = part

    for t in range(8):
        cols = pl.ds(t * 256, 256)
        part = lax.dot_general(pas[:, cols], kg[...], CONTRACT_FIRST, preferred_element_type=f32)
        w[t] = part.reshape(4, 2, 32, 256)
    pair = pltpu.make_async_remote_copy(
        src_ref=w.at[:, :, 1 - core], dst_ref=wc, send_sem=s_c.at[0], recv_sem=s_c.at[1],
        device_id={"st_2": 1 - core}, device_id_type=MESH_ID)
    pair.start()
    sent.append(pair)
    add_head(lambda r: kg[r, :], lambda r: vg[r, :], x, True, False)
    pair.wait_recv()
    for k in range(8):
        for y in range(4):
            wcs[y, k] = w[k, y, core] + wc[k, y]
    ym, ycp = a2a_copies(a2a("st_1"), wcs, wy, s_y)
    for cp, _ in ycp:
        cp.start()
        sent.append(cp)
    wy[ym] = wcs[ym]
    for ch in range(2):
        for c, a in rings:
            for d in range(2):
                a(0, d, ch).wait_recv()
                cp = c(1, d, ch)
                cp.start()
                sent.append(cp)
    for h in (lax.rem(x + 1, 4), lax.rem(x + 3, 4)):
        add_head(lambda r: kg4[h, r], lambda r: vg4[h, r], h, False, False)
    for _, r in ycp:
        r.wait_recv()
    for k in range(8):
        wys[k] = (wy[0, k] + wy[1, k]) + (wy[2, k] + wy[3, k])
    zm, zcp = a2a_copies(a2a("st_0"), wys, wz, s_z)
    for cp, _ in zcp:
        cp.start()
        sent.append(cp)
    wz[zm] = wys[zm]
    for ch in range(2):
        for c, a in rings:
            for d in range(2):
                a(1, d, ch).wait_recv()
    far = lax.rem(x + 2, 4)
    add_head(lambda r: kg4[far, r], lambda r: vg4[far, r], far, False, True)
    for _, r in zcp:
        r.wait_recv()
    total = wz[0]
    for k in range(1, 8):
        total = total + wz[k]
    w_o[...] = total
    for cp in sent:
        cp.wait_send()


def tail(kg, vg, pas, wkc, wvc, cid):
    v = pl.BlockSpec(memory_space=pltpu.VMEM)
    f32, bf16 = jnp.float32, jnp.bfloat16
    dma = pltpu.SemaphoreType.DMA
    return pl.pallas_call(
        tail_kernel,
        out_shape=[jax.ShapeDtypeStruct((1024, 512), bf16), jax.ShapeDtypeStruct((32, 256), f32)],
        in_specs=[v] * 5,
        out_specs=[v] * 2,
        scratch_shapes=[
            pltpu.VMEM((4, 1024, 256), bf16), pltpu.VMEM((4, 1024, 256), bf16), pltpu.VMEM((1024, 512), f32),
            pltpu.VMEM((8, 4, 2, 32, 256), f32), pltpu.VMEM((8, 4, 32, 256), f32),
            pltpu.VMEM((4, 8, 32, 256), f32), pltpu.VMEM((4, 8, 32, 256), f32),
            pltpu.VMEM((8, 32, 256), f32), pltpu.VMEM((8, 32, 256), f32),
            dma((2, 2, 4)), dma((2, 2, 4)), dma((2,)), dma((2, 3)), dma((2, 7))],
        compiler_params=pltpu.CompilerParams(
            collective_id=cid, has_side_effects=True, vmem_limit_bytes=56 * 1024 * 1024),
    )(kg, vg, pas, wkc, wvc)


def body(
    tokens, cotangent, mix_query, mix_key, mix_value, beta_pre, decay_pre, decay_rate,
    passages, passage_ids, query_weight, key_weight, value_weight, gate_weight,
):
    f32, bf16 = jnp.float32, jnp.bfloat16
    scale = SCORE_GAIN * 256 ** (-0.5)
    z = lax.axis_index("st_0")
    ids = passage_ids.reshape(24)
    owner, local = ids // 16, ids % 16
    match = owner[None, :] == jnp.arange(64, dtype=jnp.int32)[:, None]
    code_of = local * 8 + jnp.arange(24, dtype=jnp.int32) // 4
    code = jnp.sum(jnp.where(match, code_of[None, :], 0), axis=-1, dtype=jnp.int32)
    code = jnp.where(jnp.any(match, axis=-1), code, 128).reshape(8, 8)
    table = jnp.pad(code[None], ((0, 1), (0, 0), (0, 120)))
    flat_rows = passages.reshape(1024, 2048)
    quarter = (4, 512, 256)
    (cot_here, q_here, gate_o, tabs, query_low, gate6, key_low, key_hat, value_all, mixer_out,
     wk_cols, wv_cols, wq_cols, gw_cols) = forward(
        [tokens.reshape(6, 64, 512), cotangent.reshape(6, 64, 256), table,
         query_weight.reshape(quarter), gate_weight, flat_rows, key_weight.reshape(quarter),
         value_weight.reshape(quarter), mix_query, mix_key, mix_value, beta_pre, decay_pre, decay_rate], 1)
    cot_here, q_here = cot_here.reshape(64, 64, 256), q_here.reshape(64, 64, 256)
    codes = tabs[:, 0, :8]
    side = gate_o[:, :, 0, :].reshape(64, 128)
    gate_here = side[:, :64]
    code_here = side[:, 64].astype(jnp.int32)
    used = code_here < 128
    loc = jnp.where(used, code_here // 8, 0)
    gate_open = gate6[:, 0, :64].reshape(384)
    query_float = query_low.astype(f32)
    query_scale = lax.rsqrt(jnp.mean(query_float * query_float, axis=-1, keepdims=True) + NORM_FLOOR)
    key_float = key_low.astype(f32)
    key_scale = lax.rsqrt(jnp.mean(key_float * key_float, axis=-1, keepdims=True) + NORM_FLOOR)
    k_sel = key_hat.reshape(16, 64, 256)[loc]
    v_sel = value_all.reshape(16, 64, 256)[loc]

    scores = jnp.einsum("sid,sjd->sij", q_here, k_sel, preferred_element_type=f32) * scale
    exps = jnp.exp(scores)
    g_here = (gate_here[:, :, None] * cot_here.astype(f32)).astype(bf16)
    grad_probs = jnp.einsum("sid,sjd->sij", g_here, v_sel, preferred_element_type=f32)
    cot_dots = jnp.einsum("sid,sjd->sij", cot_here, v_sel, preferred_element_type=f32)
    sums = jnp.concatenate(
        [jnp.sum(exps, axis=-1), jnp.sum(exps * grad_probs, axis=-1), jnp.sum(exps * cot_dots, axis=-1),
         jnp.zeros((64, 64), f32)], axis=-1)

    blk = jnp.where(codes < 128, codes % 8, 7)
    mask = (blk.T[:, None, :] == jnp.arange(6, dtype=jnp.int32)[None, :, None]).astype(f32)
    mask = jnp.broadcast_to(mask[..., None], (8, 6, 8, 256))
    whole, mine = stats_exchange(sums.reshape(8, 8, 256), mask, 2)
    whole = whole.reshape(64, 256)
    mine = lax.dynamic_slice(mine, (0, z, 0), (6, 1, 256)).reshape(6, 256)
    read_dot = (mine[:, 128:192] / mine[:, :64]).reshape(384)
    total = jnp.where(used[:, None], whole[:, :64], 1.0)
    inner = jnp.where(used[:, None], whole[:, 64:128], 0.0) / total
    probs = jnp.where(used[:, None, None], exps, 0.0) / total[:, :, None]
    probs_low = probs.astype(bf16)
    score_grad = (probs * (grad_probs - inner[:, :, None])).astype(bf16)
    q_part = (scale * jnp.einsum("sij,sjd->sid", score_grad, k_sel, preferred_element_type=f32)).astype(bf16)
    q_back = lax.all_to_all(q_part, ST, split_axis=0, concat_axis=0, tiled=True)

    key_term = (scale * jnp.einsum("sij,sid->sjd", score_grad, q_here, preferred_element_type=f32)).astype(bf16)
    value_term = jnp.einsum("sij,sid->sjd", probs_low, g_here, preferred_element_type=f32).astype(bf16)
    onehot = ((loc[None, :] == jnp.arange(16, dtype=jnp.int32)[:, None]) & used[None, :]).astype(bf16)
    key_grad_hat = jnp.dot(onehot, key_term.reshape(64, -1), preferred_element_type=f32).reshape(1024, 256)
    value_grad = jnp.dot(onehot, value_term.reshape(64, -1), preferred_element_type=f32).reshape(1024, 256)
    key_grad = (
        key_scale * key_grad_hat
        - key_scale**3 * key_float * jnp.mean(key_float * key_grad_hat, axis=-1, keepdims=True)
    ).astype(bf16)
    value_grad_low = value_grad.astype(bf16)
    passage_grad, key_weight_grad = tail(key_grad, value_grad_low, flat_rows, wk_cols, wv_cols, 3)
    passage_grad = passage_grad.reshape(16, 64, 512)

    qhat_grad = jnp.sum(q_back[owner].astype(f32).reshape(6, 4, 64, 256), axis=1).reshape(384, 256)
    grad_out = cotangent.astype(f32)
    gate_grad = (read_dot - jnp.sum(grad_out * mixer_out, axis=-1)) * gate_open * (1.0 - gate_open)
    query_grad = (
        query_scale * qhat_grad
        - query_scale**3 * query_float * jnp.mean(query_float * qhat_grad, axis=-1, keepdims=True)
    ).astype(bf16)
    qg4, gg4 = comm([ring("tp", 2), ring("tp")], [query_grad, rows_of(gate_grad)], 4)
    gg4 = gg4[:, :3].reshape(4, 384)
    token_part = (
        jnp.einsum("htd,hed->hte", qg4, wq_cols, preferred_element_type=f32)
        + gg4[:, :, None] * gw_cols.astype(f32)
    ).astype(bf16)
    token_grad = jnp.sum(token_part.astype(f32), axis=0).astype(bf16)
    return token_grad, passage_grad, key_weight_grad


def solution(mesh):
    torus = Mesh(mesh.devices.reshape(8, 4, 2, mesh.shape["tp"]), ("st_0", "st_1", "st_2", "tp"))
    return jax.shard_map(
        body,
        mesh=torus,
        in_specs=(
            P(ST, "tp"),
            P(ST, "tp"),
            P(ST, "tp"),
            P(ST, "tp"),
            P(ST, "tp"),
            P("tp", ST),
            P("tp", ST),
            P("tp"),
            P(ST, None, None),
            P(ST, None),
            P(None, "tp"),
            P(None, "tp"),
            P(None, "tp"),
            P("tp", None),
        ),
        out_specs=(P(ST, "tp"), P(ST, None, "tp"), P(ST, "tp")),
        check_vma=False,
    )
```

```python
import functools

import jax
import jax.numpy as jnp
from jax import lax
from jax.experimental import pallas as pl
from jax.experimental.pallas import tpu as pltpu
from jax.sharding import Mesh
from jax.sharding import PartitionSpec as P

SPAN = 64
ST = ("st_0", "st_1", "st_2")


NORM_FLOOR = 1.0
SCORE_GAIN = 4.0
CONTRACT_LAST = (((1,), (1,)), ((), ()))
CONTRACT_FIRST = (((0,), (0,)), ((), ()))


AXES = {"st_0": 8, "st_1": 4, "st_2": 2, "tp": 4}
MESH_ID = pl.DeviceIdType.MESH


def ring_starts(job, x_ref, o_ref, sems):
    axis, n, chunks = job["axis"], AXES[job["axis"]], job.get("chunks", 1)
    rows = x_ref.shape[0]
    me = lax.axis_index(axis)
    step_rows = rows // chunks

    def part(k, d, ch):
        lo, size = ch * step_rows, step_rows
        if k == n // 2 - 1:
            size = step_rows // 2
            lo = lo + (size if d else 0)
        return pl.ds(lo, size)

    def copy(k, d, ch):
        sgn = -1 if d else 1
        origin = lax.rem(me - sgn * k + 2 * n, n)
        rng = part(k, d, ch)
        src = x_ref.at[rng] if k == 0 else o_ref.at[origin, rng]
        return pltpu.make_async_remote_copy(
            src_ref=src, dst_ref=o_ref.at[origin, rng],
            send_sem=sems.at[0, d, k * chunks + ch], recv_sem=sems.at[1, d, k * chunks + ch],
            device_id={axis: lax.rem(me + sgn + n, n)}, device_id_type=MESH_ID)

    def arrival(k, d, ch):
        sgn = -1 if d else 1
        origin = lax.rem(me - sgn * (k + 1) + 2 * n, n)
        rng = part(k, d, ch)
        return pltpu.make_async_remote_copy(
            src_ref=o_ref.at[origin, rng], dst_ref=o_ref.at[origin, rng],
            send_sem=sems.at[0, d, k * chunks + ch], recv_sem=sems.at[1, d, k * chunks + ch],
            device_id={axis: lax.rem(me + sgn + n, n)}, device_id_type=MESH_ID)

    return copy, arrival, n // 2, chunks


def ring_peers(job):
    axis, n = job["axis"], AXES[job["axis"]]
    me = lax.axis_index(axis)
    return [{axis: lax.rem(me + 1, n)}, {axis: lax.rem(me + n - 1, n)}]


def shifts_of(axes):
    out = [()]
    for a in axes:
        out = [s + (d,) for s in out for d in range(AXES[a])]
    return [s for s in out if any(s)]


def index_of(axes, shift, sign):
    idx, dev = 0, {}
    for a, d in zip(axes, shift):
        n = AXES[a]
        c = lax.rem(lax.axis_index(a) + sign * d + n, n)
        dev[a] = c
        idx = idx * n + c
    return idx, dev


def a2a_copies(job, x_ref, o_ref, sems):
    axes = job["axes"]
    my_idx, _ = index_of(axes, (0,) * len(axes), 1)
    out = []
    for i, s in enumerate(shifts_of(axes)):
        dst_i, dst_d = index_of(axes, s, 1)
        src_i, _ = index_of(axes, s, -1)
        send = pltpu.make_async_remote_copy(
            src_ref=x_ref.at[dst_i], dst_ref=o_ref.at[my_idx], send_sem=sems.at[0, i],
            recv_sem=sems.at[1, i], device_id=dst_d, device_id_type=MESH_ID)
        recv = pltpu.make_async_remote_copy(
            src_ref=o_ref.at[src_i], dst_ref=o_ref.at[src_i], send_sem=sems.at[0, i],
            recv_sem=sems.at[1, i], device_id=dst_d, device_id_type=MESH_ID)
        out.append((send, recv))
    return my_idx, out


def a2a_peers(job):
    return [index_of(job["axes"], s, 1)[1] for s in shifts_of(job["axes"])]


def comm_kernel(jobs, *refs):
    nj = len(jobs)
    xs, os_, sems = refs[:nj], refs[nj:2 * nj], refs[2 * nj:]
    barrier = pltpu.get_barrier_semaphore()
    peers = []
    for job in jobs:
        peers += ring_peers(job) if job["kind"] == "ring" else a2a_peers(job)
    for p in peers:
        pl.semaphore_signal(barrier, inc=1, device_id=p, device_id_type=MESH_ID)
    pl.semaphore_wait(barrier, len(peers))
    rings, alls, sent = [], [], []
    for job, x, o, s in zip(jobs, xs, os_, sems):
        if job["kind"] == "ring":
            rings.append(ring_starts(job, x, o, s))
            c, a, steps, chunks = rings[-1]
            for ch in range(chunks):
                for d in range(2):
                    cp = c(0, d, ch); cp.start(); sent.append(cp)
    for job, x, o, s in zip(jobs, xs, os_, sems):
        if job["kind"] == "a2a":
            mine, cps = a2a_copies(job, x, o, s)
            for cp, _ in cps:
                cp.start(); sent.append(cp)
            alls.append((cps, mine, x, o))
            o[mine] = x[mine]
    for job, x, o in zip(jobs, xs, os_):
        if job["kind"] == "ring":
            o[lax.axis_index(job["axis"])] = x[...]
    for k in range(max([r[2] for r in rings], default=0)):
        for c, a, steps, chunks in rings:
            if k < steps:
                for ch in range(chunks):
                    for d in range(2):
                        a(k, d, ch).wait_recv()
                        if k + 1 < steps:
                            cp = c(k + 1, d, ch); cp.start(); sent.append(cp)
    for cps, *_ in alls:
        for _, r in cps:
            r.wait_recv()
    for cp in sent:
        cp.wait_send()


def comm(jobs, xs, cid):
    outs, sems = [], []
    for job, x in zip(jobs, xs):
        if job["kind"] == "ring":
            n = AXES[job["axis"]]
            outs.append(jax.ShapeDtypeStruct((n, *x.shape), x.dtype))
            sems.append(pltpu.SemaphoreType.DMA((2, 2, n // 2 * job.get("chunks", 1))))
        else:
            outs.append(jax.ShapeDtypeStruct(x.shape, x.dtype))
            sems.append(pltpu.SemaphoreType.DMA((2, len(shifts_of(job["axes"])))))
    return pl.pallas_call(
        functools.partial(comm_kernel, jobs),
        out_shape=outs,
        in_specs=[pl.BlockSpec(memory_space=pltpu.VMEM)] * len(xs),
        out_specs=[pl.BlockSpec(memory_space=pltpu.VMEM)] * len(xs),
        scratch_shapes=sems,
        compiler_params=pltpu.CompilerParams(collective_id=cid, has_side_effects=True),
    )(*xs)


SHIFTS = [(0, 1), (1, 0), (1, 1), (2, 0), (2, 1), (3, 0), (3, 1)]
YC = ("st_1", "st_2")


def near_ring(axis, own, right, left, far, sems, chunks):
    n = AXES[axis]
    me = lax.axis_index(axis)
    size = own.shape[0] // chunks

    def copy(k, d, ch):
        sgn = -1 if d else 1
        line = left if d else right
        last = k == n // 2 - 1
        lo, width = ch * size, size
        if last:
            width = size // 2
            lo = lo + (width if d else 0)
        rng = pl.ds(lo, width)
        src = own if k == 0 else line[k - 1]
        dst = far if last else line[k]
        return pltpu.make_async_remote_copy(
            src_ref=src.at[rng], dst_ref=dst.at[rng],
            send_sem=sems.at[0, d, k * chunks + ch], recv_sem=sems.at[1, d, k * chunks + ch],
            device_id={axis: lax.rem(me + sgn + n, n)}, device_id_type=MESH_ID)

    def start(k, sent, which=None):
        for ch in range(chunks) if which is None else (which,):
            for d in range(2):
                cp = copy(k, d, ch)
                cp.start()
                sent.append(cp)

    def take(k, sent, which=None):
        for ch in range(chunks) if which is None else (which,):
            for d in range(2):
                copy(k, d, ch).wait_recv()
                if k + 1 < n // 2:
                    cp = copy(k + 1, d, ch)
                    cp.start()
                    sent.append(cp)

    return start, take


def low_dot(a, b, dims=(((1,), (0,)), ((), ()))):
    return lax.dot_general(
        a.astype(jnp.bfloat16), b.astype(jnp.bfloat16), dims, preferred_element_type=jnp.float32)


def mixer_pieces(mq, mk, mv, st, ld, rate, fresh, corr, attend, qdec, kdec, cdec, state, mixed):
    f32 = jnp.float32
    row_i = lax.broadcasted_iota(jnp.int32, (64, 64), 0)
    col_i = lax.broadcasted_iota(jnp.int32, (64, 64), 1)

    def prepare(m, n):
        def run():
            i = m * 6 + n
            rows, cols = pl.ds(n * 64, 64), pl.ds(m * 128, 128)
            q = mq[rows, cols].astype(f32)
            k = mk[rows, cols].astype(f32)
            v = mv[rows, cols].astype(f32)
            q = q * lax.rsqrt(jnp.sum(q * q, axis=-1, keepdims=True) + NORM_FLOOR) * 128 ** (-0.5)
            k = k * lax.rsqrt(jnp.sum(k * k, axis=-1, keepdims=True) + NORM_FLOOR)
            pre = ld[m:m + 1, n * 64:n * 64 + 64]
            soft = jnp.maximum(pre, 0.0) + jnp.log1p(jnp.exp(-jnp.abs(pre)))
            ld_row = jnp.broadcast_to(-rate[m] * soft, (64, 64))
            st_row = jnp.broadcast_to(jax.nn.sigmoid(st[m:m + 1, n * 64:n * 64 + 64]), (64, 64))
            ld_col = jnp.sum(jnp.where(row_i == col_i, ld_row, 0.0), axis=1, keepdims=True)
            st_col = jnp.sum(jnp.where(row_i == col_i, st_row, 0.0), axis=1, keepdims=True)
            cum_col = jnp.sum(jnp.where(col_i <= row_i, ld_row, 0.0), axis=1, keepdims=True)
            cum_row = jnp.sum(jnp.where(row_i <= col_i, jnp.broadcast_to(ld_col, (64, 64)), 0.0), axis=0, keepdims=True)
            whole = jnp.sum(ld_col, axis=0, keepdims=True)
            decay = jnp.where(row_i >= col_i, jnp.exp(jnp.minimum(cum_col - cum_row, 0.0)), 0.0)
            gram = low_dot(k, k, CONTRACT_LAST)
            strict = jnp.where(row_i > col_i, st_col * gram * decay, 0.0)
            eye = jnp.where(row_i == col_i, 1.0, 0.0)
            running = eye - strict
            power = strict
            for _ in range(5):
                power = low_dot(power, power)
                running = low_dot(running, eye + power)
            grow = jnp.exp(cum_col)
            fresh[i] = low_dot(running, v * st_col)
            corr[i] = low_dot(running, k * (st_col * grow)).astype(jnp.bfloat16)
            attend[i] = (low_dot(q, k, CONTRACT_LAST) * decay).astype(jnp.bfloat16)
            qdec[i] = (q * grow).astype(jnp.bfloat16)
            kdec[i] = (k * jnp.exp(whole - cum_col)).astype(jnp.bfloat16)
            cdec[i] = jnp.broadcast_to(jnp.exp(whole), (8, 128))
        return run

    def advance(n):
        def run():
            for m in range(2):
                i = m * 6 + n
                rows, cols = pl.ds(n * 64, 64), pl.ds(m * 128, 128)
                if n == 0:
                    new = fresh[i]
                    mixed[rows, cols] = low_dot(attend[i], new)
                    state[m] = low_dot(kdec[i], new, CONTRACT_FIRST)
                else:
                    held = state[m]
                    new = fresh[i] - low_dot(corr[i], held)
                    mixed[rows, cols] = low_dot(qdec[i], held) + low_dot(attend[i], new)
                    if n < 5:
                        state[m] = held * cdec[i][0:1, :] + low_dot(kdec[i], new, CONTRACT_FIRST)
        return run

    return [prepare(m, n) for n in range(6) for m in range(2)], [advance(n) for n in range(6)]


def quarters(rows_ref, rows, w):
    acc = None
    for p in range(4):
        term = jnp.dot(rows_ref[rows, p * 512:(p + 1) * 512], w[p], preferred_element_type=jnp.float32)
        acc = term if acc is None else acc + term
    return acc


def forward_kernel(
    tok, cot, tab, wq, gw, pas_hbm, wk, wv, mq, mk, mv, st, ld, rate,
    cot_o, q_o, gate_o, tabs_o, qlow, gate, klow, khat, vlow, mixed, wkc, wvc, wqc, gwc,
    t_r, t_l, t_f, c_r, c_l, c_f, q_own, q_r, q_l, q_f, g_r, g_l, g_f, b_r, b_l, b_f, tsm,
    cst, qst, gst, pas, fresh, corr, attend, qdec, kdec, cdec, state,
    s_t, s_c, s_q, s_g, s_b, s_m, s_cy, s_qy, s_gy, s_p, s_w0, s_w1, s_w2, s_w3,
):
    f32, bf16 = jnp.float32, jnp.bfloat16
    z = lax.axis_index("st_0")
    x = lax.axis_index("tp")
    store = pltpu.make_async_copy(pas_hbm, pas, s_p)
    store.start()
    jobs = [ring_peers(dict(axis="tp")), ring_peers(dict(axis="st_0")), a2a_peers(dict(axes=YC)),
            a2a_peers(dict(axes=("tp",)))]
    barrier = pltpu.get_barrier_semaphore()
    peers = [p for job in jobs for p in job]
    for p in peers:
        pl.semaphore_signal(barrier, inc=1, device_id=p, device_id_type=MESH_ID)
    pl.semaphore_wait(barrier, len(peers))
    sent = []
    b_start, b_take = near_ring("st_0", tab, b_r, b_l, b_f, s_b, 1)
    c_start, c_take = near_ring("st_0", cot, c_r, c_l, c_f, s_c, 3)
    t_start, t_take = near_ring("tp", tok, [t_r], [t_l], t_f, s_t, 3)
    q_start, q_take = near_ring("st_0", q_own, q_r, q_l, q_f, s_q, 3)
    g_start, g_take = near_ring("st_0", gate, g_r, g_l, g_f, s_g, 1)
    b_start(0, sent)
    t_start(0, sent, 0)
    t_start(0, sent, 1)
    c_start(0, sent)

    my_yc, _ = index_of(YC, (0, 0), 1)
    dsts = [index_of(YC, s, 1) for s in SHIFTS]
    srcs = [index_of(YC, s, -1)[0] for s in SHIFTS]
    tabs = [tab] + list(b_r) + list(b_l) + [b_f]
    origins = [lax.rem(z - d + 8, 8) for d in (0, 1, 2, 3, -1, -2, -3, 4)]

    def table_copy(i):
        return pltpu.make_async_copy(tabs[i].at[0], tsm.at[i], s_m.at[i])

    def block_for(i, j):
        return lax.rem(tsm[i, z, j], 8)

    def push(i, buf, stage, out, sems):
        zr = origins[i]
        for s in range(7):
            stage[s, zr] = buf[block_for(i, dsts[s][0])]
        out[zr, my_yc] = buf[block_for(i, my_yc)]
        for s in range(7):
            cp = pltpu.make_async_remote_copy(
                src_ref=stage.at[s, zr], dst_ref=out.at[zr, my_yc], send_sem=sems.at[0, i, s],
                recv_sem=sems.at[1, i, s], device_id=dsts[s][1], device_id_type=MESH_ID)
            cp.start()
            sent.append(cp)

    def pulled(out, sems):
        for i in range(8):
            for s in range(7):
                pltpu.make_async_remote_copy(
                    src_ref=out.at[origins[i], srcs[s]], dst_ref=out.at[origins[i], srcs[s]],
                    send_sem=sems.at[0, i, s], recv_sem=sems.at[1, i, s], device_id=dsts[s][1],
                    device_id_type=MESH_ID).wait_recv()

    cots = [cot] + list(c_r) + list(c_l) + [c_f]
    qs = [q_own] + list(q_r) + list(q_l) + [q_f]
    gs = [gate] + list(g_r) + list(g_l) + [g_f]

    def project(t):
        def run():
            rows = pl.ds(t * 256, 256)
            low = quarters(pas, rows, wk).astype(bf16)
            klow[rows, :] = low
            wide = low.astype(f32)
            norm = lax.rsqrt(jnp.mean(wide * wide, axis=-1, keepdims=True) + NORM_FLOOR)
            khat[rows, :] = (wide * norm).astype(bf16)
            vlow[rows, :] = quarters(pas, rows, wv).astype(bf16)
        return run

    prep, scan = mixer_pieces(mq, mk, mv, st, ld, rate, fresh, corr, attend, qdec, kdec, cdec, state, mixed)
    work = [project(t) for t in range(4)] + prep + scan
    work.reverse()
    count_all = len(work)

    def fill(count):
        if len(work) == count_all and count:
            store.wait()
        for _ in range(count):
            if work:
                work.pop()()

    parts = [(tok, x), (t_r, lax.rem(x + 3, 4)), (t_l, lax.rem(x + 1, 4)), (t_f, lax.rem(x + 2, 4))]

    def queries(ch):
        acc = None
        for buf, p in parts:
            term = jnp.dot(buf[ch * 2:ch * 2 + 2].reshape(128, 512), wq[p], preferred_element_type=f32)
            acc = term if acc is None else acc + term
        low = acc.astype(bf16)
        qlow[ch * 128:ch * 128 + 128, :] = low
        wide = low.astype(f32)
        norm = lax.rsqrt(jnp.mean(wide * wide, axis=-1, keepdims=True) + NORM_FLOOR)
        q_own[ch * 2:ch * 2 + 2] = (wide * norm).astype(bf16).reshape(2, 64, 256)
        for b in range(ch * 2, ch * 2 + 2):
            acc = None
            for buf, p in parts:
                cols = pl.ds(pl.multiple_of(p * 512, 512), 512)
                term = lax.dot_general(gw[:, cols], buf[b], CONTRACT_LAST, preferred_element_type=f32)
                acc = term if acc is None else acc + term
            gate[b, :, 0:64] = jnp.broadcast_to(jax.nn.sigmoid(acc[0:1]), (8, 64))
            gate[b, :, 64:128] = jnp.zeros((8, 64), f32)
        q_start(0, sent, ch)

    def cot_push(*some):
        for i in some:
            table_copy(i).wait()
            push(i, cots[i], cst, cot_o, s_cy)

    table_copy(0).start()
    fill(1)
    cot_push(0)
    b_take(0, sent)
    table_copy(1).start()
    table_copy(4).start()
    c_take(0, sent, 0)
    t_take(0, sent, 0)
    t_start(0, sent, 2)
    c_take(0, sent, 1)
    c_take(0, sent, 2)
    cot_push(1, 4)
    t_take(0, sent, 1)
    b_take(1, sent)
    table_copy(2).start()
    table_copy(5).start()
    c_take(1, sent, 0)
    t_take(1, sent, 0)
    queries(0)
    c_take(1, sent, 1)
    c_take(1, sent, 2)
    cot_push(2, 5)
    t_take(0, sent, 2)
    b_take(2, sent)
    table_copy(3).start()
    table_copy(6).start()
    c_take(2, sent, 0)
    t_take(1, sent, 1)
    queries(1)
    c_take(2, sent, 1)
    c_take(2, sent, 2)
    t_take(1, sent, 2)
    queries(2)
    g_start(0, sent)
    wcp = []
    for i in range(1, 4):
        to, frm = lax.rem(x + i, 4), lax.rem(x + 4 - i, 4)
        cols = pl.ds(pl.multiple_of(to * 512, 512), 512)
        mine = pltpu.make_async_remote_copy(
            src_ref=gw.at[:, cols], dst_ref=gwc.at[x], send_sem=s_w3.at[0, i - 1], recv_sem=s_w3.at[1, i - 1],
            device_id={"tp": to}, device_id_type=MESH_ID)
        mine.start()
        sent.append(mine)
        wcp.append((mine, pltpu.make_async_remote_copy(
            src_ref=gw.at[:, cols], dst_ref=gwc.at[frm], send_sem=s_w3.at[0, i - 1], recv_sem=s_w3.at[1, i - 1],
            device_id={"tp": to}, device_id_type=MESH_ID)))
    gwc[x] = gw[:, pl.ds(pl.multiple_of(x * 512, 512), 512)]
    for src, dst, sem in ((wk, wkc, s_w0), (wv, wvc, s_w1), (wq, wqc, s_w2)):
        mine, cps = a2a_copies(dict(axes=("tp",)), src, dst, sem)
        for cp, _ in cps:
            cp.start()
            sent.append(cp)
        dst[mine] = src[mine]
        wcp += cps

    q_take(0, sent, 0)
    cot_push(3, 6)
    q_take(0, sent, 1)
    b_take(3, sent)
    table_copy(7).start()
    c_take(3, sent)
    push(0, q_own, qst, q_o, s_qy)
    q_take(0, sent, 2)
    cot_push(7)
    g_take(0, sent)
    for k, some in ((1, (1, 4)), (2, (2, 5)), (3, (3, 6))):
        q_take(k, sent, 0)
        for i in some:
            push(i, qs[i], qst, q_o, s_qy)
        fill(1)
        q_take(k, sent, 1)
        fill(1)
        q_take(k, sent, 2)
        g_take(k, sent)
    push(7, q_f, qst, q_o, s_qy)
    left_half = lax.broadcasted_iota(jnp.int32, (8, 128), 1) < 64

    def side_for(i, j):
        return jnp.where(left_half, gs[i][block_for(i, j)], tsm[i, z, j].astype(f32))

    for i in range(8):
        zr = origins[i]
        tabs_o[zr] = jnp.broadcast_to(tabs[i][0, pl.ds(z, 1), :], (8, 128))
        for s in range(7):
            gst[s, zr] = side_for(i, dsts[s][0])
        gate_o[zr, my_yc] = side_for(i, my_yc)
    side = []
    for s in range(7):
        cp = pltpu.make_async_remote_copy(
            src_ref=gst.at[s], dst_ref=gate_o.at[:, my_yc], send_sem=s_gy.at[0, s], recv_sem=s_gy.at[1, s],
            device_id=dsts[s][1], device_id_type=MESH_ID)
        cp.start()
        sent.append(cp)
        side.append(pltpu.make_async_remote_copy(
            src_ref=gst.at[s], dst_ref=gate_o.at[:, srcs[s]], send_sem=s_gy.at[0, s], recv_sem=s_gy.at[1, s],
            device_id=dsts[s][1], device_id_type=MESH_ID))
    fill(99)
    for r in side:
        r.wait_recv()
    for _, r in wcp:
        r.wait_recv()
    pulled(cot_o, s_cy)
    pulled(q_o, s_qy)
    for cp in sent:
        cp.wait_send()


def forward(ins, cid):
    v = pl.BlockSpec(memory_space=pltpu.VMEM)
    f32, bf16, i32 = jnp.float32, jnp.bfloat16, jnp.int32
    sds = jax.ShapeDtypeStruct
    dma = pltpu.SemaphoreType.DMA
    slots = sds((8, 8, 64, 256), bf16)
    wide = sds((4, 512, 256), bf16)
    return pl.pallas_call(
        forward_kernel,
        out_shape=[
            slots, slots, sds((8, 8, 8, 128), f32), sds((8, 8, 128), i32),
            sds((384, 256), bf16), sds((6, 8, 128), f32), sds((1024, 256), bf16), sds((1024, 256), bf16),
            sds((1024, 256), bf16), sds((384, 256), f32), wide, wide, wide, sds((4, 1, 512), bf16)],
        in_specs=[v] * 5 + [pl.BlockSpec(memory_space=pl.ANY)] + [v] * 7 + [pl.BlockSpec(memory_space=pltpu.SMEM)],
        out_specs=[v] * 14,
        scratch_shapes=[
            pltpu.VMEM((6, 64, 512), bf16), pltpu.VMEM((6, 64, 512), bf16), pltpu.VMEM((6, 64, 512), bf16),
            [pltpu.VMEM((6, 64, 256), bf16)] * 3, [pltpu.VMEM((6, 64, 256), bf16)] * 3, pltpu.VMEM((6, 64, 256), bf16),
            pltpu.VMEM((6, 64, 256), bf16),
            [pltpu.VMEM((6, 64, 256), bf16)] * 3, [pltpu.VMEM((6, 64, 256), bf16)] * 3, pltpu.VMEM((6, 64, 256), bf16),
            [pltpu.VMEM((6, 8, 128), f32)] * 3, [pltpu.VMEM((6, 8, 128), f32)] * 3, pltpu.VMEM((6, 8, 128), f32),
            [pltpu.VMEM((2, 8, 128), i32)] * 3, [pltpu.VMEM((2, 8, 128), i32)] * 3, pltpu.VMEM((2, 8, 128), i32),
            pltpu.SMEM((8, 8, 128), i32),
            pltpu.VMEM((7, 8, 64, 256), bf16), pltpu.VMEM((7, 8, 64, 256), bf16), pltpu.VMEM((7, 8, 8, 128), f32),
            pltpu.VMEM((1024, 2048), bf16), pltpu.VMEM((12, 64, 128), f32), pltpu.VMEM((12, 64, 128), bf16), pltpu.VMEM((12, 64, 64), bf16),
            pltpu.VMEM((12, 64, 128), bf16), pltpu.VMEM((12, 64, 128), bf16), pltpu.VMEM((12, 8, 128), f32),
            pltpu.VMEM((2, 128, 128), f32),
            dma((2, 2, 6)), dma((2, 2, 12)), dma((2, 2, 12)), dma((2, 2, 4)), dma((2, 2, 4)), dma((8,)),
            dma((2, 8, 7)), dma((2, 8, 7)), dma((2, 7)), dma,
            dma((2, 3)), dma((2, 3)), dma((2, 3)), dma((2, 3))],
        compiler_params=pltpu.CompilerParams(
            collective_id=cid, has_side_effects=True, vmem_limit_bytes=60 * 1024 * 1024),
    )(*ins)


def ring(axis, chunks=1):
    return dict(kind="ring", axis=axis, chunks=chunks)


def a2a(*axes):
    return dict(kind="a2a", axes=axes)


def rows_of(vec):
    flat = vec.reshape(-1, 128)
    return jnp.pad(flat, ((0, 16 - flat.shape[0]), (0, 0)))


def stats_kernel(x_ref, m_ref, o_ref, whole, got, tot, every, back, s1, s2, s3):
    job = a2a(*YC)
    barrier = pltpu.get_barrier_semaphore()
    peers = a2a_peers(job) + a2a_peers(a2a("st_0"))
    for p in peers:
        pl.semaphore_signal(barrier, inc=1, device_id=p, device_id_type=MESH_ID)
    pl.semaphore_wait(barrier, len(peers))
    sent = []
    my_yc, _ = index_of(YC, (0, 0), 1)
    dsts = [index_of(YC, s, 1) for s in SHIFTS]
    srcs = [index_of(YC, s, -1)[0] for s in SHIFTS]

    def swap(s, sems, out):
        if out:
            src, dst, land = back.at[dsts[s][0]], o_ref.at[:, my_yc], o_ref.at[:, srcs[s]]
        else:
            src, dst, land = x_ref.at[:, dsts[s][0]], got.at[my_yc], got.at[srcs[s]]
        return [pltpu.make_async_remote_copy(
            src_ref=src, dst_ref=d, send_sem=sems.at[0, s], recv_sem=sems.at[1, s],
            device_id=dsts[s][1], device_id_type=MESH_ID) for d in (dst, land)]

    first = [swap(s, s1, False) for s in range(7)]
    for cp, _ in first:
        cp.start()
        sent.append(cp)
    got[my_yc] = x_ref[:, my_yc]
    for _, r in first:
        r.wait_recv()
    for b in range(6):
        acc = got[0] * m_ref[0, b]
        for j in range(1, 8):
            acc = acc + got[j] * m_ref[j, b]
        tot[b] = acc
    z = lax.axis_index("st_0")
    arrivals = []
    for s in range(1, 8):
        dst = lax.rem(z + s, 8)
        src = lax.rem(z - s + 8, 8)
        cp = pltpu.make_async_remote_copy(
            src_ref=tot, dst_ref=every.at[z], send_sem=s2.at[0, s], recv_sem=s2.at[1, s],
            device_id={"st_0": dst}, device_id_type=MESH_ID)
        rv = pltpu.make_async_remote_copy(
            src_ref=tot, dst_ref=every.at[src], send_sem=s2.at[0, s], recv_sem=s2.at[1, s],
            device_id={"st_0": dst}, device_id_type=MESH_ID)
        cp.start()
        sent.append(cp)
        arrivals.append(rv)
    every[z] = tot[...]
    for rv in arrivals:
        rv.wait_recv()
    for b in range(6):
        acc = every[0, b]
        for k in range(1, 8):
            acc = acc + every[k, b]
        whole[b] = acc
    for j in range(8):
        acc = whole[0] * m_ref[j, 0]
        for b in range(1, 6):
            acc = acc + whole[b] * m_ref[j, b]
        back[j] = acc
    last = [swap(s, s3, True) for s in range(7)]
    for cp, _ in last:
        cp.start()
        sent.append(cp)
    o_ref[:, my_yc] = back[my_yc]
    for _, r in last:
        r.wait_recv()
    for cp in sent:
        cp.wait_send()


def stats_exchange(x, mask, cid):
    v = pl.BlockSpec(memory_space=pltpu.VMEM)
    f = jnp.float32
    return pl.pallas_call(
        stats_kernel,
        out_shape=[jax.ShapeDtypeStruct(x.shape, f), jax.ShapeDtypeStruct((6, 8, 256), f)],
        in_specs=[v] * 2,
        out_specs=[v] * 2,
        scratch_shapes=[
            pltpu.VMEM((8, 8, 256), f), pltpu.VMEM((6, 8, 256), f), pltpu.VMEM((8, 6, 8, 256), f),
            pltpu.VMEM((8, 8, 256), f), pltpu.SemaphoreType.DMA((2, 7)), pltpu.SemaphoreType.DMA((2, 8)),
            pltpu.SemaphoreType.DMA((2, 7))],
        compiler_params=pltpu.CompilerParams(collective_id=cid, has_side_effects=True),
    )(x, mask)


def tail_kernel(
    kg, vg, pas_hbm, wkc, wvc, rows_o, w_o, kg4, vg4, acc, pas, w, wc, wcs, wy, s_k, s_v, s_c, s_y, s_p):
    f32, bf16 = jnp.float32, jnp.bfloat16
    store = pltpu.make_async_copy(pas_hbm, pas, s_p)
    store.start()
    barrier = pltpu.get_barrier_semaphore()
    peers = ring_peers(ring("tp")) + a2a_peers(a2a("st_2")) + a2a_peers(a2a("st_1"))
    for p in peers:
        pl.semaphore_signal(barrier, inc=1, device_id=p, device_id_type=MESH_ID)
    pl.semaphore_wait(barrier, len(peers))
    sent = []
    rings = []
    for src, dst, sems in ((kg, kg4, s_k), (vg, vg4, s_v)):
        c, a, steps, chunks = ring_starts(ring("tp", 2), src, dst, sems)
        rings.append((c, a))
        for ch in range(2):
            for d in range(2):
                cp = c(0, d, ch)
                cp.start()
                sent.append(cp)
    core = lax.axis_index("st_2")
    x = lax.axis_index("tp")

    def add_head(k_of, v_of, h, first, final):
        for t in range(4):
            rows = pl.ds(t * 256, 256)
            part = lax.dot_general(k_of(rows), wkc[h], CONTRACT_LAST, preferred_element_type=f32)
            part = part + lax.dot_general(v_of(rows), wvc[h], CONTRACT_LAST, preferred_element_type=f32)
            part = part.astype(bf16).astype(f32)
            part = part if first else acc[rows, :] + part
            if final:
                rows_o[rows, :] = part.astype(bf16)
            else:
                acc[rows, :] = part

    store.wait()
    for t in range(8):
        cols = pl.ds(t * 256, 256)
        part = lax.dot_general(pas[:, cols], kg[...], CONTRACT_FIRST, preferred_element_type=f32)
        w[t] = part.reshape(4, 2, 32, 256)
    pair = pltpu.make_async_remote_copy(
        src_ref=w.at[:, :, 1 - core], dst_ref=wc, send_sem=s_c.at[0], recv_sem=s_c.at[1],
        device_id={"st_2": 1 - core}, device_id_type=MESH_ID)
    pair.start()
    sent.append(pair)
    add_head(lambda r: kg[r, :], lambda r: vg[r, :], x, True, False)
    pair.wait_recv()
    for k in range(8):
        for y in range(4):
            wcs[y, k] = w[k, y, core] + wc[k, y]
    ym, ycp = a2a_copies(a2a("st_1"), wcs, wy, s_y)
    for cp, _ in ycp:
        cp.start()
        sent.append(cp)
    wy[ym] = wcs[ym]
    for ch in range(2):
        for c, a in rings:
            for d in range(2):
                a(0, d, ch).wait_recv()
                cp = c(1, d, ch)
                cp.start()
                sent.append(cp)
    for h in (lax.rem(x + 1, 4), lax.rem(x + 3, 4)):
        add_head(lambda r: kg4[h, r], lambda r: vg4[h, r], h, False, False)
    for ch in range(2):
        for c, a in rings:
            for d in range(2):
                a(1, d, ch).wait_recv()
    far = lax.rem(x + 2, 4)
    add_head(lambda r: kg4[far, r], lambda r: vg4[far, r], far, False, True)
    for _, r in ycp:
        r.wait_recv()
    for k in range(8):
        w_o[k] = (wy[0, k] + wy[1, k]) + (wy[2, k] + wy[3, k])
    for cp in sent:
        cp.wait_send()


def tail(kg, vg, pas, wkc, wvc, cid):
    v = pl.BlockSpec(memory_space=pltpu.VMEM)
    f32, bf16 = jnp.float32, jnp.bfloat16
    dma = pltpu.SemaphoreType.DMA
    return pl.pallas_call(
        tail_kernel,
        out_shape=[jax.ShapeDtypeStruct((1024, 512), bf16), jax.ShapeDtypeStruct((8, 32, 256), f32)],
        in_specs=[v, v, pl.BlockSpec(memory_space=pl.ANY), v, v],
        out_specs=[v] * 2,
        scratch_shapes=[
            pltpu.VMEM((4, 1024, 256), bf16), pltpu.VMEM((4, 1024, 256), bf16), pltpu.VMEM((1024, 512), f32),
            pltpu.VMEM((1024, 2048), bf16),
            pltpu.VMEM((8, 4, 2, 32, 256), f32), pltpu.VMEM((8, 4, 32, 256), f32),
            pltpu.VMEM((4, 8, 32, 256), f32), pltpu.VMEM((4, 8, 32, 256), f32),
            dma((2, 2, 4)), dma((2, 2, 4)), dma((2,)), dma((2, 3)), dma],
        compiler_params=pltpu.CompilerParams(
            collective_id=cid, has_side_effects=True, vmem_limit_bytes=56 * 1024 * 1024),
    )(kg, vg, pas, wkc, wvc)


def body(
    tokens, cotangent, mix_query, mix_key, mix_value, beta_pre, decay_pre, decay_rate,
    passages, passage_ids, query_weight, key_weight, value_weight, gate_weight,
):
    f32, bf16 = jnp.float32, jnp.bfloat16
    scale = SCORE_GAIN * 256 ** (-0.5)
    z = lax.axis_index("st_0")
    ids = passage_ids.reshape(24)
    owner, local = ids // 16, ids % 16
    match = owner[None, :] == jnp.arange(64, dtype=jnp.int32)[:, None]
    code_of = local * 8 + jnp.arange(24, dtype=jnp.int32) // 4
    code = jnp.sum(jnp.where(match, code_of[None, :], 0), axis=-1, dtype=jnp.int32)
    code = jnp.where(jnp.any(match, axis=-1), code, 128).reshape(8, 8)
    table = jnp.pad(code[None], ((0, 1), (0, 0), (0, 120)))
    flat_rows = passages.reshape(1024, 2048)
    quarter = (4, 512, 256)
    (cot_here, q_here, gate_o, tabs, query_low, gate6, key_low, key_hat, value_all, mixer_out,
     wk_cols, wv_cols, wq_cols, gw_cols) = forward(
        [tokens.reshape(6, 64, 512), cotangent.reshape(6, 64, 256), table,
         query_weight.reshape(quarter), gate_weight, flat_rows, key_weight.reshape(quarter),
         value_weight.reshape(quarter), mix_query, mix_key, mix_value, beta_pre, decay_pre, decay_rate], 1)
    cot_here, q_here = cot_here.reshape(64, 64, 256), q_here.reshape(64, 64, 256)
    codes = tabs[:, 0, :8]
    side = gate_o[:, :, 0, :].reshape(64, 128)
    gate_here = side[:, :64]
    code_here = side[:, 64].astype(jnp.int32)
    used = code_here < 128
    loc = jnp.where(used, code_here // 8, 0)
    gate_open = gate6[:, 0, :64].reshape(384)
    query_float = query_low.astype(f32)
    query_scale = lax.rsqrt(jnp.mean(query_float * query_float, axis=-1, keepdims=True) + NORM_FLOOR)
    key_float = key_low.astype(f32)
    key_scale = lax.rsqrt(jnp.mean(key_float * key_float, axis=-1, keepdims=True) + NORM_FLOOR)
    k_sel = key_hat.reshape(16, 64, 256)[loc]
    v_sel = value_all.reshape(16, 64, 256)[loc]

    scores = jnp.einsum("sid,sjd->sij", q_here, k_sel, preferred_element_type=f32) * scale
    exps = jnp.exp(scores)
    g_here = (gate_here[:, :, None] * cot_here.astype(f32)).astype(bf16)
    grad_probs = jnp.einsum("sid,sjd->sij", g_here, v_sel, preferred_element_type=f32)
    cot_dots = jnp.einsum("sid,sjd->sij", cot_here, v_sel, preferred_element_type=f32)
    sums = jnp.concatenate(
        [jnp.sum(exps, axis=-1), jnp.sum(exps * grad_probs, axis=-1), jnp.sum(exps * cot_dots, axis=-1),
         jnp.zeros((64, 64), f32)], axis=-1)

    blk = jnp.where(codes < 128, codes % 8, 7)
    mask = (blk.T[:, None, :] == jnp.arange(6, dtype=jnp.int32)[None, :, None]).astype(f32)
    mask = jnp.broadcast_to(mask[..., None], (8, 6, 8, 256))
    whole, mine = stats_exchange(sums.reshape(8, 8, 256), mask, 2)
    whole = whole.reshape(64, 256)
    mine = lax.dynamic_slice(mine, (0, z, 0), (6, 1, 256)).reshape(6, 256)
    read_dot = (mine[:, 128:192] / mine[:, :64]).reshape(384)
    total = jnp.where(used[:, None], whole[:, :64], 1.0)
    inner = jnp.where(used[:, None], whole[:, 64:128], 0.0) / total
    probs = jnp.where(used[:, None, None], exps, 0.0) / total[:, :, None]
    probs_low = probs.astype(bf16)
    score_grad = (probs * (grad_probs - inner[:, :, None])).astype(bf16)
    q_part = (scale * jnp.einsum("sij,sjd->sid", score_grad, k_sel, preferred_element_type=f32)).astype(bf16)
    q_back = lax.all_to_all(q_part, ST, split_axis=0, concat_axis=0, tiled=True)

    key_term = (scale * jnp.einsum("sij,sid->sjd", score_grad, q_here, preferred_element_type=f32)).astype(bf16)
    value_term = jnp.einsum("sij,sid->sjd", probs_low, g_here, preferred_element_type=f32).astype(bf16)
    onehot = ((loc[:, None] == jnp.arange(16, dtype=jnp.int32)[None, :]) & used[:, None]).astype(bf16)
    key_grad_hat = jnp.einsum("sp,sjd->pjd", onehot, key_term, preferred_element_type=f32)
    value_grad = jnp.einsum("sp,sjd->pjd", onehot, value_term, preferred_element_type=f32)
    key_grad_hat, value_grad = key_grad_hat.reshape(1024, 256), value_grad.reshape(1024, 256)
    key_grad = (
        key_scale * key_grad_hat
        - key_scale**3 * key_float * jnp.mean(key_float * key_grad_hat, axis=-1, keepdims=True)
    ).astype(bf16)
    value_grad_low = value_grad.astype(bf16)
    passage_grad, weight_term = tail(key_grad, value_grad_low, flat_rows, wk_cols, wv_cols, 3)
    passage_grad = passage_grad.reshape(16, 64, 512)

    qhat_grad = jnp.sum(q_back[owner].astype(f32).reshape(6, 4, 64, 256), axis=1).reshape(384, 256)
    grad_out = cotangent.astype(f32)
    gate_grad = (read_dot - jnp.sum(grad_out * mixer_out, axis=-1)) * gate_open * (1.0 - gate_open)
    query_grad = (
        query_scale * qhat_grad
        - query_scale**3 * query_float * jnp.mean(query_float * qhat_grad, axis=-1, keepdims=True)
    ).astype(bf16)
    qg4, gg4, w_z = comm(
        [ring("tp", 2), ring("tp"), a2a("st_0")], [query_grad, rows_of(gate_grad), weight_term], 4)
    key_weight_grad = jnp.sum(w_z, axis=0)
    gg4 = gg4[:, :3].reshape(4, 384)
    token_part = (
        jnp.einsum("htd,hed->hte", qg4, wq_cols, preferred_element_type=f32)
        + gg4[:, :, None] * gw_cols.astype(f32)
    ).astype(bf16)
    token_grad = jnp.sum(token_part.astype(f32), axis=0).astype(bf16)
    return token_grad, passage_grad, key_weight_grad


def solution(mesh):
    torus = Mesh(mesh.devices.reshape(8, 4, 2, mesh.shape["tp"]), ("st_0", "st_1", "st_2", "tp"))
    return jax.shard_map(
        body,
        mesh=torus,
        in_specs=(
            P(ST, "tp"),
            P(ST, "tp"),
            P(ST, "tp"),
            P(ST, "tp"),
            P(ST, "tp"),
            P("tp", ST),
            P("tp", ST),
            P("tp"),
            P(ST, None, None),
            P(ST, None),
            P(None, "tp"),
            P(None, "tp"),
            P(None, "tp"),
            P("tp", None),
        ),
        out_specs=(P(ST, "tp"), P(ST, None, "tp"), P(ST, "tp")),
        check_vma=False,
    )
```

```python
import functools

import jax
import jax.numpy as jnp
from jax import lax
from jax.experimental import pallas as pl
from jax.experimental.pallas import tpu as pltpu
from jax.sharding import Mesh
from jax.sharding import PartitionSpec as P

SPAN = 64
ST = ("st_0", "st_1", "st_2")


NORM_FLOOR = 1.0
SCORE_GAIN = 4.0
CONTRACT_LAST = (((1,), (1,)), ((), ()))
CONTRACT_FIRST = (((0,), (0,)), ((), ()))


AXES = {"st_0": 8, "st_1": 4, "st_2": 2, "tp": 4}
MESH_ID = pl.DeviceIdType.MESH


def ring_starts(job, x_ref, o_ref, sems):
    axis, n, chunks = job["axis"], AXES[job["axis"]], job.get("chunks", 1)
    rows = x_ref.shape[0]
    me = lax.axis_index(axis)
    step_rows = rows // chunks

    def part(k, d, ch):
        lo, size = ch * step_rows, step_rows
        if k == n // 2 - 1:
            size = step_rows // 2
            lo = lo + (size if d else 0)
        return pl.ds(lo, size)

    def copy(k, d, ch):
        sgn = -1 if d else 1
        origin = lax.rem(me - sgn * k + 2 * n, n)
        rng = part(k, d, ch)
        src = x_ref.at[rng] if k == 0 else o_ref.at[origin, rng]
        return pltpu.make_async_remote_copy(
            src_ref=src, dst_ref=o_ref.at[origin, rng],
            send_sem=sems.at[0, d, k * chunks + ch], recv_sem=sems.at[1, d, k * chunks + ch],
            device_id={axis: lax.rem(me + sgn + n, n)}, device_id_type=MESH_ID)

    def arrival(k, d, ch):
        sgn = -1 if d else 1
        origin = lax.rem(me - sgn * (k + 1) + 2 * n, n)
        rng = part(k, d, ch)
        return pltpu.make_async_remote_copy(
            src_ref=o_ref.at[origin, rng], dst_ref=o_ref.at[origin, rng],
            send_sem=sems.at[0, d, k * chunks + ch], recv_sem=sems.at[1, d, k * chunks + ch],
            device_id={axis: lax.rem(me + sgn + n, n)}, device_id_type=MESH_ID)

    return copy, arrival, n // 2, chunks


def ring_peers(job):
    axis, n = job["axis"], AXES[job["axis"]]
    me = lax.axis_index(axis)
    return [{axis: lax.rem(me + 1, n)}, {axis: lax.rem(me + n - 1, n)}]


def shifts_of(axes):
    out = [()]
    for a in axes:
        out = [s + (d,) for s in out for d in range(AXES[a])]
    return [s for s in out if any(s)]


def index_of(axes, shift, sign):
    idx, dev = 0, {}
    for a, d in zip(axes, shift):
        n = AXES[a]
        c = lax.rem(lax.axis_index(a) + sign * d + n, n)
        dev[a] = c
        idx = idx * n + c
    return idx, dev


def a2a_copies(job, x_ref, o_ref, sems):
    axes = job["axes"]
    my_idx, _ = index_of(axes, (0,) * len(axes), 1)
    out = []
    for i, s in enumerate(shifts_of(axes)):
        dst_i, dst_d = index_of(axes, s, 1)
        src_i, _ = index_of(axes, s, -1)
        send = pltpu.make_async_remote_copy(
            src_ref=x_ref.at[dst_i], dst_ref=o_ref.at[my_idx], send_sem=sems.at[0, i],
            recv_sem=sems.at[1, i], device_id=dst_d, device_id_type=MESH_ID)
        recv = pltpu.make_async_remote_copy(
            src_ref=o_ref.at[src_i], dst_ref=o_ref.at[src_i], send_sem=sems.at[0, i],
            recv_sem=sems.at[1, i], device_id=dst_d, device_id_type=MESH_ID)
        out.append((send, recv))
    return my_idx, out


def a2a_peers(job):
    return [index_of(job["axes"], s, 1)[1] for s in shifts_of(job["axes"])]


def comm_kernel(jobs, *refs):
    nj = len(jobs)
    xs, os_, sems = refs[:nj], refs[nj:2 * nj], refs[2 * nj:]
    barrier = pltpu.get_barrier_semaphore()
    peers = []
    for job in jobs:
        peers += ring_peers(job) if job["kind"] == "ring" else a2a_peers(job)
    for p in peers:
        pl.semaphore_signal(barrier, inc=1, device_id=p, device_id_type=MESH_ID)
    pl.semaphore_wait(barrier, len(peers))
    rings, alls, sent = [], [], []
    for job, x, o, s in zip(jobs, xs, os_, sems):
        if job["kind"] == "ring":
            rings.append(ring_starts(job, x, o, s))
            c, a, steps, chunks = rings[-1]
            for ch in range(chunks):
                for d in range(2):
                    cp = c(0, d, ch); cp.start(); sent.append(cp)
    for job, x, o, s in zip(jobs, xs, os_, sems):
        if job["kind"] == "a2a":
            mine, cps = a2a_copies(job, x, o, s)
            for cp, _ in cps:
                cp.start(); sent.append(cp)
            alls.append((cps, mine, x, o))
            o[mine] = x[mine]
    for job, x, o in zip(jobs, xs, os_):
        if job["kind"] == "ring":
            o[lax.axis_index(job["axis"])] = x[...]
    for k in range(max([r[2] for r in rings], default=0)):
        for c, a, steps, chunks in rings:
            if k < steps:
                for ch in range(chunks):
                    for d in range(2):
                        a(k, d, ch).wait_recv()
                        if k + 1 < steps:
                            cp = c(k + 1, d, ch); cp.start(); sent.append(cp)
    for cps, *_ in alls:
        for _, r in cps:
            r.wait_recv()
    for cp in sent:
        cp.wait_send()


def comm(jobs, xs, cid):
    outs, sems = [], []
    for job, x in zip(jobs, xs):
        if job["kind"] == "ring":
            n = AXES[job["axis"]]
            outs.append(jax.ShapeDtypeStruct((n, *x.shape), x.dtype))
            sems.append(pltpu.SemaphoreType.DMA((2, 2, n // 2 * job.get("chunks", 1))))
        else:
            outs.append(jax.ShapeDtypeStruct(x.shape, x.dtype))
            sems.append(pltpu.SemaphoreType.DMA((2, len(shifts_of(job["axes"])))))
    return pl.pallas_call(
        functools.partial(comm_kernel, jobs),
        out_shape=outs,
        in_specs=[pl.BlockSpec(memory_space=pltpu.VMEM)] * len(xs),
        out_specs=[pl.BlockSpec(memory_space=pltpu.VMEM)] * len(xs),
        scratch_shapes=sems,
        compiler_params=pltpu.CompilerParams(collective_id=cid, has_side_effects=True),
    )(*xs)


SHIFTS = [(0, 1), (1, 0), (1, 1), (2, 0), (2, 1), (3, 0), (3, 1)]
YC = ("st_1", "st_2")


def near_ring(axis, own, right, left, far, sems, chunks):
    n = AXES[axis]
    me = lax.axis_index(axis)
    size = own.shape[0] // chunks

    def copy(k, d, ch):
        sgn = -1 if d else 1
        line = left if d else right
        last = k == n // 2 - 1
        lo, width = ch * size, size
        if last:
            width = size // 2
            lo = lo + (width if d else 0)
        rng = pl.ds(lo, width)
        src = own if k == 0 else line[k - 1]
        dst = far if last else line[k]
        return pltpu.make_async_remote_copy(
            src_ref=src.at[rng], dst_ref=dst.at[rng],
            send_sem=sems.at[0, d, k * chunks + ch], recv_sem=sems.at[1, d, k * chunks + ch],
            device_id={axis: lax.rem(me + sgn + n, n)}, device_id_type=MESH_ID)

    def start(k, sent, which=None):
        for ch in range(chunks) if which is None else (which,):
            for d in range(2):
                cp = copy(k, d, ch)
                cp.start()
                sent.append(cp)

    def take(k, sent, which=None):
        for ch in range(chunks) if which is None else (which,):
            for d in range(2):
                copy(k, d, ch).wait_recv()
                if k + 1 < n // 2:
                    cp = copy(k + 1, d, ch)
                    cp.start()
                    sent.append(cp)

    return start, take


def low_dot(a, b, dims=(((1,), (0,)), ((), ()))):
    return lax.dot_general(
        a.astype(jnp.bfloat16), b.astype(jnp.bfloat16), dims, preferred_element_type=jnp.float32)


def mixer_pieces(mq, mk, mv, st, ld, rate, fresh, corr, attend, qdec, kdec, cdec, state, mixed):
    f32 = jnp.float32
    row_i = lax.broadcasted_iota(jnp.int32, (64, 64), 0)
    col_i = lax.broadcasted_iota(jnp.int32, (64, 64), 1)

    def prepare(m, n):
        def run():
            i = m * 6 + n
            rows, cols = pl.ds(n * 64, 64), pl.ds(m * 128, 128)
            q = mq[rows, cols].astype(f32)
            k = mk[rows, cols].astype(f32)
            v = mv[rows, cols].astype(f32)
            q = q * lax.rsqrt(jnp.sum(q * q, axis=-1, keepdims=True) + NORM_FLOOR) * 128 ** (-0.5)
            k = k * lax.rsqrt(jnp.sum(k * k, axis=-1, keepdims=True) + NORM_FLOOR)
            pre = ld[m:m + 1, n * 64:n * 64 + 64]
            soft = jnp.maximum(pre, 0.0) + jnp.log1p(jnp.exp(-jnp.abs(pre)))
            ld_row = jnp.broadcast_to(-rate[m] * soft, (64, 64))
            st_row = jnp.broadcast_to(jax.nn.sigmoid(st[m:m + 1, n * 64:n * 64 + 64]), (64, 64))
            ld_col = jnp.sum(jnp.where(row_i == col_i, ld_row, 0.0), axis=1, keepdims=True)
            st_col = jnp.sum(jnp.where(row_i == col_i, st_row, 0.0), axis=1, keepdims=True)
            cum_col = jnp.sum(jnp.where(col_i <= row_i, ld_row, 0.0), axis=1, keepdims=True)
            cum_row = jnp.sum(jnp.where(row_i <= col_i, jnp.broadcast_to(ld_col, (64, 64)), 0.0), axis=0, keepdims=True)
            whole = jnp.sum(ld_col, axis=0, keepdims=True)
            decay = jnp.where(row_i >= col_i, jnp.exp(jnp.minimum(cum_col - cum_row, 0.0)), 0.0)
            gram = low_dot(k, k, CONTRACT_LAST)
            strict = jnp.where(row_i > col_i, st_col * gram * decay, 0.0)
            eye = jnp.where(row_i == col_i, 1.0, 0.0)
            running = eye - strict
            power = strict
            for _ in range(5):
                power = low_dot(power, power)
                running = low_dot(running, eye + power)
            grow = jnp.exp(cum_col)
            fresh[i] = low_dot(running, v * st_col)
            corr[i] = low_dot(running, k * (st_col * grow)).astype(jnp.bfloat16)
            attend[i] = (low_dot(q, k, CONTRACT_LAST) * decay).astype(jnp.bfloat16)
            qdec[i] = (q * grow).astype(jnp.bfloat16)
            kdec[i] = (k * jnp.exp(whole - cum_col)).astype(jnp.bfloat16)
            cdec[i] = jnp.broadcast_to(jnp.exp(whole), (8, 128))
        return run

    def advance(n):
        def run():
            for m in range(2):
                i = m * 6 + n
                rows, cols = pl.ds(n * 64, 64), pl.ds(m * 128, 128)
                if n == 0:
                    new = fresh[i]
                    mixed[rows, cols] = low_dot(attend[i], new)
                    state[m] = low_dot(kdec[i], new, CONTRACT_FIRST)
                else:
                    held = state[m]
                    new = fresh[i] - low_dot(corr[i], held)
                    mixed[rows, cols] = low_dot(qdec[i], held) + low_dot(attend[i], new)
                    if n < 5:
                        state[m] = held * cdec[i][0:1, :] + low_dot(kdec[i], new, CONTRACT_FIRST)
        return run

    return [prepare(m, n) for n in range(6) for m in range(2)], [advance(n) for n in range(6)]


def quarters(rows_ref, rows, w):
    acc = None
    for p in range(4):
        term = jnp.dot(rows_ref[rows, p * 512:(p + 1) * 512], w[p], preferred_element_type=jnp.float32)
        acc = term if acc is None else acc + term
    return acc


def forward_kernel(
    tok, cot, tab, wq, gw, pas_hbm, wk, wv, mq, mk, mv, st, ld, rate,
    cot_o, q_o, gate_o, tabs_o, qlow, gate, klow, khat, vlow, mixed, wkc, wvc, wqc, gwc,
    t_r, t_l, t_f, c_r, c_l, c_f, q_own, q_r, q_l, q_f, g_r, g_l, g_f, b_r, b_l, b_f, tsm,
    cst, qst, gst, pas, fresh, corr, attend, qdec, kdec, cdec, state,
    s_t, s_c, s_q, s_g, s_b, s_m, s_cy, s_qy, s_gy, s_p, s_w0, s_w1, s_w2, s_w3,
):
    f32, bf16 = jnp.float32, jnp.bfloat16
    z = lax.axis_index("st_0")
    x = lax.axis_index("tp")
    store = pltpu.make_async_copy(pas_hbm, pas, s_p)
    store.start()
    jobs = [ring_peers(dict(axis="tp")), ring_peers(dict(axis="st_0")), a2a_peers(dict(axes=YC)),
            a2a_peers(dict(axes=("tp",)))]
    barrier = pltpu.get_barrier_semaphore()
    peers = [p for job in jobs for p in job]
    for p in peers:
        pl.semaphore_signal(barrier, inc=1, device_id=p, device_id_type=MESH_ID)
    pl.semaphore_wait(barrier, len(peers))
    sent = []
    kept = []
    b_start, b_take = near_ring("st_0", tab, b_r, b_l, b_f, s_b, 1)
    c_start, c_take = near_ring("st_0", cot, c_r, c_l, c_f, s_c, 3)
    t_start, t_take = near_ring("tp", tok, [t_r], [t_l], t_f, s_t, 3)
    q_start, q_take = near_ring("st_0", q_own, q_r, q_l, q_f, s_q, 3)
    g_start, g_take = near_ring("st_0", gate, g_r, g_l, g_f, s_g, 1)
    b_start(0, sent)
    t_start(0, sent, 0)
    t_start(0, sent, 1)
    c_start(0, sent)

    my_yc, _ = index_of(YC, (0, 0), 1)
    dsts = [index_of(YC, s, 1) for s in SHIFTS]
    srcs = [index_of(YC, s, -1)[0] for s in SHIFTS]
    tabs = [tab] + list(b_r) + list(b_l) + [b_f]
    origins = [lax.rem(z - d + 8, 8) for d in (0, 1, 2, 3, -1, -2, -3, 4)]

    def table_copy(i):
        return pltpu.make_async_copy(tabs[i].at[0], tsm.at[i], s_m.at[i])

    def block_for(i, j):
        return lax.rem(tsm[i, z, j], 8)

    def push(i, buf, stage, out, sems):
        zr = origins[i]
        for s in range(7):
            stage[s, zr] = buf[block_for(i, dsts[s][0])]
        stage[7, zr] = buf[block_for(i, my_yc)]
        for s in range(7):
            cp = pltpu.make_async_remote_copy(
                src_ref=stage.at[s, zr], dst_ref=out.at[zr, my_yc], send_sem=sems.at[0, i, s],
                recv_sem=sems.at[1, i, s], device_id=dsts[s][1], device_id_type=MESH_ID)
            cp.start()
            sent.append(cp)
        cp = pltpu.make_async_copy(stage.at[7, zr], out.at[zr, my_yc], sems.at[0, i, 7])
        cp.start()
        kept.append(cp)

    def pulled(out, sems):
        for i in range(8):
            for s in range(7):
                pltpu.make_async_remote_copy(
                    src_ref=out.at[origins[i], srcs[s]], dst_ref=out.at[origins[i], srcs[s]],
                    send_sem=sems.at[0, i, s], recv_sem=sems.at[1, i, s], device_id=dsts[s][1],
                    device_id_type=MESH_ID).wait_recv()

    cots = [cot] + list(c_r) + list(c_l) + [c_f]
    qs = [q_own] + list(q_r) + list(q_l) + [q_f]
    gs = [gate] + list(g_r) + list(g_l) + [g_f]

    def project(t):
        def run():
            rows = pl.ds(t * 256, 256)
            low = quarters(pas, rows, wk).astype(bf16)
            klow[rows, :] = low
            wide = low.astype(f32)
            norm = lax.rsqrt(jnp.mean(wide * wide, axis=-1, keepdims=True) + NORM_FLOOR)
            khat[rows, :] = (wide * norm).astype(bf16)
            vlow[rows, :] = quarters(pas, rows, wv).astype(bf16)
        return run

    prep, scan = mixer_pieces(mq, mk, mv, st, ld, rate, fresh, corr, attend, qdec, kdec, cdec, state, mixed)
    work = [project(t) for t in range(4)] + prep + scan
    work.reverse()
    count_all = len(work)

    def fill(count):
        if len(work) == count_all and count:
            store.wait()
        for _ in range(count):
            if work:
                work.pop()()

    parts = [(tok, x), (t_r, lax.rem(x + 3, 4)), (t_l, lax.rem(x + 1, 4)), (t_f, lax.rem(x + 2, 4))]

    def queries(ch):
        acc = None
        for buf, p in parts:
            term = jnp.dot(buf[ch * 2:ch * 2 + 2].reshape(128, 512), wq[p], preferred_element_type=f32)
            acc = term if acc is None else acc + term
        low = acc.astype(bf16)
        qlow[ch * 128:ch * 128 + 128, :] = low
        wide = low.astype(f32)
        norm = lax.rsqrt(jnp.mean(wide * wide, axis=-1, keepdims=True) + NORM_FLOOR)
        q_own[ch * 2:ch * 2 + 2] = (wide * norm).astype(bf16).reshape(2, 64, 256)
        for b in range(ch * 2, ch * 2 + 2):
            acc = None
            for buf, p in parts:
                cols = pl.ds(pl.multiple_of(p * 512, 512), 512)
                term = lax.dot_general(gw[:, cols], buf[b], CONTRACT_LAST, preferred_element_type=f32)
                acc = term if acc is None else acc + term
            gate[b, :, 0:64] = jnp.broadcast_to(jax.nn.sigmoid(acc[0:1]), (8, 64))
            gate[b, :, 64:128] = jnp.zeros((8, 64), f32)
        q_start(0, sent, ch)

    def cot_push(*some):
        for i in some:
            table_copy(i).wait()
            push(i, cots[i], cst, cot_o, s_cy)

    table_copy(0).start()
    fill(1)
    cot_push(0)
    b_take(0, sent)
    table_copy(1).start()
    table_copy(4).start()
    c_take(0, sent, 0)
    t_take(0, sent, 0)
    t_start(0, sent, 2)
    c_take(0, sent, 1)
    c_take(0, sent, 2)
    cot_push(1, 4)
    t_take(0, sent, 1)
    b_take(1, sent)
    table_copy(2).start()
    table_copy(5).start()
    c_take(1, sent, 0)
    t_take(1, sent, 0)
    queries(0)
    c_take(1, sent, 1)
    c_take(1, sent, 2)
    cot_push(2, 5)
    t_take(0, sent, 2)
    b_take(2, sent)
    table_copy(3).start()
    table_copy(6).start()
    c_take(2, sent, 0)
    t_take(1, sent, 1)
    queries(1)
    c_take(2, sent, 1)
    c_take(2, sent, 2)
    t_take(1, sent, 2)
    queries(2)
    g_start(0, sent)
    wcp = []
    for i in range(1, 4):
        to, frm = lax.rem(x + i, 4), lax.rem(x + 4 - i, 4)
        cols = pl.ds(pl.multiple_of(to * 512, 512), 512)
        mine = pltpu.make_async_remote_copy(
            src_ref=gw.at[:, cols], dst_ref=gwc.at[x], send_sem=s_w3.at[0, i - 1], recv_sem=s_w3.at[1, i - 1],
            device_id={"tp": to}, device_id_type=MESH_ID)
        mine.start()
        sent.append(mine)
        wcp.append((mine, pltpu.make_async_remote_copy(
            src_ref=gw.at[:, cols], dst_ref=gwc.at[frm], send_sem=s_w3.at[0, i - 1], recv_sem=s_w3.at[1, i - 1],
            device_id={"tp": to}, device_id_type=MESH_ID)))
    gwc[x] = gw[:, pl.ds(pl.multiple_of(x * 512, 512), 512)]
    for src, dst, sem in ((wk, wkc, s_w0), (wv, wvc, s_w1), (wq, wqc, s_w2)):
        mine, cps = a2a_copies(dict(axes=("tp",)), src, dst, sem)
        for cp, _ in cps:
            cp.start()
            sent.append(cp)
        cp = pltpu.make_async_copy(src.at[mine], dst.at[mine], sem.at[0, 3])
        cp.start()
        kept.append(cp)
        wcp += cps

    q_take(0, sent, 0)
    cot_push(3, 6)
    q_take(0, sent, 1)
    b_take(3, sent)
    table_copy(7).start()
    c_take(3, sent)
    push(0, q_own, qst, q_o, s_qy)
    q_take(0, sent, 2)
    cot_push(7)
    g_take(0, sent)
    for k, some in ((1, (1, 4)), (2, (2, 5)), (3, (3, 6))):
        q_take(k, sent, 0)
        for i in some:
            push(i, qs[i], qst, q_o, s_qy)
        fill(1)
        q_take(k, sent, 1)
        fill(1)
        q_take(k, sent, 2)
        g_take(k, sent)
    push(7, q_f, qst, q_o, s_qy)
    left_half = lax.broadcasted_iota(jnp.int32, (8, 128), 1) < 64

    def side_for(i, j):
        return jnp.where(left_half, gs[i][block_for(i, j)], tsm[i, z, j].astype(f32))

    for i in range(8):
        zr = origins[i]
        tabs_o[zr] = jnp.broadcast_to(tabs[i][0, pl.ds(z, 1), :], (8, 128))
        for s in range(7):
            gst[s, zr] = side_for(i, dsts[s][0])
        gate_o[zr, my_yc] = side_for(i, my_yc)
    side = []
    for s in range(7):
        cp = pltpu.make_async_remote_copy(
            src_ref=gst.at[s], dst_ref=gate_o.at[:, my_yc], send_sem=s_gy.at[0, s], recv_sem=s_gy.at[1, s],
            device_id=dsts[s][1], device_id_type=MESH_ID)
        cp.start()
        sent.append(cp)
        side.append(pltpu.make_async_remote_copy(
            src_ref=gst.at[s], dst_ref=gate_o.at[:, srcs[s]], send_sem=s_gy.at[0, s], recv_sem=s_gy.at[1, s],
            device_id=dsts[s][1], device_id_type=MESH_ID))
    fill(99)
    for r in side:
        r.wait_recv()
    for _, r in wcp:
        r.wait_recv()
    pulled(cot_o, s_cy)
    pulled(q_o, s_qy)
    for cp in sent:
        cp.wait_send()
    for cp in kept:
        cp.wait()


def forward(ins, cid):
    v = pl.BlockSpec(memory_space=pltpu.VMEM)
    f32, bf16, i32 = jnp.float32, jnp.bfloat16, jnp.int32
    sds = jax.ShapeDtypeStruct
    dma = pltpu.SemaphoreType.DMA
    far = pl.BlockSpec(memory_space=pl.ANY)
    slots = sds((8, 8, 64, 256), bf16)
    wide = sds((4, 512, 256), bf16)
    return pl.pallas_call(
        forward_kernel,
        out_shape=[
            slots, slots, sds((8, 8, 8, 128), f32), sds((8, 8, 128), i32),
            sds((384, 256), bf16), sds((6, 8, 128), f32), sds((1024, 256), bf16), sds((1024, 256), bf16),
            sds((1024, 256), bf16), sds((384, 256), f32), wide, wide, wide, sds((4, 1, 512), bf16)],
        in_specs=[v] * 5 + [pl.BlockSpec(memory_space=pl.ANY)] + [v] * 7 + [pl.BlockSpec(memory_space=pltpu.SMEM)],
        out_specs=[far, far] + [v] * 8 + [far] * 3 + [v],
        scratch_shapes=[
            pltpu.VMEM((6, 64, 512), bf16), pltpu.VMEM((6, 64, 512), bf16), pltpu.VMEM((6, 64, 512), bf16),
            [pltpu.VMEM((6, 64, 256), bf16)] * 3, [pltpu.VMEM((6, 64, 256), bf16)] * 3, pltpu.VMEM((6, 64, 256), bf16),
            pltpu.VMEM((6, 64, 256), bf16),
            [pltpu.VMEM((6, 64, 256), bf16)] * 3, [pltpu.VMEM((6, 64, 256), bf16)] * 3, pltpu.VMEM((6, 64, 256), bf16),
            [pltpu.VMEM((6, 8, 128), f32)] * 3, [pltpu.VMEM((6, 8, 128), f32)] * 3, pltpu.VMEM((6, 8, 128), f32),
            [pltpu.VMEM((2, 8, 128), i32)] * 3, [pltpu.VMEM((2, 8, 128), i32)] * 3, pltpu.VMEM((2, 8, 128), i32),
            pltpu.SMEM((8, 8, 128), i32),
            pltpu.VMEM((8, 8, 64, 256), bf16), pltpu.VMEM((8, 8, 64, 256), bf16), pltpu.VMEM((7, 8, 8, 128), f32),
            pltpu.VMEM((1024, 2048), bf16), pltpu.VMEM((12, 64, 128), f32), pltpu.VMEM((12, 64, 128), bf16), pltpu.VMEM((12, 64, 64), bf16),
            pltpu.VMEM((12, 64, 128), bf16), pltpu.VMEM((12, 64, 128), bf16), pltpu.VMEM((12, 8, 128), f32),
            pltpu.VMEM((2, 128, 128), f32),
            dma((2, 2, 6)), dma((2, 2, 12)), dma((2, 2, 12)), dma((2, 2, 4)), dma((2, 2, 4)), dma((8,)),
            dma((2, 8, 8)), dma((2, 8, 8)), dma((2, 7)), dma,
            dma((2, 4)), dma((2, 4)), dma((2, 4)), dma((2, 4))],
        compiler_params=pltpu.CompilerParams(
            collective_id=cid, has_side_effects=True, vmem_limit_bytes=60 * 1024 * 1024),
    )(*ins)


def ring(axis, chunks=1):
    return dict(kind="ring", axis=axis, chunks=chunks)


def a2a(*axes):
    return dict(kind="a2a", axes=axes)


def rows_of(vec):
    flat = vec.reshape(-1, 128)
    return jnp.pad(flat, ((0, 16 - flat.shape[0]), (0, 0)))


def stats_kernel(x_ref, m_ref, o_ref, whole, got, tot, every, back, s1, s2, s3):
    job = a2a(*YC)
    barrier = pltpu.get_barrier_semaphore()
    peers = a2a_peers(job) + a2a_peers(a2a("st_0"))
    for p in peers:
        pl.semaphore_signal(barrier, inc=1, device_id=p, device_id_type=MESH_ID)
    pl.semaphore_wait(barrier, len(peers))
    sent = []
    my_yc, _ = index_of(YC, (0, 0), 1)
    dsts = [index_of(YC, s, 1) for s in SHIFTS]
    srcs = [index_of(YC, s, -1)[0] for s in SHIFTS]

    def swap(s, sems, out):
        if out:
            src, dst, land = back.at[dsts[s][0]], o_ref.at[:, my_yc], o_ref.at[:, srcs[s]]
        else:
            src, dst, land = x_ref.at[:, dsts[s][0]], got.at[my_yc], got.at[srcs[s]]
        return [pltpu.make_async_remote_copy(
            src_ref=src, dst_ref=d, send_sem=sems.at[0, s], recv_sem=sems.at[1, s],
            device_id=dsts[s][1], device_id_type=MESH_ID) for d in (dst, land)]

    first = [swap(s, s1, False) for s in range(7)]
    for cp, _ in first:
        cp.start()
        sent.append(cp)
    got[my_yc] = x_ref[:, my_yc]
    for _, r in first:
        r.wait_recv()
    for b in range(6):
        acc = got[0] * m_ref[0, b]
        for j in range(1, 8):
            acc = acc + got[j] * m_ref[j, b]
        tot[b] = acc
    z = lax.axis_index("st_0")
    arrivals = []
    for s in range(1, 8):
        dst = lax.rem(z + s, 8)
        src = lax.rem(z - s + 8, 8)
        cp = pltpu.make_async_remote_copy(
            src_ref=tot, dst_ref=every.at[z], send_sem=s2.at[0, s], recv_sem=s2.at[1, s],
            device_id={"st_0": dst}, device_id_type=MESH_ID)
        rv = pltpu.make_async_remote_copy(
            src_ref=tot, dst_ref=every.at[src], send_sem=s2.at[0, s], recv_sem=s2.at[1, s],
            device_id={"st_0": dst}, device_id_type=MESH_ID)
        cp.start()
        sent.append(cp)
        arrivals.append(rv)
    every[z] = tot[...]
    for rv in arrivals:
        rv.wait_recv()
    for b in range(6):
        acc = every[0, b]
        for k in range(1, 8):
            acc = acc + every[k, b]
        whole[b] = acc
    for j in range(8):
        acc = whole[0] * m_ref[j, 0]
        for b in range(1, 6):
            acc = acc + whole[b] * m_ref[j, b]
        back[j] = acc
    last = [swap(s, s3, True) for s in range(7)]
    for cp, _ in last:
        cp.start()
        sent.append(cp)
    o_ref[:, my_yc] = back[my_yc]
    for _, r in last:
        r.wait_recv()
    for cp in sent:
        cp.wait_send()


def stats_exchange(x, mask, cid):
    v = pl.BlockSpec(memory_space=pltpu.VMEM)
    f = jnp.float32
    return pl.pallas_call(
        stats_kernel,
        out_shape=[jax.ShapeDtypeStruct(x.shape, f), jax.ShapeDtypeStruct((6, 8, 256), f)],
        in_specs=[v] * 2,
        out_specs=[v] * 2,
        scratch_shapes=[
            pltpu.VMEM((8, 8, 256), f), pltpu.VMEM((6, 8, 256), f), pltpu.VMEM((8, 6, 8, 256), f),
            pltpu.VMEM((8, 8, 256), f), pltpu.SemaphoreType.DMA((2, 7)), pltpu.SemaphoreType.DMA((2, 8)),
            pltpu.SemaphoreType.DMA((2, 7))],
        compiler_params=pltpu.CompilerParams(collective_id=cid, has_side_effects=True),
    )(x, mask)


def tail_kernel(
    kg, vg, pas_hbm, wkc, wvc, rows_o, w_o, kg4, vg4, acc, pas, w, wc, wcs, wy, s_k, s_v, s_c, s_y, s_p):
    f32, bf16 = jnp.float32, jnp.bfloat16
    store = pltpu.make_async_copy(pas_hbm, pas, s_p)
    store.start()
    barrier = pltpu.get_barrier_semaphore()
    peers = ring_peers(ring("tp")) + a2a_peers(a2a("st_2")) + a2a_peers(a2a("st_1"))
    for p in peers:
        pl.semaphore_signal(barrier, inc=1, device_id=p, device_id_type=MESH_ID)
    pl.semaphore_wait(barrier, len(peers))
    sent = []
    rings = []
    for src, dst, sems in ((kg, kg4, s_k), (vg, vg4, s_v)):
        c, a, steps, chunks = ring_starts(ring("tp", 2), src, dst, sems)
        rings.append((c, a))
        for ch in range(2):
            for d in range(2):
                cp = c(0, d, ch)
                cp.start()
                sent.append(cp)
    core = lax.axis_index("st_2")
    x = lax.axis_index("tp")

    def add_head(k_of, v_of, h, first, final):
        for t in range(4):
            rows = pl.ds(t * 256, 256)
            part = lax.dot_general(k_of(rows), wkc[h], CONTRACT_LAST, preferred_element_type=f32)
            part = part + lax.dot_general(v_of(rows), wvc[h], CONTRACT_LAST, preferred_element_type=f32)
            part = part.astype(bf16).astype(f32)
            part = part if first else acc[rows, :] + part
            if final:
                rows_o[rows, :] = part.astype(bf16)
            else:
                acc[rows, :] = part

    store.wait()
    for t in range(8):
        cols = pl.ds(t * 256, 256)
        part = lax.dot_general(pas[:, cols], kg[...], CONTRACT_FIRST, preferred_element_type=f32)
        w[t] = part.reshape(4, 2, 32, 256)
    pair = pltpu.make_async_remote_copy(
        src_ref=w.at[:, :, 1 - core], dst_ref=wc, send_sem=s_c.at[0], recv_sem=s_c.at[1],
        device_id={"st_2": 1 - core}, device_id_type=MESH_ID)
    pair.start()
    sent.append(pair)
    add_head(lambda r: kg[r, :], lambda r: vg[r, :], x, True, False)
    pair.wait_recv()
    for k in range(8):
        for y in range(4):
            wcs[y, k] = w[k, y, core] + wc[k, y]
    ym, ycp = a2a_copies(a2a("st_1"), wcs, wy, s_y)
    for cp, _ in ycp:
        cp.start()
        sent.append(cp)
    wy[ym] = wcs[ym]
    for ch in range(2):
        for c, a in rings:
            for d in range(2):
                a(0, d, ch).wait_recv()
                cp = c(1, d, ch)
                cp.start()
                sent.append(cp)
    for h in (lax.rem(x + 1, 4), lax.rem(x + 3, 4)):
        add_head(lambda r: kg4[h, r], lambda r: vg4[h, r], h, False, False)
    for ch in range(2):
        for c, a in rings:
            for d in range(2):
                a(1, d, ch).wait_recv()
    far = lax.rem(x + 2, 4)
    add_head(lambda r: kg4[far, r], lambda r: vg4[far, r], far, False, True)
    for _, r in ycp:
        r.wait_recv()
    for k in range(8):
        w_o[k] = (wy[0, k] + wy[1, k]) + (wy[2, k] + wy[3, k])
    for cp in sent:
        cp.wait_send()


def tail(kg, vg, pas, wkc, wvc, cid):
    v = pl.BlockSpec(memory_space=pltpu.VMEM)
    f32, bf16 = jnp.float32, jnp.bfloat16
    dma = pltpu.SemaphoreType.DMA
    return pl.pallas_call(
        tail_kernel,
        out_shape=[jax.ShapeDtypeStruct((1024, 512), bf16), jax.ShapeDtypeStruct((8, 32, 256), f32)],
        in_specs=[v, v, pl.BlockSpec(memory_space=pl.ANY), v, v],
        out_specs=[v] * 2,
        scratch_shapes=[
            pltpu.VMEM((4, 1024, 256), bf16), pltpu.VMEM((4, 1024, 256), bf16), pltpu.VMEM((1024, 512), f32),
            pltpu.VMEM((1024, 2048), bf16),
            pltpu.VMEM((8, 4, 2, 32, 256), f32), pltpu.VMEM((8, 4, 32, 256), f32),
            pltpu.VMEM((4, 8, 32, 256), f32), pltpu.VMEM((4, 8, 32, 256), f32),
            dma((2, 2, 4)), dma((2, 2, 4)), dma((2,)), dma((2, 3)), dma],
        compiler_params=pltpu.CompilerParams(
            collective_id=cid, has_side_effects=True, vmem_limit_bytes=56 * 1024 * 1024),
    )(kg, vg, pas, wkc, wvc)


def body(
    tokens, cotangent, mix_query, mix_key, mix_value, beta_pre, decay_pre, decay_rate,
    passages, passage_ids, query_weight, key_weight, value_weight, gate_weight,
):
    f32, bf16 = jnp.float32, jnp.bfloat16
    scale = SCORE_GAIN * 256 ** (-0.5)
    z = lax.axis_index("st_0")
    ids = passage_ids.reshape(24)
    owner, local = ids // 16, ids % 16
    match = owner[None, :] == jnp.arange(64, dtype=jnp.int32)[:, None]
    code_of = local * 8 + jnp.arange(24, dtype=jnp.int32) // 4
    code = jnp.sum(jnp.where(match, code_of[None, :], 0), axis=-1, dtype=jnp.int32)
    code = jnp.where(jnp.any(match, axis=-1), code, 128).reshape(8, 8)
    table = jnp.pad(code[None], ((0, 1), (0, 0), (0, 120)))
    flat_rows = passages.reshape(1024, 2048)
    quarter = (4, 512, 256)
    (cot_here, q_here, gate_o, tabs, query_low, gate6, key_low, key_hat, value_all, mixer_out,
     wk_cols, wv_cols, wq_cols, gw_cols) = forward(
        [tokens.reshape(6, 64, 512), cotangent.reshape(6, 64, 256), table,
         query_weight.reshape(quarter), gate_weight, flat_rows, key_weight.reshape(quarter),
         value_weight.reshape(quarter), mix_query, mix_key, mix_value, beta_pre, decay_pre, decay_rate], 1)
    cot_here, q_here = cot_here.reshape(64, 64, 256), q_here.reshape(64, 64, 256)
    codes = tabs[:, 0, :8]
    side = gate_o[:, :, 0, :].reshape(64, 128)
    gate_here = side[:, :64]
    code_here = side[:, 64].astype(jnp.int32)
    used = code_here < 128
    loc = jnp.where(used, code_here // 8, 0)
    gate_open = gate6[:, 0, :64].reshape(384)
    query_float = query_low.astype(f32)
    query_scale = lax.rsqrt(jnp.mean(query_float * query_float, axis=-1, keepdims=True) + NORM_FLOOR)
    key_float = key_low.astype(f32)
    key_scale = lax.rsqrt(jnp.mean(key_float * key_float, axis=-1, keepdims=True) + NORM_FLOOR)
    k_sel = key_hat.reshape(16, 64, 256)[loc]
    v_sel = value_all.reshape(16, 64, 256)[loc]

    scores = jnp.einsum("sid,sjd->sij", q_here, k_sel, preferred_element_type=f32) * scale
    exps = jnp.exp(scores)
    g_here = (gate_here[:, :, None] * cot_here.astype(f32)).astype(bf16)
    grad_probs = jnp.einsum("sid,sjd->sij", g_here, v_sel, preferred_element_type=f32)
    cot_dots = jnp.einsum("sid,sjd->sij", cot_here, v_sel, preferred_element_type=f32)
    sums = jnp.concatenate(
        [jnp.sum(exps, axis=-1), jnp.sum(exps * grad_probs, axis=-1), jnp.sum(exps * cot_dots, axis=-1),
         jnp.zeros((64, 64), f32)], axis=-1)

    blk = jnp.where(codes < 128, codes % 8, 7)
    mask = (blk.T[:, None, :] == jnp.arange(6, dtype=jnp.int32)[None, :, None]).astype(f32)
    mask = jnp.broadcast_to(mask[..., None], (8, 6, 8, 256))
    whole, mine = stats_exchange(sums.reshape(8, 8, 256), mask, 2)
    whole = whole.reshape(64, 256)
    mine = lax.dynamic_slice(mine, (0, z, 0), (6, 1, 256)).reshape(6, 256)
    read_dot = (mine[:, 128:192] / mine[:, :64]).reshape(384)
    total = jnp.where(used[:, None], whole[:, :64], 1.0)
    inner = jnp.where(used[:, None], whole[:, 64:128], 0.0) / total
    probs = jnp.where(used[:, None, None], exps, 0.0) / total[:, :, None]
    probs_low = probs.astype(bf16)
    score_grad = (probs * (grad_probs - inner[:, :, None])).astype(bf16)
    q_part = (scale * jnp.einsum("sij,sjd->sid", score_grad, k_sel, preferred_element_type=f32)).astype(bf16)
    q_back = lax.all_to_all(q_part, ST, split_axis=0, concat_axis=0, tiled=True)

    key_term = (scale * jnp.einsum("sij,sid->sjd", score_grad, q_here, preferred_element_type=f32)).astype(bf16)
    value_term = jnp.einsum("sij,sid->sjd", probs_low, g_here, preferred_element_type=f32).astype(bf16)
    onehot = ((loc[:, None] == jnp.arange(16, dtype=jnp.int32)[None, :]) & used[:, None]).astype(bf16)
    key_grad_hat = jnp.einsum("sp,sjd->pjd", onehot, key_term, preferred_element_type=f32)
    value_grad = jnp.einsum("sp,sjd->pjd", onehot, value_term, preferred_element_type=f32)
    key_grad_hat, value_grad = key_grad_hat.reshape(1024, 256), value_grad.reshape(1024, 256)
    key_grad = (
        key_scale * key_grad_hat
        - key_scale**3 * key_float * jnp.mean(key_float * key_grad_hat, axis=-1, keepdims=True)
    ).astype(bf16)
    value_grad_low = value_grad.astype(bf16)
    passage_grad, weight_term = tail(key_grad, value_grad_low, flat_rows, wk_cols, wv_cols, 3)
    passage_grad = passage_grad.reshape(16, 64, 512)

    qhat_grad = jnp.sum(q_back[owner].astype(f32).reshape(6, 4, 64, 256), axis=1).reshape(384, 256)
    grad_out = cotangent.astype(f32)
    gate_grad = (read_dot - jnp.sum(grad_out * mixer_out, axis=-1)) * gate_open * (1.0 - gate_open)
    query_grad = (
        query_scale * qhat_grad
        - query_scale**3 * query_float * jnp.mean(query_float * qhat_grad, axis=-1, keepdims=True)
    ).astype(bf16)
    qg4, gg4, w_z = comm(
        [ring("tp", 2), ring("tp"), a2a("st_0")], [query_grad, rows_of(gate_grad), weight_term], 4)
    key_weight_grad = jnp.sum(w_z, axis=0)
    gg4 = gg4[:, :3].reshape(4, 384)
    token_part = (
        jnp.einsum("htd,hed->hte", qg4, wq_cols, preferred_element_type=f32)
        + gg4[:, :, None] * gw_cols.astype(f32)
    ).astype(bf16)
    token_grad = jnp.sum(token_part.astype(f32), axis=0).astype(bf16)
    return token_grad, passage_grad, key_weight_grad


def solution(mesh):
    torus = Mesh(mesh.devices.reshape(8, 4, 2, mesh.shape["tp"]), ("st_0", "st_1", "st_2", "tp"))
    return jax.shard_map(
        body,
        mesh=torus,
        in_specs=(
            P(ST, "tp"),
            P(ST, "tp"),
            P(ST, "tp"),
            P(ST, "tp"),
            P(ST, "tp"),
            P("tp", ST),
            P("tp", ST),
            P("tp"),
            P(ST, None, None),
            P(ST, None),
            P(None, "tp"),
            P(None, "tp"),
            P(None, "tp"),
            P("tp", None),
        ),
        out_specs=(P(ST, "tp"), P(ST, None, "tp"), P(ST, "tp")),
        check_vma=False,
    )
```
